128 devices in a mesh: ep: 32 (over z, y, core), tp: 4 (over x).
Axes of the slice: x: 4, y: 4, z: 4, core: 2. Of those that a mesh axis runs over, the one named last changes fastest.
Arguments:
- sequence_entry_features: bfloat16 [49152, 4096], P('ep', 'tp'), may hold values from -6 to 6
- sequence_exit_gating: bfloat16 [49152, 4096], P('ep', 'tp'), may hold values from -6 to 6
- memory_insert_clusters: bfloat16 [49152, 1024], P('ep', 'tp'), may hold values from -6 to 6
- memory_query_clusters: bfloat16 [49152, 1024], P('ep', 'tp'), may hold values from -6 to 6
- interval_presoftplus: bfloat16 [49152, 64], P('ep', 'tp'), may hold values from -4 to 4
- entry_filter_taps: bfloat16 [4, 4096], P(None, 'tp'), may hold values from -3 to 3
- insert_filter_taps: bfloat16 [4, 1024], P(None, 'tp'), may hold values from -3 to 3
- query_filter_taps: bfloat16 [4, 1024], P(None, 'tp'), may hold values from -3 to 3
- interval_offset: float32 [64], P('tp'), may hold values from -6 to -1
- head_fading_exponent: float32 [64], P('tp'), may hold values from -8 to -1
- skip_connection_factor: float32 [64], P('tp'), may hold values from 0.1 to 1.9
- spike_fading_exponent: float32 [49152, 64], P('ep', 'tp'), may hold values from -1 to 0
- cluster_scaling_vector: float32 [4096], P('tp'), may hold values from 0.1 to 1.9
- sequence_exit_projection: bfloat16 [4096, 2048], P('tp'), may hold values from -0.09375 to 0.09375
- specialist_sample_slice: bfloat16 [16384, 2048], P(('ep', 'tp')), may hold values from -6 to 6
- specialist_scaling_vector: float32 [2048], replicated, may hold values from 0.1 to 1.9
- chosen_specialists: int32 [16384, 4], P(('ep', 'tp')), may hold values from 0 to 31, all different within a row; in each aligned block of 128 rows (0 to 127, 128 to 255, ...) at most 20 rows name the same one
- dispatcher_affinity_matrix: float32 [16384, 4], P(('ep', 'tp')), may hold values from -4 to 4
- gating_projection: bfloat16 [32, 2048, 2048], P('ep', None, 'tp'), may hold values from -0.5 to 0.5
- expand_projection: bfloat16 [32, 2048, 2048], P('ep', None, 'tp'), may hold values from -0.5 to 0.5
- shrink_projection: bfloat16 [32, 2048, 2048], P('ep', 'tp'), may hold values from -0.03125 to 0.03125
Outputs:
- mixed: bfloat16 [49152, 2048], P(('ep', 'tp'))
- moe_out: bfloat16 [16384, 2048], P(('ep', 'tp'))
The draws below stay inside these ranges and needn't reach their ends.
Inputs may be any that keep to these rules, and one draw needn't show every extreme that they name: `chosen_specialists`: in each aligned block of 128 rows (the rows of one device) no expert is named by more than 20 rows, a bound that some block reaches; the 4 experts of a row differ.
All inputs are finite; a program needn't handle non-finite values.
Results may differ from the reference program's by a relative error of at most 0.015.
Values may be sent and summed in bfloat16 or wider, within the bound.
A program may use at most 192 MiB of HBM per device.

```python
import math
import jax
import jax.numpy as jnp
import numpy as np
from jax import lax

D = 2048
HEADS = 64
HEAD = 64
GROUPS = 8
STATE = 128
TAPS = 4
SPAN = 128
FF = 2048
TOPK = 4
TOKA = 1536
TOK_B = 128
INNER = 4096
EXPERTS = 32
CAP = 20
SEQUENCE_LENGTH = 49152
TOKENS_B = 16384
N_TP = 4


def head_speed(key):
    share = 0.5
    return jax.random.bernoulli(jax.random.fold_in(key, 101), share, (HEADS,))


def draw_head_fading_exponent(key, part):
    quick = head_speed(key)
    fast_rate = jax.random.uniform(jax.random.fold_in(key, 102), (HEADS,), jnp.float32, 0.1, 0.25)
    slow_rate = jax.random.uniform(jax.random.fold_in(key, 103), (HEADS,), jnp.float32, 30.0, 77.0) / SEQUENCE_LENGTH
    return jnp.log(jnp.where(quick, fast_rate, slow_rate)).astype(jnp.float32)


def draw_interval_offset(key, part):
    quick = head_speed(key)
    fast_step = jnp.exp(jax.random.uniform(jax.random.fold_in(key, 104), (HEADS,), jnp.float32, -2.302585, -1.386294))
    slow_step = jnp.exp(jax.random.uniform(jax.random.fold_in(key, 105), (HEADS,), jnp.float32, -5.521461, -4.60517))
    chosen = jnp.where(quick, fast_step, slow_step)
    return (chosen + jnp.log(-jnp.expm1(-chosen))).astype(jnp.float32)


def draw_interval_presoftplus(key, part):
    noise = jnp.clip(0.5 * jax.random.normal(jax.random.fold_in(key, 106), (SEQUENCE_LENGTH, HEADS), jnp.float32), -2.5, 2.5)
    shifts = jax.random.uniform(jax.random.fold_in(key, 107), (SEQUENCE_LENGTH // TOKA, HEADS), jnp.float32, -0.8, 0.8)
    return (noise + jnp.repeat(shifts, TOKA, axis=0)).astype(jnp.bfloat16)


def draw_spike_fading_exponent(key, part):
    spike_positions = jax.random.randint(jax.random.fold_in(key, 108), (3,), 0, SEQUENCE_LENGTH)
    spike_mask = jnp.any(jnp.arange(SEQUENCE_LENGTH)[:, None] == spike_positions[None, :], axis=1)
    objective_values = jnp.log(jax.random.uniform(jax.random.fold_in(key, 109), (SEQUENCE_LENGTH, HEADS), jnp.float32, 0.65, 0.8))
    return jnp.where(spike_mask[:, None], objective_values, 0.0).astype(jnp.float32)


def levels(stream_key, dims, split, smallest, high):
    level, own = 1.0, jax.random.fold_in(stream_key, 6)
    for axis_at, shards_of in split:
        steps = jnp.exp(jax.random.uniform(jax.random.fold_in(own, axis_at), (shards_of,), jnp.float32, smallest / len(split), high / len(split)))
        level = level * jnp.repeat(steps, dims[axis_at] // shards_of).reshape([-1 if axis == axis_at else 1 for axis in range(len(dims))])
    return level


def shared_out(stream_key, own, number, rows, count, top, reach, skew):
    order = jax.random.permutation(stream_key, count)
    packed, usual = shares(count, rows * top, reach, skew, True), shares(count, rows * top, reach, skew, False)
    places = jnp.arange(count)

    def named(lengths, rotation):
        used = int((lengths > 0).sum())
        fixed = max(1, used // 4)
        passed = fixed + (places - fixed + rotation * (used - fixed)) % max(1, count - fixed)
        return jnp.zeros((count,), jnp.int32).at[order[jnp.where(places < fixed, places, passed)]].set(jnp.asarray(lengths, jnp.int32))

    lengths = jnp.where(number % 4 == 0, named(packed, number // 4), named(usual, number - number // 4 - 1))
    mixed = jax.random.permutation(jax.random.fold_in(own, 3), count)
    giver, taker = mixed[0:count // 2 * 2:2], mixed[1:count // 2 * 2:2]
    margin = jnp.minimum(lengths[giver] - 1, reach - lengths[taker]) // 2
    margin = jnp.where((giver == order[0]) | (taker == order[0]) | (lengths[taker] == 0), 0, jnp.maximum(margin, 0))
    passed = jax.random.randint(jax.random.fold_in(own, 4), (count // 2,), 0, 1 << 20) % (margin + 1)
    lengths = lengths.at[giver].add(-passed).at[taker].add(passed)
    labels = jnp.searchsorted(jnp.cumsum(lengths), jnp.arange(rows * top), side="right").astype(jnp.int32)
    listing = labels.reshape(top, rows).T
    listing = listing[jax.random.permutation(jax.random.fold_in(own, 1), rows)]
    rotation = jax.random.randint(jax.random.fold_in(own, 2), (rows, 1), 0, top)
    return jnp.take_along_axis(listing, (jnp.arange(top)[None, :] + rotation) % top, axis=1)


def shares(amount, total, reach, slope, full):
    portions = [(1 << 20) // math.isqrt(rank ** slope) + 1 for rank in range(1, amount + 1)]
    largest = reach if full else min(reach, max(-(-total // amount), total * portions[0] // sum(portions)))
    least = 1 if total - largest >= amount - 1 else 0
    given, rest = [largest] + [least] * (amount - 1), total - largest - least * (amount - 1)
    while rest > 0:
        free = [i for i in range(1, amount) if given[i] < largest] or [i for i in range(1, amount) if given[i] < reach]
        mass, remaining = sum([portions[i] for i in free]), rest
        for i in free:
            more = min(reach - given[i], max(1, remaining * portions[i] // mass), rest)
            given[i] = given[i] + more
            rest = rest - more
    return np.array(given)


def scatter_about(rng, shape, spread, reach, cuts=(), kind=jnp.bfloat16):
    array = spread * jax.random.normal(rng, shape, jnp.float32)
    if cuts:
        array = array * levels(rng, shape, cuts, -0.22, 0.18)
    return jnp.clip(array, -reach, reach).astype(kind)


def setup_inputs(seed: int = 0) -> dict:
    key_list = jax.random.split(jax.random.key(seed), 22)
    sequence_entry_features = scatter_about(key_list[0], (SEQUENCE_LENGTH, INNER), 1.0, 6.0, ((0, 32), (1, 4)))
    sequence_exit_gating = scatter_about(key_list[1], (SEQUENCE_LENGTH, INNER), 1.0, 6.0, ((0, 32), (1, 4)))
    memory_insert_clusters = scatter_about(key_list[2], (SEQUENCE_LENGTH, GROUPS * STATE), 1.0, 6.0, ((0, 32), (1, 4)))
    memory_query_clusters = scatter_about(key_list[3], (SEQUENCE_LENGTH, GROUPS * STATE), 1.0, 6.0, ((0, 32), (1, 4)))
    interval_presoftplus = draw_interval_presoftplus(jax.random.fold_in(key_list[21], 71), 0)
    entry_filter_taps = scatter_about(key_list[5], (TAPS, INNER), 0.5, 3.0, ((1, 4),))
    insert_filter_taps = scatter_about(key_list[6], (TAPS, GROUPS * STATE), 0.5, 3.0, ((1, 4),))
    query_filter_taps = scatter_about(key_list[7], (TAPS, GROUPS * STATE), 0.5, 3.0, ((1, 4),))
    interval_offset = draw_interval_offset(jax.random.fold_in(key_list[21], 71), 0)
    head_fading_exponent = draw_head_fading_exponent(jax.random.fold_in(key_list[21], 71), 0)
    skip_connection_factor = jnp.clip(1.0 + 0.18 * jax.random.normal(key_list[10], (HEADS,), jnp.float32), 0.1, 1.9)
    spike_fading_exponent = draw_spike_fading_exponent(jax.random.fold_in(key_list[21], 71), 0)
    cluster_scaling_vector = jnp.clip(1.0 + 0.18 * jax.random.normal(key_list[12], (INNER,), jnp.float32), 0.1, 1.9)
    sequence_exit_projection = scatter_about(key_list[13], (INNER, D), INNER ** -0.5, 0.09375, ((0, 4),))
    specialist_sample_slice = scatter_about(key_list[14], (TOKENS_B, D), 1.0, 6.0, ((0, 128),))
    specialist_scaling_vector = jnp.clip(1.0 + 0.18 * jax.random.normal(key_list[15], (D,), jnp.float32), 0.1, 1.9)
    chosen_specialists_keys = jax.random.split(jax.random.fold_in(key_list[16], 1), TOKENS_B // TOK_B)
    chosen_specialists_turns = jax.random.permutation(jax.random.fold_in(key_list[16], 3), TOKENS_B // TOK_B)
    chosen_specialists = jax.vmap(lambda own, number: shared_out(jax.random.fold_in(key_list[16], 2), own, number, TOK_B, EXPERTS, TOPK, CAP, 1))(chosen_specialists_keys, chosen_specialists_turns).reshape((TOKENS_B, TOPK))
    dispatcher_affinity_matrix = scatter_about(key_list[17], (TOKENS_B, TOPK), 1.0, 4.0, ((0, 128),), jnp.float32)
    gating_projection = scatter_about(key_list[18], (EXPERTS, D, FF), (D // 16) ** -0.5, 0.5, ((0, 32), (2, 4)))
    expand_projection = scatter_about(key_list[19], (EXPERTS, D, FF), (D // 16) ** -0.5, 0.5, ((0, 32), (2, 4)))
    shrink_projection = scatter_about(key_list[20], (EXPERTS, FF, D), (16 * FF) ** -0.5, 0.03125, ((0, 32), (1, 4)))
    return dict(sequence_entry_features=sequence_entry_features, sequence_exit_gating=sequence_exit_gating, memory_insert_clusters=memory_insert_clusters, memory_query_clusters=memory_query_clusters, interval_presoftplus=interval_presoftplus, entry_filter_taps=entry_filter_taps, insert_filter_taps=insert_filter_taps, query_filter_taps=query_filter_taps, interval_offset=interval_offset, head_fading_exponent=head_fading_exponent, skip_connection_factor=skip_connection_factor, spike_fading_exponent=spike_fading_exponent, cluster_scaling_vector=cluster_scaling_vector, sequence_exit_projection=sequence_exit_projection, specialist_sample_slice=specialist_sample_slice, specialist_scaling_vector=specialist_scaling_vector, chosen_specialists=chosen_specialists, dispatcher_affinity_matrix=dispatcher_affinity_matrix, gating_projection=gating_projection, expand_projection=expand_projection, shrink_projection=shrink_projection)


norm_eps = 1e-05
clamp_top = 7.0
sigmoid_sharp = 1.702
highest = lax.Precision.HIGHEST

def causal_conv(values, kernel):
    length = values.shape[0]
    joined = jnp.pad(values.astype(jnp.float32), ((kernel.shape[0] - 1, 0), (0, 0)))
    summed = jnp.zeros(values.shape, jnp.float32)
    for offset in range(kernel.shape[0]):
        summed = summed + joined[offset:offset + length] * kernel[offset].astype(jnp.float32)
    return jax.nn.silu(summed)

def sequence_reference_result(sequence_entry_features, sequence_exit_gating, memory_insert_clusters, memory_query_clusters, interval_presoftplus, entry_filter_taps, insert_filter_taps, query_filter_taps, interval_offset, head_fading_exponent, skip_connection_factor, spike_fading_exponent, cluster_scaling_vector, sequence_exit_projection):
    per_group = HEADS // GROUPS
    blocks = SEQUENCE_LENGTH // SPAN
    group_cols = HEADS * HEAD // GROUPS
    seq_x = causal_conv(sequence_entry_features, entry_filter_taps)
    seq_b = causal_conv(memory_insert_clusters, insert_filter_taps)
    seq_c = causal_conv(memory_query_clusters, query_filter_taps)
    discretization_interval = jax.nn.softplus(interval_presoftplus.astype(jnp.float32) + interval_offset)
    fading_exponent = spike_fading_exponent - jnp.exp(head_fading_exponent) * discretization_interval
    scaled = (seq_x.reshape(SEQUENCE_LENGTH, HEADS, HEAD) * discretization_interval[:, :, None]).reshape(blocks, SPAN, GROUPS, per_group, HEAD)
    direct = seq_x.reshape(blocks, SPAN, GROUPS, per_group, HEAD)
    gate_z = sequence_exit_gating.reshape(blocks, SPAN, GROUPS, group_cols)
    keys_b = seq_b.reshape(blocks, SPAN, GROUPS, STATE)
    query_c = seq_c.reshape(blocks, SPAN, GROUPS, STATE)
    decays = fading_exponent.reshape(blocks, SPAN, GROUPS, per_group)
    causal = jnp.tril(jnp.ones((SPAN, SPAN), bool))[:, :, None, None]
    skip_heads = skip_connection_factor.reshape(GROUPS, per_group)[:, :, None]
    gain_groups = cluster_scaling_vector.reshape(GROUPS, group_cols)

    def block_step(running, pieces):
        block_x, block_direct, block_z, block_b, block_c, block_decay = pieces
        cumulative = jnp.cumsum(block_decay, axis=0)
        weight = jnp.exp(jnp.where(causal, cumulative[:, None] - cumulative[None, :], -jnp.inf))
        scores = jnp.einsum('tgn,sgn->tsg', block_c, block_b, precision=highest)
        within = jnp.einsum('tsge,sgep->tgep', scores[..., None] * weight, block_x, precision=highest)
        carried = jnp.einsum('tgn,gepn->tgep', block_c, running, precision=highest) * jnp.exp(cumulative)[..., None]
        block_end = cumulative[-1]
        added = jnp.einsum('sgn,sgep->gepn', block_b, block_x * jnp.exp(block_end[None] - cumulative)[..., None], precision=highest)
        mixer_y = within + carried + block_direct * skip_heads
        gated_y = mixer_y.reshape(SPAN, GROUPS, group_cols) * jax.nn.silu(block_z.astype(jnp.float32))
        normed = gated_y * lax.rsqrt(lax.optimization_barrier(jnp.mean(gated_y * gated_y, axis=2, keepdims=True)) + norm_eps) * gain_groups
        return (running * jnp.exp(block_end)[:, :, None, None] + added, normed.astype(jnp.bfloat16))
    initial = jnp.zeros((GROUPS, per_group, HEAD, STATE), jnp.float32)
    normed_all = lax.scan(block_step, initial, (scaled, direct, gate_z, keys_b, query_c, decays))[1]
    normed_all = normed_all.reshape(SEQUENCE_LENGTH, HEADS * HEAD)
    part_cols = HEADS * HEAD // N_TP
    summed = jnp.zeros((SEQUENCE_LENGTH, D), jnp.float32)
    for member in range(N_TP):
        part_sum = jnp.dot(normed_all[:, member * part_cols:(member + 1) * part_cols], sequence_exit_projection[member * part_cols:(member + 1) * part_cols], preferred_element_type=jnp.float32)
        summed = summed + lax.optimization_barrier(part_sum.astype(jnp.bfloat16)).astype(jnp.float32)
    return summed.astype(jnp.bfloat16)

def specialist_reference_result(specialist_sample_slice, specialist_scaling_vector, chosen_specialists, dispatcher_affinity_matrix, gating_projection, expand_projection, shrink_projection):
    as_float = specialist_sample_slice.astype(jnp.float32)
    centred = as_float - lax.optimization_barrier(jnp.mean(as_float, axis=1, keepdims=True))
    normed = (centred * lax.rsqrt(lax.optimization_barrier(jnp.mean(centred * centred, axis=1, keepdims=True)) + norm_eps) * specialist_scaling_vector).astype(jnp.bfloat16)
    route_weight = jnp.exp(dispatcher_affinity_matrix) / lax.optimization_barrier(jnp.sum(jnp.exp(dispatcher_affinity_matrix), axis=1, keepdims=True))
    blocks_b = TOKENS_B // TOK_B
    slots_each = blocks_b * CAP
    flat_routes = chosen_specialists.reshape(blocks_b, TOK_B * TOPK)
    onehot = (flat_routes[:, :, None] == jnp.arange(EXPERTS, dtype=jnp.int32)[None, None, :]).astype(jnp.int32)
    position = lax.optimization_barrier(jnp.sum(onehot * (jnp.cumsum(onehot, axis=1) - 1), axis=2))
    target = (flat_routes * slots_each + jnp.arange(blocks_b, dtype=jnp.int32)[:, None] * CAP + position).reshape(-1)
    token_ids = jnp.arange(TOKENS_B * TOPK, dtype=jnp.int32) // TOPK
    source_table = jnp.full((EXPERTS * slots_each,), TOKENS_B, jnp.int32).at[target].set(token_ids)
    slot_weight = jnp.zeros((EXPERTS * slots_each,), jnp.float32).at[target].set(route_weight.reshape(-1))
    padded = jnp.concatenate([normed, jnp.zeros((1, D), jnp.bfloat16)], axis=0)
    part_cols = FF // N_TP

    def expert_step(running, pieces):
        gate_one, up_one, down_one, rows_index, rows_weight = pieces
        rows_in = padded[rows_index]
        gate_h = jnp.dot(rows_in, gate_one, preferred_element_type=jnp.float32)
        up_h = jnp.dot(rows_in, up_one, preferred_element_type=jnp.float32)
        clipped = jnp.minimum(gate_h, clamp_top)
        hidden_act = (clipped * jax.nn.sigmoid(sigmoid_sharp * clipped) * (jnp.clip(up_h, -clamp_top, clamp_top) + 1.0)).astype(jnp.bfloat16)
        result = jnp.zeros((slots_each, D), jnp.float32)
        for member in range(N_TP):
            part_sum = jnp.dot(hidden_act[:, member * part_cols:(member + 1) * part_cols], down_one[member * part_cols:(member + 1) * part_cols], preferred_element_type=jnp.float32)
            result = result + lax.optimization_barrier(part_sum.astype(jnp.bfloat16)).astype(jnp.float32)
        result = lax.optimization_barrier(result.astype(jnp.bfloat16)).astype(jnp.float32)
        return (running.at[rows_index].add(rows_weight[:, None] * result), None)
    initial = jnp.zeros((TOKENS_B + 1, D), jnp.float32)
    summed = lax.scan(expert_step, initial, (gating_projection, expand_projection, shrink_projection, source_table.reshape(EXPERTS, slots_each), slot_weight.reshape(EXPERTS, slots_each)))[0]
    return summed[:TOKENS_B].astype(jnp.bfloat16)

def reference(sequence_entry_features, sequence_exit_gating, memory_insert_clusters, memory_query_clusters, interval_presoftplus, entry_filter_taps, insert_filter_taps, query_filter_taps, interval_offset, head_fading_exponent, skip_connection_factor, spike_fading_exponent, cluster_scaling_vector, sequence_exit_projection, specialist_sample_slice, specialist_scaling_vector, chosen_specialists, dispatcher_affinity_matrix, gating_projection, expand_projection, shrink_projection):
    return (sequence_reference_result(sequence_entry_features, sequence_exit_gating, memory_insert_clusters, memory_query_clusters, interval_presoftplus, entry_filter_taps, insert_filter_taps, query_filter_taps, interval_offset, head_fading_exponent, skip_connection_factor, spike_fading_exponent, cluster_scaling_vector, sequence_exit_projection), specialist_reference_result(specialist_sample_slice, specialist_scaling_vector, chosen_specialists, dispatcher_affinity_matrix, gating_projection, expand_projection, shrink_projection))
```

```python
import functools

import jax
import jax.numpy as jnp
from jax import lax
from jax.experimental import pallas as pl
from jax.experimental.pallas import tpu as pltpu
from jax.sharding import Mesh
from jax.sharding import PartitionSpec as P


HEAD = 64
STATE = 128
SPAN = 128
PAIR = 2 * HEAD
CAP = 20
LATE = 8
EARLY = CAP - LATE
ROW_TILE = 256
EP = ("ep_0", "ep_1", "ep_2")
EP_TP = ("ep_0", "ep_1", "ep_2", "tp")

norm_eps = 1e-05
clamp_top = 7.0
sigmoid_sharp = 1.702
LOG2E = 1.4426950408889634
HIGHEST = lax.Precision.HIGHEST
f32 = jnp.float32
bf16 = jnp.bfloat16


def silu(v):
    half = 0.5 * v
    return half + half * jnp.tanh(half)


def mm(a, b):
    return jnp.dot(a, b, preferred_element_type=f32)


def mm_last(a, b):
    return lax.dot_general(a, b, (((1,), (1,)), ((), ())), preferred_element_type=f32)


def lanes_below(shape, limit):
    return lax.broadcasted_iota(jnp.int32, shape, 1) < limit


def params(*sem):
    return pltpu.CompilerParams(dimension_semantics=sem, vmem_limit_bytes=60 * 1024 * 1024)


def cost(flops, nbytes):
    return pl.CostEstimate(flops=int(flops), bytes_accessed=int(nbytes), transcendentals=0)


def expand_heads(row, heads):
    low = lanes_below((1, PAIR), HEAD)
    return [
        jnp.where(low, row[:, 2 * p : 2 * p + 1], row[:, 2 * p + 1 : 2 * p + 2])
        for p in range(heads // 2)
    ]


def states_kernel(
    x_ref, b_ref, c_ref, halo_ref, taps_ref, dtp_ref, spike_ref, off_ref, fade_ref,
    xs_ref, bs_ref, cs_ref, row_ref, state_ref, total_ref, send_ref, buf,
):
    step = pl.program_id(0)
    inner = x_ref.shape[1]
    group = b_ref.shape[1]
    heads = dtp_ref.shape[0]
    groups = group // STATE
    pairs = heads // groups // 2

    @pl.when(step == 0)
    def _():
        buf[0:8, :] = halo_ref[...].astype(f32)
        state_ref[...] = jnp.zeros_like(state_ref)
        total_ref[...] = jnp.zeros_like(total_ref)

    taps = taps_ref[...].astype(f32)
    for ref, out, base in ((x_ref, xs_ref, 0), (b_ref, bs_ref, inner), (c_ref, cs_ref, inner + group)):
        for j in range(0, ref.shape[1], 128):
            at = base + j
            cols = slice(at, at + 128)
            new = ref[:, j : j + 128].astype(f32)
            buf[8 : 8 + SPAN, cols] = new
            acc = new * taps[3:4, cols]
            for k in range(3):
                acc = acc + buf[5 + k : 5 + k + SPAN, cols] * taps[k : k + 1, cols]
            out[:, j : j + 128] = silu(acc).astype(bf16)
    buf[0:8, :] = buf[SPAN : SPAN + 8, :]

    pre = dtp_ref[...].astype(f32) + off_ref[...]
    dt = jnp.maximum(pre, 0.0) + jnp.log1p(jnp.exp(-jnp.abs(pre)))
    log_decay = (spike_ref[...] - jnp.exp(fade_ref[...]) * dt) * LOG2E
    upto = (
        lax.broadcasted_iota(jnp.int32, (SPAN, SPAN), 0)
        <= lax.broadcasted_iota(jnp.int32, (SPAN, SPAN), 1)
    ).astype(f32)
    cum = jnp.dot(log_decay, upto, precision=HIGHEST, preferred_element_type=f32)
    rows = cum - jnp.log2(dt)
    row_ref[0:heads, :] = rows
    row_ref[heads : 2 * heads, :] = cum
    factor = jnp.exp2(cum[:, SPAN - 1 : SPAN] - rows)
    end = jnp.concatenate([cum, jnp.zeros((128 - heads, SPAN), f32)], axis=0).T[SPAN - 1 : SPAN, 0:heads]
    total_ref[...] = total_ref[...] + jnp.concatenate(expand_heads(end, heads), axis=1)
    low = lanes_below((STATE, PAIR), HEAD)
    shrink = expand_heads(jnp.exp2(end), heads)
    for g in range(groups):
        bt = bs_ref[:, g * STATE : (g + 1) * STATE].astype(f32).T
        for p in range(pairs):
            q = g * pairs + p
            cols = slice(q * PAIR, (q + 1) * PAIR)
            left = jnp.concatenate(
                [bt * factor[2 * q : 2 * q + 1, :], bt * factor[2 * q + 1 : 2 * q + 2, :]], axis=0
            ).astype(bf16)
            res = mm(left, xs_ref[:, cols])
            state_ref[:, cols] = state_ref[:, cols] * shrink[q] + jnp.where(low, res[:STATE], res[STATE:])

    @pl.when(step == pl.num_programs(0) - 1)
    def _():
        put_message(send_ref, state_ref[...], total_ref[0:1, :])


def put_message(ref, state, total):
    hi = total.astype(bf16).astype(f32)
    mid = (total - hi).astype(bf16).astype(f32)
    low = total - hi - mid
    ref[0:STATE, :] = state.astype(bf16)
    ref[STATE : STATE + 16, :] = jnp.concatenate(
        [hi, mid, low, jnp.zeros((13, total.shape[1]), f32)], axis=0
    ).astype(bf16)


def prefix_kernel(msg_ref, own_ref, total_ref, own_out, total_out, send_ref):
    tail = msg_ref[STATE : STATE + 16, :].astype(f32)
    came = msg_ref[0:STATE, :].astype(f32)
    decay = tail[0:1] + tail[1:2] + tail[2:3]
    own = own_ref[0] + jnp.exp2(total_ref[0:1, :]) * came
    total = total_ref[0:1, :] + decay
    own_out[0] = own
    own_out[1] = own_ref[1] + jnp.exp2(total_ref[1:2, :]) * came
    total_out[...] = jnp.concatenate([total, total_ref[1:2, :] + decay], axis=0)
    put_message(send_ref, own, total)


def first_kernel(msg_ref, state_ref, total_ref, own_out, total_out, send_ref):
    tail = msg_ref[STATE : STATE + 16, :].astype(f32)
    came = msg_ref[0:STATE, :].astype(f32)
    decay = tail[0:1] + tail[1:2] + tail[2:3]
    own = state_ref[...] + jnp.exp2(total_ref[0:1, :]) * came
    total = total_ref[0:1, :] + decay
    own_out[0] = own
    own_out[1] = came
    total_out[...] = jnp.concatenate([total, decay], axis=0)
    put_message(send_ref, own, total)


def last_kernel(msg_ref, own_ref, total_ref, out_ref):
    out_ref[...] = own_ref[...] + jnp.exp2(total_ref[1:2, :]) * msg_ref[0:STATE, :].astype(f32)


def shifted(value, distance):
    return lax.ppermute(value, EP, [(i, i + distance) for i in range(lax.axis_size(EP) - distance)])


def entering_state(state, total, message):
    inner = state.shape[1]
    own_shape = [
        jax.ShapeDtypeStruct((2, STATE, inner), f32),
        jax.ShapeDtypeStruct((2, inner), f32),
        jax.ShapeDtypeStruct(message.shape, bf16),
    ]
    distance, ep = 1, lax.axis_size(EP)
    own = state
    while distance < ep:
        message = shifted(message, distance)
        last = 2 * distance >= ep
        if last:
            whole = pl.BlockSpec((None, STATE, inner), lambda i: (1, 0, 0))
            return pl.pallas_call(
                last_kernel,
                grid=(1,),
                in_specs=[
                    pl.BlockSpec(message.shape, lambda i: (0, 0)),
                    whole,
                    pl.BlockSpec((2, inner), lambda i: (0, 0)),
                ],
                out_specs=pl.BlockSpec((STATE, inner), lambda i: (0, 0)),
                out_shape=jax.ShapeDtypeStruct((STATE, inner), f32),
                compiler_params=params("arbitrary"),
                cost_estimate=cost(1e9, 2e6),
                name="last",
            )(message, own, total)
        own, total, message = pl.pallas_call(
            first_kernel if distance == 1 else prefix_kernel,
            out_shape=own_shape,
            compiler_params=params(),
            cost_estimate=cost(1e9, 3e6),
            name="prefix",
        )(message, own, total)
        distance *= 2


def mixer_kernel(
    xs_ref, bs_ref, cs_ref, z_ref, row_ref, enter_ref, skip_ref, gain_ref, w_ref,
    out_ref, state, gated, normed,
):
    step = pl.program_id(0)
    inner = xs_ref.shape[1]
    group = bs_ref.shape[1]
    heads = row_ref.shape[0] // 2
    groups = group // STATE
    pairs = heads // groups // 2
    wide = inner // groups

    @pl.when(step == 0)
    def _():
        state[...] = enter_ref[...]

    mask = lax.broadcasted_iota(jnp.int32, (SPAN, SPAN), 0) >= lax.broadcasted_iota(
        jnp.int32, (SPAN, SPAN), 1
    )
    low = lanes_below((STATE, PAIR), HEAD)
    rows = row_ref[0:heads, :]
    cum = jnp.concatenate(
        [row_ref[heads : 2 * heads, :], jnp.zeros((128 - heads, SPAN), f32)], axis=0
    ).T
    factor = jnp.exp2(row_ref[heads : 2 * heads, SPAN - 1 : SPAN] - rows)
    shrink = expand_heads(jnp.exp2(cum[SPAN - 1 : SPAN, 0:heads]), heads)
    for g in range(groups):
        gcols = slice(g * STATE, (g + 1) * STATE)
        bt = bs_ref[:, gcols].astype(f32).T
        cmat = cs_ref[:, gcols]
        c32 = cmat.astype(f32)
        scores = mm_last(cmat, bs_ref[:, gcols])
        squares = jnp.zeros((SPAN, PAIR), f32)
        for p in range(pairs):
            q = g * pairs + p
            cols = slice(q * PAIR, (q + 1) * PAIR)
            lefts, downs = [], []
            for h in (2 * q, 2 * q + 1):
                col = jnp.broadcast_to(cum[:, h : h + 1], (SPAN, SPAN))
                decay = jnp.exp2(jnp.where(mask, col - rows[h : h + 1, :], -1e30))
                lefts.append(
                    jnp.concatenate([(scores * decay).astype(bf16), (c32 * jnp.exp2(col)).astype(bf16)], axis=1)
                )
                downs.append((bt * factor[h : h + 1, :]).astype(bf16))
            xp = xs_ref[:, cols]
            sp = state[:, cols]
            res = mm(jnp.concatenate(lefts, axis=0), jnp.concatenate([xp, sp.astype(bf16)], axis=0))
            add = mm(jnp.concatenate(downs, axis=0), xp)
            state[:, cols] = sp * shrink[q] + jnp.where(low, add[:STATE], add[STATE:])
            y = jnp.where(low, res[:SPAN], res[SPAN:]) + xp.astype(f32) * skip_ref[:, cols]
            y = y * silu(z_ref[:, cols].astype(f32))
            gated[:, cols] = y
            squares = squares + y * y
        scale = lax.rsqrt(jnp.sum(squares, axis=1, keepdims=True) * (1.0 / wide) + norm_eps)
        wcols = slice(g * wide, (g + 1) * wide)
        normed[:, wcols] = (gated[:, wcols] * scale * gain_ref[:, wcols]).astype(bf16)
    out_ref[...] = mm(normed[...], w_ref[...]).astype(bf16)


def mixer_half(
    features, gating, insert, query, presoftplus, entry_taps, insert_taps, query_taps,
    offset, fading, skip, spike, gain, projection,
):
    rows, inner = features.shape
    group = insert.shape[1]
    heads = offset.shape[0]
    width = projection.shape[1]
    every = inner + 2 * group
    last = jnp.concatenate([a[rows - 8 :] for a in (features, insert, query)], axis=1)
    halo = shifted(last, 1)
    taps = jnp.concatenate([entry_taps, insert_taps, query_taps], axis=1)
    steps = rows // SPAN

    def block(n):
        return pl.BlockSpec((SPAN, n), lambda i: (i, 0))

    def whole(*shape):
        return pl.BlockSpec(shape, lambda i: (0,) * len(shape))

    def across(n):
        return pl.BlockSpec((n, SPAN), lambda i: (0, i))

    xs, bs, cs, row, state, total, message = pl.pallas_call(
        states_kernel,
        grid=(steps,),
        in_specs=[
            block(inner), block(group), block(group), whole(8, every), whole(4, every),
            across(heads), across(heads), whole(heads, 1), whole(heads, 1),
        ],
        out_specs=[
            block(inner), block(group), block(group), across(2 * heads),
            whole(STATE, inner), whole(1, inner), whole(STATE + 16, inner),
        ],
        out_shape=[
            jax.ShapeDtypeStruct((rows, inner), bf16),
            jax.ShapeDtypeStruct((rows, group), bf16),
            jax.ShapeDtypeStruct((rows, group), bf16),
            jax.ShapeDtypeStruct((2 * heads, rows), f32),
            jax.ShapeDtypeStruct((STATE, inner), f32),
            jax.ShapeDtypeStruct((1, inner), f32),
            jax.ShapeDtypeStruct((STATE + 16, inner), bf16),
        ],
        scratch_shapes=[pltpu.VMEM((SPAN + 8, every), f32)],
        compiler_params=params("arbitrary"),
        cost_estimate=cost(8e9, 1e7),
        name="states",
    )(
        features, insert, query, halo, taps, presoftplus.T, spike.T,
        offset.reshape(heads, 1), fading.reshape(heads, 1),
    )
    entering = entering_state(state, total, message)
    partial = pl.pallas_call(
        mixer_kernel,
        grid=(steps,),
        in_specs=[
            block(inner), block(group), block(group), block(inner), across(2 * heads),
            whole(STATE, inner), whole(1, inner), whole(1, inner), whole(inner, width),
        ],
        out_specs=block(width),
        out_shape=jax.ShapeDtypeStruct((rows, width), bf16),
        scratch_shapes=[
            pltpu.VMEM((STATE, inner), f32),
            pltpu.VMEM((SPAN, inner), f32),
            pltpu.VMEM((SPAN, inner), bf16),
        ],
        compiler_params=params("arbitrary"),
        cost_estimate=cost(2e10, 2e7),
        name="mixer",
    )(
        xs, bs, cs, gating, row, entering,
        jnp.repeat(skip, HEAD).reshape(1, inner), gain.reshape(1, inner), projection,
    )
    return lax.psum_scatter(partial, "tp", scatter_dimension=0, tiled=True)


FIRST = 16
SECOND = 40
OTHERS = 36


def second_slot(inside):
    other = inside < OTHERS
    return (
        jnp.where(other, inside // EARLY + 1, 0),
        jnp.where(other, inside % EARLY + LATE, inside - OTHERS + FIRST),
    )


def expert_of(rows, first, per, experts):
    at = lax.broadcasted_iota(jnp.int32, (rows, experts), 0) + first
    return (at // per == lax.broadcasted_iota(jnp.int32, (rows, experts), 1)).astype(bf16)


def route_kernel(x_ref, gain_ref, pick_ref, score_ref, token_ref, first_ref):
    tokens, width = x_ref.shape
    experts = first_ref.shape[0] // FIRST
    x = x_ref[...].astype(f32)
    x = x - jnp.mean(x, axis=1, keepdims=True)
    x = x * lax.rsqrt(jnp.mean(x * x, axis=1, keepdims=True) + norm_eps) * gain_ref[...]
    normed = x.astype(bf16)
    token_ref[:, 0:width] = normed
    weight = jnp.exp(score_ref[...])
    weight = weight / jnp.sum(weight, axis=0, keepdims=True)
    lane = lax.broadcasted_iota(jnp.int32, (experts, tokens), 0)
    taken = jnp.zeros((experts, tokens), f32)
    dense = jnp.zeros((experts, tokens), f32)
    for k in range(pick_ref.shape[0]):
        hit = pick_ref[k : k + 1, :] == lane
        taken = jnp.where(hit, 1.0, taken)
        dense = jnp.where(hit, weight[k : k + 1, :], dense)
    earlier = (
        lax.broadcasted_iota(jnp.int32, (tokens, tokens), 0)
        < lax.broadcasted_iota(jnp.int32, (tokens, tokens), 1)
    ).astype(bf16)
    slot = jnp.where(taken > 0, mm(taken.astype(bf16), earlier), -1.0)
    token_ref[:, width : width + 128] = jnp.concatenate(
        [slot, dense, jnp.zeros((128 - 2 * experts, tokens), f32)], axis=0
    ).T.astype(bf16)
    rows = experts * FIRST
    spread = mm(expert_of(rows, 0, FIRST, experts), slot.astype(bf16))
    wanted = lax.broadcasted_iota(jnp.int32, (rows, 1), 0) % FIRST
    first_ref[...] = mm((spread == wanted.astype(f32)).astype(bf16), normed).astype(bf16)


def second_kernel(table_ref, apart_ref, out_ref, *, experts):
    width = table_ref.shape[1] - 128
    rows = out_ref.shape[0]
    first = pl.program_id(0) * rows
    spread = mm_last(expert_of(rows, first, SECOND, experts), table_ref[:, width : width + experts])
    at = lax.broadcasted_iota(jnp.int32, (rows, 1), 0) + first
    block, wanted = second_slot(at % SECOND)
    hit = (spread == wanted.astype(f32)) & (apart_ref[...] == block)
    out_ref[...] = mm(hit.astype(bf16), table_ref[:, 0:width]).astype(bf16)


def expert_kernel(x_ref, gate_ref, up_ref, down_ref, out_ref):
    x = x_ref[...]
    g = jnp.minimum(mm(x, gate_ref[...]), clamp_top)
    u = jnp.clip(mm(x, up_ref[...]), -clamp_top, clamp_top) + 1.0
    act = g * (0.5 + 0.5 * jnp.tanh((0.5 * sigmoid_sharp) * g)) * u
    out_ref[...] = mm(act.astype(bf16), down_ref[...]).astype(bf16)


def expert(rows_in, gate, up, down):
    rows, width = rows_in.shape
    hidden = gate.shape[2]
    return pl.pallas_call(
        expert_kernel,
        grid=(rows // ROW_TILE,),
        in_specs=[
            pl.BlockSpec((ROW_TILE, width), lambda i: (i, 0)),
            pl.BlockSpec((None, width, hidden), lambda i: (0, 0, 0)),
            pl.BlockSpec((None, width, hidden), lambda i: (0, 0, 0)),
            pl.BlockSpec((None, hidden, width), lambda i: (0, 0, 0)),
        ],
        out_specs=pl.BlockSpec((ROW_TILE, width), lambda i: (i, 0)),
        out_shape=jax.ShapeDtypeStruct((rows, width), bf16),
        compiler_params=params("arbitrary"),
        cost_estimate=cost(6 * rows * width * hidden, 3 * 2 * width * hidden + 4 * rows * width),
        name="expert",
    )(rows_in, gate, up, down)


def gather_kernel(table_ref, apart_ref, back_ref, out_ref, pick, *, experts):
    rows = back_ref.shape[0]

    @pl.when(pl.program_id(0) == 0)
    def _():
        chosen = expert_of(rows, 0, SECOND, experts)
        table = table_ref[...]
        slot = mm_last(table[:, 0:experts], chosen)
        weight = mm_last(table[:, experts : 2 * experts], chosen)
        block, wanted = second_slot(lax.broadcasted_iota(jnp.int32, (1, rows), 1) % SECOND)
        hit = (slot == wanted.astype(f32)) & (apart_ref[...] == block)
        pick[...] = jnp.where(hit, weight, 0.0).astype(bf16)

    out_ref[...] = mm(pick[...], back_ref[...]).astype(bf16)


def final_kernel(table_ref, back_ref, sum_ref, out_ref, *, experts):
    rows = back_ref.shape[0]
    table = table_ref[...]
    chosen = expert_of(rows, 0, FIRST, experts)
    slot = mm_last(table[:, 0:experts], chosen)
    weight = mm_last(table[:, experts : 2 * experts], chosen)
    at = lax.broadcasted_iota(jnp.int32, (1, rows), 1) % FIRST
    own = mm(jnp.where(slot == at.astype(f32), weight, 0.0).astype(bf16), back_ref[...])
    out_ref[...] = (own + sum_ref[...].astype(f32)).astype(bf16)


def exchanged(value):
    return lax.all_to_all(value, EP, split_axis=0, concat_axis=0, tiled=True)


def experts_half(sample, gain, pick, score, gate, up, down):
    tokens, width = sample.shape
    experts = lax.axis_size(EP)
    blocks = lax.axis_size("tp")
    every = width + 128
    own, first_out = pl.pallas_call(
        route_kernel,
        out_shape=[
            jax.ShapeDtypeStruct((tokens, every), bf16),
            jax.ShapeDtypeStruct((experts * FIRST, width), bf16),
        ],
        compiler_params=params(),
        cost_estimate=cost(1e9, 3e6),
        name="route",
    )(sample, gain.reshape(1, width), pick.T, score.T)
    apart = (jnp.arange(blocks * tokens, dtype=jnp.int32) // tokens - lax.axis_index("tp")) % blocks
    table = lax.all_gather(own, "tp", axis=0, tiled=True)
    first_in = exchanged(first_out.reshape(experts, FIRST, width))
    late_rows = lax.all_gather(first_in[:, :LATE], "tp", axis=0, tiled=True).reshape(-1, width)

    count = experts * SECOND
    tile = count // 4
    second_out = pl.pallas_call(
        functools.partial(second_kernel, experts=experts),
        grid=(count // tile,),
        in_specs=[
            pl.BlockSpec((blocks * tokens, every), lambda i: (0, 0)),
            pl.BlockSpec((1, blocks * tokens), lambda i: (0, 0)),
        ],
        out_specs=pl.BlockSpec((tile, width), lambda i: (i, 0)),
        out_shape=jax.ShapeDtypeStruct((count, width), bf16),
        compiler_params=params("arbitrary"),
        cost_estimate=cost(3.2e9, 1e7),
        name="second",
    )(table, apart.reshape(1, -1))
    second_in = exchanged(second_out.reshape(experts, SECOND, width))

    late_part = expert(late_rows, gate, up, down)
    own_part = expert(first_in[:, LATE:].reshape(-1, width), gate, up, down)
    late_sum = lax.psum_scatter(
        late_part.reshape(blocks * experts, LATE, width), "tp", scatter_dimension=0, tiled=True
    )
    second_part = expert(second_in.reshape(count, width), gate, up, down)
    second_back = exchanged(second_part.reshape(experts, SECOND, width))
    first_back = exchanged(
        jnp.concatenate([late_sum, own_part.reshape(experts, FIRST - LATE, width)], axis=1)
    )
    col_tile = 512
    second_mix = pl.pallas_call(
        functools.partial(gather_kernel, experts=experts),
        grid=(width // col_tile,),
        in_specs=[
            pl.BlockSpec((blocks * tokens, 128), lambda i: (0, width // 128)),
            pl.BlockSpec((blocks * tokens, 1), lambda i: (0, 0)),
            pl.BlockSpec((count, col_tile), lambda i: (0, i)),
        ],
        out_specs=pl.BlockSpec((blocks * tokens, col_tile), lambda i: (0, i)),
        out_shape=jax.ShapeDtypeStruct((blocks * tokens, width), bf16),
        scratch_shapes=[pltpu.VMEM((blocks * tokens, count), bf16)],
        compiler_params=params("arbitrary"),
        cost_estimate=cost(3.2e9, 1e7),
        name="gather",
    )(table, apart.reshape(-1, 1), second_back.reshape(count, width))
    second_sum = lax.psum_scatter(second_mix, "tp", scatter_dimension=0, tiled=True)
    return pl.pallas_call(
        functools.partial(final_kernel, experts=experts),
        grid=(1,),
        in_specs=[
            pl.BlockSpec((tokens, 128), lambda i: (0, width // 128)),
            pl.BlockSpec((experts * FIRST, width), lambda i: (0, 0)),
            pl.BlockSpec((tokens, width), lambda i: (0, 0)),
        ],
        out_specs=pl.BlockSpec((tokens, width), lambda i: (0, 0)),
        out_shape=jax.ShapeDtypeStruct((tokens, width), bf16),
        compiler_params=params("arbitrary"),
        cost_estimate=cost(2e8, 2e6),
        name="final",
    )(own, first_back.reshape(experts * FIRST, width), second_sum)


def body(*args):
    moe_out = experts_half(*args[14:])
    mixed = mixer_half(*args[:14])
    return (mixed, moe_out)


def solution(mesh):
    split = Mesh(mesh.devices.reshape(4, 4, 2, mesh.shape["tp"]), ("ep_0", "ep_1", "ep_2", "tp"))
    return jax.shard_map(
        body,
        mesh=split,
        in_specs=(
            P(EP, "tp"),
            P(EP, "tp"),
            P(EP, "tp"),
            P(EP, "tp"),
            P(EP, "tp"),
            P(None, "tp"),
            P(None, "tp"),
            P(None, "tp"),
            P("tp"),
            P("tp"),
            P("tp"),
            P(EP, "tp"),
            P("tp"),
            P("tp", None),
            P(EP_TP, None),
            P(),
            P(EP_TP, None),
            P(EP_TP, None),
            P(EP, None, "tp"),
            P(EP, None, "tp"),
            P(EP, "tp", None),
        ),
        out_specs=(P(EP_TP, None), P(EP_TP, None)),
        check_vma=False,
    )
```

```python
import functools

import jax
import jax.numpy as jnp
from jax import lax
from jax.experimental import pallas as pl
from jax.experimental.pallas import tpu as pltpu
from jax.sharding import Mesh
from jax.sharding import PartitionSpec as P


HEAD = 64
STATE = 128
SPAN = 128
PAIR = 2 * HEAD
CAP = 20
LATE = 8
EARLY = CAP - LATE
ROW_TILE = 256
EP = ("ep_0", "ep_1", "ep_2")
EP_TP = ("ep_0", "ep_1", "ep_2", "tp")

norm_eps = 1e-05
clamp_top = 7.0
sigmoid_sharp = 1.702
LOG2E = 1.4426950408889634
HIGHEST = lax.Precision.HIGHEST
f32 = jnp.float32
bf16 = jnp.bfloat16


def silu(v):
    half = 0.5 * v
    return half + half * jnp.tanh(half)


def mm(a, b):
    return jnp.dot(a, b, preferred_element_type=f32)


def mm_last(a, b):
    return lax.dot_general(a, b, (((1,), (1,)), ((), ())), preferred_element_type=f32)


def lanes_below(shape, limit):
    return lax.broadcasted_iota(jnp.int32, shape, 1) < limit


def params(*sem):
    return pltpu.CompilerParams(dimension_semantics=sem, vmem_limit_bytes=60 * 1024 * 1024)


def cost(flops, nbytes):
    return pl.CostEstimate(flops=int(flops), bytes_accessed=int(nbytes), transcendentals=0)


def expand_heads(row, heads):
    low = lanes_below((1, PAIR), HEAD)
    return [
        jnp.where(low, row[:, 2 * p : 2 * p + 1], row[:, 2 * p + 1 : 2 * p + 2])
        for p in range(heads // 2)
    ]


def states_kernel(
    x_ref, b_ref, c_ref, halo_ref, taps_ref, dtp_ref, spike_ref, off_ref, fade_ref,
    xs_ref, bs_ref, cs_ref, row_ref, send_ref, buf, state, total,
):
    step = pl.program_id(0)
    inner = x_ref.shape[1]
    group = b_ref.shape[1]
    heads = dtp_ref.shape[0]
    groups = group // STATE
    pairs = heads // groups // 2

    @pl.when(step == 0)
    def _():
        buf[0:8, :] = halo_ref[...].astype(f32)
        state[...] = jnp.zeros_like(state)
        total[...] = jnp.zeros_like(total)

    taps = taps_ref[...].astype(f32)
    for ref, out, base in ((x_ref, xs_ref, 0), (b_ref, bs_ref, inner), (c_ref, cs_ref, inner + group)):
        for j in range(0, ref.shape[1], 128):
            at = base + j
            cols = slice(at, at + 128)
            new = ref[:, j : j + 128].astype(f32)
            buf[8 : 8 + SPAN, cols] = new
            acc = new * taps[3:4, cols]
            for k in range(3):
                acc = acc + buf[5 + k : 5 + k + SPAN, cols] * taps[k : k + 1, cols]
            out[:, j : j + 128] = silu(acc).astype(bf16)
    buf[0:8, :] = buf[SPAN : SPAN + 8, :]

    pre = dtp_ref[...].astype(f32) + off_ref[...]
    dt = jnp.maximum(pre, 0.0) + jnp.log1p(jnp.exp(-jnp.abs(pre)))
    log_decay = (spike_ref[...] - jnp.exp(fade_ref[...]) * dt) * LOG2E
    upto = (
        lax.broadcasted_iota(jnp.int32, (SPAN, SPAN), 0)
        <= lax.broadcasted_iota(jnp.int32, (SPAN, SPAN), 1)
    ).astype(f32)
    cum = jnp.dot(log_decay, upto, precision=HIGHEST, preferred_element_type=f32)
    rows = cum - jnp.log2(dt)
    row_ref[0:heads, :] = rows
    row_ref[heads : 2 * heads, :] = cum
    factor = jnp.exp2(cum[:, SPAN - 1 : SPAN] - rows)
    end = jnp.concatenate([cum, jnp.zeros((128 - heads, SPAN), f32)], axis=0).T[SPAN - 1 : SPAN, 0:heads]
    total[...] = total[...] + jnp.concatenate(expand_heads(end, heads), axis=1)
    low = lanes_below((STATE, PAIR), HEAD)
    shrink = expand_heads(jnp.exp2(end), heads)
    for g in range(groups):
        bt = bs_ref[:, g * STATE : (g + 1) * STATE].astype(f32).T
        for p in range(pairs):
            q = g * pairs + p
            cols = slice(q * PAIR, (q + 1) * PAIR)
            left = jnp.concatenate(
                [bt * factor[2 * q : 2 * q + 1, :], bt * factor[2 * q + 1 : 2 * q + 2, :]], axis=0
            ).astype(bf16)
            res = mm(left, xs_ref[:, cols])
            state[:, cols] = state[:, cols] * shrink[q] + jnp.where(low, res[:STATE], res[STATE:])

    @pl.when(step == pl.num_programs(0) - 1)
    def _():
        half_cols = inner // 2
        t = total[0:1, :]
        hi = t.astype(bf16).astype(f32)
        mid = (t - hi).astype(bf16).astype(f32)
        tail = jnp.concatenate([hi, mid, t - hi - mid, jnp.zeros((5, inner), f32)], axis=0)
        for e in range(send_ref.shape[0]):
            rows_of, cols = slice(8 * (e // 2), 8 * (e // 2) + 8), slice(e % 2 * half_cols, (e % 2 + 1) * half_cols)
            send_ref[e] = jnp.concatenate([state[rows_of, cols], tail[:, cols]], axis=0).astype(bf16)


def place_of(device):
    return {"ep_0": device // 8, "ep_1": device // 2 % 4, "ep_2": device % 2}


def entering_kernel(msg_ref, out_ref, came, before, back, send_sem, recv_sem, send_sem2, recv_sem2):
    ep = msg_ref.shape[0]
    half_cols = msg_ref.shape[2]
    me = (lax.axis_index("ep_0") * 4 + lax.axis_index("ep_1")) * 2 + lax.axis_index("ep_2")
    barrier = pltpu.get_barrier_semaphore()

    @pl.loop(1, ep)
    def _(k):
        pl.semaphore_signal(
            barrier, inc=1, device_id=place_of((me + k) % ep), device_id_type=pl.DeviceIdType.MESH
        )

    pl.semaphore_wait(barrier, ep - 1)

    def there(k):
        to = (me + k) % ep
        return pltpu.make_async_remote_copy(
            src_ref=msg_ref.at[to], dst_ref=came.at[me], send_sem=send_sem.at[k], recv_sem=recv_sem.at[k],
            device_id=place_of(to), device_id_type=pl.DeviceIdType.MESH,
        )

    def returned(k):
        to = (me + k) % ep
        return pltpu.make_async_remote_copy(
            src_ref=before.at[to], dst_ref=back.at[me], send_sem=send_sem2.at[k], recv_sem=recv_sem2.at[k],
            device_id=place_of(to), device_id_type=pl.DeviceIdType.MESH,
        )

    @pl.loop(1, ep)
    def _(k):
        there(k).start()

    came[me] = msg_ref[me]

    @pl.loop(1, ep)
    def _(k):
        there(k).wait()

    running = jnp.zeros((8, half_cols), f32)
    for i in range(ep):
        before[i] = running
        block = came[i].astype(f32)
        running = running * jnp.exp2(block[8:9] + block[9:10] + block[10:11]) + block[0:8]

    @pl.loop(1, ep)
    def _(k):
        returned(k).start()

    back[me] = before[me]

    @pl.loop(1, ep)
    def _(k):
        returned(k).wait()

    for e in range(ep):
        out_ref[8 * (e // 2) : 8 * (e // 2) + 8, e % 2 * half_cols : (e % 2 + 1) * half_cols] = back[e]


def shifted(value, distance):
    return lax.ppermute(value, EP, [(i, i + distance) for i in range(lax.axis_size(EP) - distance)])


def entering_state(message):
    ep, _, half_cols = message.shape
    sems = pltpu.SemaphoreType.DMA((ep,))
    return pl.pallas_call(
        entering_kernel,
        in_specs=[pl.BlockSpec(memory_space=pltpu.VMEM)],
        out_specs=pl.BlockSpec(memory_space=pltpu.VMEM),
        out_shape=jax.ShapeDtypeStruct((STATE, 2 * half_cols), f32),
        scratch_shapes=[
            pltpu.VMEM((ep, 16, half_cols), bf16),
            pltpu.VMEM((ep, 8, half_cols), f32),
            pltpu.VMEM((ep, 8, half_cols), f32),
            sems, sems, sems, sems,
        ],
        compiler_params=pltpu.CompilerParams(collective_id=0, has_side_effects=True),
        cost_estimate=cost(1e10, 3e6),
        name="entering",
    )(message)


def mixer_kernel(
    xs_ref, bs_ref, cs_ref, z_ref, row_ref, enter_ref, skip_ref, gain_ref, w_ref,
    out_ref, state, gated, normed,
):
    step = pl.program_id(0)
    inner = xs_ref.shape[1]
    group = bs_ref.shape[1]
    heads = row_ref.shape[0] // 2
    groups = group // STATE
    pairs = heads // groups // 2
    wide = inner // groups

    @pl.when(step == 0)
    def _():
        state[...] = enter_ref[...]

    mask = lax.broadcasted_iota(jnp.int32, (SPAN, SPAN), 0) >= lax.broadcasted_iota(
        jnp.int32, (SPAN, SPAN), 1
    )
    low = lanes_below((STATE, PAIR), HEAD)
    rows = row_ref[0:heads, :]
    cum = jnp.concatenate(
        [row_ref[heads : 2 * heads, :], jnp.zeros((128 - heads, SPAN), f32)], axis=0
    ).T
    factor = jnp.exp2(row_ref[heads : 2 * heads, SPAN - 1 : SPAN] - rows)
    shrink = expand_heads(jnp.exp2(cum[SPAN - 1 : SPAN, 0:heads]), heads)
    for g in range(groups):
        gcols = slice(g * STATE, (g + 1) * STATE)
        bt = bs_ref[:, gcols].astype(f32).T
        cmat = cs_ref[:, gcols]
        c32 = cmat.astype(f32)
        scores = mm_last(cmat, bs_ref[:, gcols])
        squares = jnp.zeros((SPAN, PAIR), f32)
        for p in range(pairs):
            q = g * pairs + p
            cols = slice(q * PAIR, (q + 1) * PAIR)
            lefts, downs = [], []
            for h in (2 * q, 2 * q + 1):
                col = jnp.broadcast_to(cum[:, h : h + 1], (SPAN, SPAN))
                decay = jnp.exp2(jnp.where(mask, col - rows[h : h + 1, :], -1e30))
                lefts.append(
                    jnp.concatenate([(scores * decay).astype(bf16), (c32 * jnp.exp2(col)).astype(bf16)], axis=1)
                )
                downs.append((bt * factor[h : h + 1, :]).astype(bf16))
            xp = xs_ref[:, cols]
            sp = state[:, cols]
            res = mm(jnp.concatenate(lefts, axis=0), jnp.concatenate([xp, sp.astype(bf16)], axis=0))
            add = mm(jnp.concatenate(downs, axis=0), xp)
            state[:, cols] = sp * shrink[q] + jnp.where(low, add[:STATE], add[STATE:])
            y = jnp.where(low, res[:SPAN], res[SPAN:]) + xp.astype(f32) * skip_ref[:, cols]
            y = y * silu(z_ref[:, cols].astype(f32))
            gated[:, cols] = y
            squares = squares + y * y
        scale = lax.rsqrt(jnp.sum(squares, axis=1, keepdims=True) * (1.0 / wide) + norm_eps)
        wcols = slice(g * wide, (g + 1) * wide)
        normed[:, wcols] = (gated[:, wcols] * scale * gain_ref[:, wcols]).astype(bf16)
    out_ref[...] = mm(normed[...], w_ref[...]).astype(bf16)


def mixer_half(
    features, gating, insert, query, presoftplus, entry_taps, insert_taps, query_taps,
    offset, fading, skip, spike, gain, projection,
):
    rows, inner = features.shape
    group = insert.shape[1]
    heads = offset.shape[0]
    width = projection.shape[1]
    every = inner + 2 * group
    ep = lax.axis_size(EP)
    last = jnp.concatenate([a[rows - 8 :] for a in (features, insert, query)], axis=1)
    halo = shifted(last, 1)
    taps = jnp.concatenate([entry_taps, insert_taps, query_taps], axis=1)
    steps = rows // SPAN

    def block(n):
        return pl.BlockSpec((SPAN, n), lambda i: (i, 0))

    def whole(*shape):
        return pl.BlockSpec(shape, lambda i: (0,) * len(shape))

    def across(n):
        return pl.BlockSpec((n, SPAN), lambda i: (0, i))

    xs, bs, cs, row, message = pl.pallas_call(
        states_kernel,
        grid=(steps,),
        in_specs=[
            block(inner), block(group), block(group), whole(8, every), whole(4, every),
            across(heads), across(heads), whole(heads, 1), whole(heads, 1),
        ],
        out_specs=[
            block(inner), block(group), block(group), across(2 * heads),
            whole(ep, 16, inner // 2),
        ],
        out_shape=[
            jax.ShapeDtypeStruct((rows, inner), bf16),
            jax.ShapeDtypeStruct((rows, group), bf16),
            jax.ShapeDtypeStruct((rows, group), bf16),
            jax.ShapeDtypeStruct((2 * heads, rows), f32),
            jax.ShapeDtypeStruct((ep, 16, inner // 2), bf16),
        ],
        scratch_shapes=[
            pltpu.VMEM((SPAN + 8, every), f32),
            pltpu.VMEM((STATE, inner), f32),
            pltpu.VMEM((1, inner), f32),
        ],
        compiler_params=params("arbitrary"),
        cost_estimate=cost(8e9, 1e7),
        name="states",
    )(
        features, insert, query, halo, taps, presoftplus.T, spike.T,
        offset.reshape(heads, 1), fading.reshape(heads, 1),
    )
    entering = entering_state(message)
    partial = pl.pallas_call(
        mixer_kernel,
        grid=(steps,),
        in_specs=[
            block(inner), block(group), block(group), block(inner), across(2 * heads),
            whole(STATE, inner), whole(1, inner), whole(1, inner), whole(inner, width),
        ],
        out_specs=block(width),
        out_shape=jax.ShapeDtypeStruct((rows, width), bf16),
        scratch_shapes=[
            pltpu.VMEM((STATE, inner), f32),
            pltpu.VMEM((SPAN, inner), f32),
            pltpu.VMEM((SPAN, inner), bf16),
        ],
        compiler_params=params("arbitrary"),
        cost_estimate=cost(2e10, 2e7),
        name="mixer",
    )(
        xs, bs, cs, gating, row, entering,
        jnp.repeat(skip, HEAD).reshape(1, inner), gain.reshape(1, inner), projection,
    )
    return lax.psum_scatter(partial, "tp", scatter_dimension=0, tiled=True)


FIRST = 16
SECOND = 40
OTHERS = 36


def second_slot(inside):
    other = inside < OTHERS
    return (
        jnp.where(other, inside // EARLY + 1, 0),
        jnp.where(other, inside % EARLY + LATE, inside - OTHERS + FIRST),
    )


def expert_of(rows, first, per, experts):
    at = lax.broadcasted_iota(jnp.int32, (rows, experts), 0) + first
    return (at // per == lax.broadcasted_iota(jnp.int32, (rows, experts), 1)).astype(bf16)


def route_kernel(x_ref, gain_ref, pick_ref, score_ref, token_ref, first_ref):
    tokens, width = x_ref.shape
    experts = first_ref.shape[0] // FIRST
    x = x_ref[...].astype(f32)
    x = x - jnp.mean(x, axis=1, keepdims=True)
    x = x * lax.rsqrt(jnp.mean(x * x, axis=1, keepdims=True) + norm_eps) * gain_ref[...]
    normed = x.astype(bf16)
    token_ref[:, 0:width] = normed
    weight = jnp.exp(score_ref[...])
    weight = weight / jnp.sum(weight, axis=0, keepdims=True)
    lane = lax.broadcasted_iota(jnp.int32, (experts, tokens), 0)
    taken = jnp.zeros((experts, tokens), f32)
    dense = jnp.zeros((experts, tokens), f32)
    for k in range(pick_ref.shape[0]):
        hit = pick_ref[k : k + 1, :] == lane
        taken = jnp.where(hit, 1.0, taken)
        dense = jnp.where(hit, weight[k : k + 1, :], dense)
    earlier = (
        lax.broadcasted_iota(jnp.int32, (tokens, tokens), 0)
        < lax.broadcasted_iota(jnp.int32, (tokens, tokens), 1)
    ).astype(bf16)
    slot = jnp.where(taken > 0, mm(taken.astype(bf16), earlier), -1.0)
    token_ref[:, width : width + 128] = jnp.concatenate(
        [slot, dense, jnp.zeros((128 - 2 * experts, tokens), f32)], axis=0
    ).T.astype(bf16)
    rows = experts * FIRST
    spread = mm(expert_of(rows, 0, FIRST, experts), slot.astype(bf16))
    wanted = lax.broadcasted_iota(jnp.int32, (rows, 1), 0) % FIRST
    first_ref[...] = mm((spread == wanted.astype(f32)).astype(bf16), normed).astype(bf16)


def second_kernel(table_ref, apart_ref, out_ref, *, experts):
    width = table_ref.shape[1] - 128
    rows = out_ref.shape[0]
    first = pl.program_id(0) * rows
    spread = mm_last(expert_of(rows, first, SECOND, experts), table_ref[:, width : width + experts])
    at = lax.broadcasted_iota(jnp.int32, (rows, 1), 0) + first
    block, wanted = second_slot(at % SECOND)
    hit = (spread == wanted.astype(f32)) & (apart_ref[...] == block)
    out_ref[...] = mm(hit.astype(bf16), table_ref[:, 0:width]).astype(bf16)


def expert_kernel(x_ref, gate_ref, up_ref, down_ref, out_ref):
    x = x_ref[...]
    g = jnp.minimum(mm(x, gate_ref[...]), clamp_top)
    u = jnp.clip(mm(x, up_ref[...]), -clamp_top, clamp_top) + 1.0
    act = g * (0.5 + 0.5 * jnp.tanh((0.5 * sigmoid_sharp) * g)) * u
    out_ref[...] = mm(act.astype(bf16), down_ref[...]).astype(bf16)


def expert(rows_in, gate, up, down):
    rows, width = rows_in.shape
    hidden = gate.shape[2]
    return pl.pallas_call(
        expert_kernel,
        grid=(rows // ROW_TILE,),
        in_specs=[
            pl.BlockSpec((ROW_TILE, width), lambda i: (i, 0)),
            pl.BlockSpec((None, width, hidden), lambda i: (0, 0, 0)),
            pl.BlockSpec((None, width, hidden), lambda i: (0, 0, 0)),
            pl.BlockSpec((None, hidden, width), lambda i: (0, 0, 0)),
        ],
        out_specs=pl.BlockSpec((ROW_TILE, width), lambda i: (i, 0)),
        out_shape=jax.ShapeDtypeStruct((rows, width), bf16),
        compiler_params=params("arbitrary"),
        cost_estimate=cost(6 * rows * width * hidden, 3 * 2 * width * hidden + 4 * rows * width),
        name="expert",
    )(rows_in, gate, up, down)


def gather_kernel(table_ref, apart_ref, back_ref, out_ref, pick, *, experts):
    rows = back_ref.shape[0]

    @pl.when(pl.program_id(0) == 0)
    def _():
        chosen = expert_of(rows, 0, SECOND, experts)
        table = table_ref[...]
        slot = mm_last(table[:, 0:experts], chosen)
        weight = mm_last(table[:, experts : 2 * experts], chosen)
        block, wanted = second_slot(lax.broadcasted_iota(jnp.int32, (1, rows), 1) % SECOND)
        hit = (slot == wanted.astype(f32)) & (apart_ref[...] == block)
        pick[...] = jnp.where(hit, weight, 0.0).astype(bf16)

    out_ref[...] = mm(pick[...], back_ref[...]).astype(bf16)


def final_kernel(table_ref, back_ref, sum_ref, out_ref, *, experts):
    rows = back_ref.shape[0]
    table = table_ref[...]
    chosen = expert_of(rows, 0, FIRST, experts)
    slot = mm_last(table[:, 0:experts], chosen)
    weight = mm_last(table[:, experts : 2 * experts], chosen)
    at = lax.broadcasted_iota(jnp.int32, (1, rows), 1) % FIRST
    own = mm(jnp.where(slot == at.astype(f32), weight, 0.0).astype(bf16), back_ref[...])
    out_ref[...] = (own + sum_ref[...].astype(f32)).astype(bf16)


def exchanged(value):
    return lax.all_to_all(value, EP, split_axis=0, concat_axis=0, tiled=True)


def experts_half(sample, gain, pick, score, gate, up, down):
    tokens, width = sample.shape
    experts = lax.axis_size(EP)
    blocks = lax.axis_size("tp")
    every = width + 128
    own, first_out = pl.pallas_call(
        route_kernel,
        out_shape=[
            jax.ShapeDtypeStruct((tokens, every), bf16),
            jax.ShapeDtypeStruct((experts * FIRST, width), bf16),
        ],
        compiler_params=params(),
        cost_estimate=cost(1e9, 3e6),
        name="route",
    )(sample, gain.reshape(1, width), pick.T, score.T)
    apart = (jnp.arange(blocks * tokens, dtype=jnp.int32) // tokens - lax.axis_index("tp")) % blocks
    table = lax.all_gather(own, "tp", axis=0, tiled=True)
    first_in = exchanged(first_out.reshape(experts, FIRST, width))
    late_rows = lax.all_gather(first_in[:, :LATE], "tp", axis=0, tiled=True).reshape(-1, width)

    count = experts * SECOND
    tile = count // 4
    second_out = pl.pallas_call(
        functools.partial(second_kernel, experts=experts),
        grid=(count // tile,),
        in_specs=[
            pl.BlockSpec((blocks * tokens, every), lambda i: (0, 0)),
            pl.BlockSpec((1, blocks * tokens), lambda i: (0, 0)),
        ],
        out_specs=pl.BlockSpec((tile, width), lambda i: (i, 0)),
        out_shape=jax.ShapeDtypeStruct((count, width), bf16),
        compiler_params=params("arbitrary"),
        cost_estimate=cost(3.2e9, 1e7),
        name="second",
    )(table, apart.reshape(1, -1))
    second_in = exchanged(second_out.reshape(experts, SECOND, width))

    late_part = expert(late_rows, gate, up, down)
    own_part = expert(first_in[:, LATE:].reshape(-1, width), gate, up, down)
    late_sum = lax.psum_scatter(
        late_part.reshape(blocks * experts, LATE, width), "tp", scatter_dimension=0, tiled=True
    )
    second_part = expert(second_in.reshape(count, width), gate, up, down)
    second_back = exchanged(second_part.reshape(experts, SECOND, width))
    first_back = exchanged(
        jnp.concatenate([late_sum, own_part.reshape(experts, FIRST - LATE, width)], axis=1)
    )
    col_tile = 512
    second_mix = pl.pallas_call(
        functools.partial(gather_kernel, experts=experts),
        grid=(width // col_tile,),
        in_specs=[
            pl.BlockSpec((blocks * tokens, 128), lambda i: (0, width // 128)),
            pl.BlockSpec((blocks * tokens, 1), lambda i: (0, 0)),
            pl.BlockSpec((count, col_tile), lambda i: (0, i)),
        ],
        out_specs=pl.BlockSpec((blocks * tokens, col_tile), lambda i: (0, i)),
        out_shape=jax.ShapeDtypeStruct((blocks * tokens, width), bf16),
        scratch_shapes=[pltpu.VMEM((blocks * tokens, count), bf16)],
        compiler_params=params("arbitrary"),
        cost_estimate=cost(3.2e9, 1e7),
        name="gather",
    )(table, apart.reshape(-1, 1), second_back.reshape(count, width))
    second_sum = lax.psum_scatter(second_mix, "tp", scatter_dimension=0, tiled=True)
    return pl.pallas_call(
        functools.partial(final_kernel, experts=experts),
        grid=(1,),
        in_specs=[
            pl.BlockSpec((tokens, 128), lambda i: (0, width // 128)),
            pl.BlockSpec((experts * FIRST, width), lambda i: (0, 0)),
            pl.BlockSpec((tokens, width), lambda i: (0, 0)),
        ],
        out_specs=pl.BlockSpec((tokens, width), lambda i: (0, 0)),
        out_shape=jax.ShapeDtypeStruct((tokens, width), bf16),
        compiler_params=params("arbitrary"),
        cost_estimate=cost(2e8, 2e6),
        name="final",
    )(own, first_back.reshape(experts * FIRST, width), second_sum)


def body(*args):
    moe_out = experts_half(*args[14:])
    mixed = mixer_half(*args[:14])
    return (mixed, moe_out)


def solution(mesh):
    split = Mesh(mesh.devices.reshape(4, 4, 2, mesh.shape["tp"]), ("ep_0", "ep_1", "ep_2", "tp"))
    return jax.shard_map(
        body,
        mesh=split,
        in_specs=(
            P(EP, "tp"),
            P(EP, "tp"),
            P(EP, "tp"),
            P(EP, "tp"),
            P(EP, "tp"),
            P(None, "tp"),
            P(None, "tp"),
            P(None, "tp"),
            P("tp"),
            P("tp"),
            P("tp"),
            P(EP, "tp"),
            P("tp"),
            P("tp", None),
            P(EP_TP, None),
            P(),
            P(EP_TP, None),
            P(EP_TP, None),
            P(EP, None, "tp"),
            P(EP, None, "tp"),
            P(EP, "tp", None),
        ),
        out_specs=(P(EP_TP, None), P(EP_TP, None)),
        check_vma=False,
    )
```

```python
import functools

import jax
import jax.numpy as jnp
from jax import lax
from jax.experimental import pallas as pl
from jax.experimental.pallas import tpu as pltpu
from jax.sharding import Mesh
from jax.sharding import PartitionSpec as P


HEAD = 64
STATE = 128
SPAN = 128
PAIR = 2 * HEAD
CAP = 20
LATE = 8
EARLY = CAP - LATE
ROW_TILE = 256
EP = ("ep_0", "ep_1", "ep_2")
EP_TP = ("ep_0", "ep_1", "ep_2", "tp")

norm_eps = 1e-05
clamp_top = 7.0
sigmoid_sharp = 1.702
LOG2E = 1.4426950408889634
HIGHEST = lax.Precision.HIGHEST
f32 = jnp.float32
bf16 = jnp.bfloat16


def silu(v):
    half = 0.5 * v
    return half + half * jnp.tanh(half)


def mm(a, b):
    return jnp.dot(a, b, preferred_element_type=f32)


def mm_last(a, b):
    return lax.dot_general(a, b, (((1,), (1,)), ((), ())), preferred_element_type=f32)


def lanes_below(shape, limit):
    return lax.broadcasted_iota(jnp.int32, shape, 1) < limit


def params(*sem):
    return pltpu.CompilerParams(dimension_semantics=sem, vmem_limit_bytes=60 * 1024 * 1024)


def cost(flops, nbytes):
    return pl.CostEstimate(flops=int(flops), bytes_accessed=int(nbytes), transcendentals=0)


def expand_heads(row, heads):
    low = lanes_below((1, PAIR), HEAD)
    return [
        jnp.where(low, row[:, 2 * p : 2 * p + 1], row[:, 2 * p + 1 : 2 * p + 2])
        for p in range(heads // 2)
    ]


def states_kernel(
    x_ref, b_ref, c_ref, halo_ref, taps_ref, dtp_ref, spike_ref, off_ref, fade_ref,
    xs_ref, bs_ref, cs_ref, row_ref, send_ref, buf, state, total,
):
    step = pl.program_id(0)
    inner = x_ref.shape[1]
    group = b_ref.shape[1]
    heads = dtp_ref.shape[0]
    groups = group // STATE
    pairs = heads // groups // 2

    @pl.when(step == 0)
    def _():
        buf[0:8, :] = halo_ref[...].astype(f32)
        state[...] = jnp.zeros_like(state)
        total[...] = jnp.zeros_like(total)

    taps = taps_ref[...].astype(f32)
    for ref, out, base in ((x_ref, xs_ref, 0), (b_ref, bs_ref, inner), (c_ref, cs_ref, inner + group)):
        for j in range(0, ref.shape[1], 128):
            at = base + j
            cols = slice(at, at + 128)
            new = ref[:, j : j + 128].astype(f32)
            buf[8 : 8 + SPAN, cols] = new
            acc = new * taps[3:4, cols]
            for k in range(3):
                acc = acc + buf[5 + k : 5 + k + SPAN, cols] * taps[k : k + 1, cols]
            out[:, j : j + 128] = silu(acc).astype(bf16)
    buf[0:8, :] = buf[SPAN : SPAN + 8, :]

    pre = dtp_ref[...].astype(f32) + off_ref[...]
    dt = jnp.maximum(pre, 0.0) + jnp.log1p(jnp.exp(-jnp.abs(pre)))
    log_decay = (spike_ref[...] - jnp.exp(fade_ref[...]) * dt) * LOG2E
    upto = (
        lax.broadcasted_iota(jnp.int32, (SPAN, SPAN), 0)
        <= lax.broadcasted_iota(jnp.int32, (SPAN, SPAN), 1)
    ).astype(f32)
    cum = jnp.dot(log_decay, upto, precision=HIGHEST, preferred_element_type=f32)
    rows = cum - jnp.log2(dt)
    row_ref[0:heads, :] = rows
    row_ref[heads : 2 * heads, :] = cum
    factor = jnp.exp2(cum[:, SPAN - 1 : SPAN] - rows)
    end = jnp.concatenate([cum, jnp.zeros((128 - heads, SPAN), f32)], axis=0).T[SPAN - 1 : SPAN, 0:heads]
    total[...] = total[...] + jnp.concatenate(expand_heads(end, heads), axis=1)
    low = lanes_below((STATE, PAIR), HEAD)
    shrink = expand_heads(jnp.exp2(end), heads)
    for g in range(groups):
        bt = bs_ref[:, g * STATE : (g + 1) * STATE].astype(f32).T
        for p in range(pairs):
            q = g * pairs + p
            cols = slice(q * PAIR, (q + 1) * PAIR)
            left = jnp.concatenate(
                [bt * factor[2 * q : 2 * q + 1, :], bt * factor[2 * q + 1 : 2 * q + 2, :]], axis=0
            ).astype(bf16)
            res = mm(left, xs_ref[:, cols])
            state[:, cols] = state[:, cols] * shrink[q] + jnp.where(low, res[:STATE], res[STATE:])

    @pl.when(step == pl.num_programs(0) - 1)
    def _():
        half_cols = inner // 2
        t = total[0:1, :]
        hi = t.astype(bf16).astype(f32)
        mid = (t - hi).astype(bf16).astype(f32)
        tail = jnp.concatenate([hi, mid, t - hi - mid, jnp.zeros((5, inner), f32)], axis=0)
        for e in range(send_ref.shape[0]):
            rows_of, cols = slice(8 * (e // 2), 8 * (e // 2) + 8), slice(e % 2 * half_cols, (e % 2 + 1) * half_cols)
            send_ref[e] = jnp.concatenate([state[rows_of, cols], tail[:, cols]], axis=0).astype(bf16)


def place_of(device):
    return {"ep_0": device // 8, "ep_1": device // 2 % 4, "ep_2": device % 2}


def entering_kernel(msg_ref, out_ref, came, before, back, send_sem, recv_sem, send_sem2, recv_sem2):
    ep = msg_ref.shape[0]
    half_cols = msg_ref.shape[2]
    me = (lax.axis_index("ep_0") * 4 + lax.axis_index("ep_1")) * 2 + lax.axis_index("ep_2")
    barrier = pltpu.get_barrier_semaphore()

    @pl.loop(1, ep)
    def _(k):
        pl.semaphore_signal(
            barrier, inc=1, device_id=place_of((me + k) % ep), device_id_type=pl.DeviceIdType.MESH
        )

    pl.semaphore_wait(barrier, ep - 1)

    def there(k):
        to = (me + k) % ep
        return pltpu.make_async_remote_copy(
            src_ref=msg_ref.at[to], dst_ref=came.at[me], send_sem=send_sem.at[k], recv_sem=recv_sem.at[k],
            device_id=place_of(to), device_id_type=pl.DeviceIdType.MESH,
        )

    def returned(k):
        to = (me + k) % ep
        return pltpu.make_async_remote_copy(
            src_ref=before.at[to], dst_ref=back.at[me], send_sem=send_sem2.at[k], recv_sem=recv_sem2.at[k],
            device_id=place_of(to), device_id_type=pl.DeviceIdType.MESH,
        )

    @pl.loop(1, ep)
    def _(k):
        there(k).start()

    came[me] = msg_ref[me]

    @pl.loop(1, ep)
    def _(k):
        there(k).wait()

    running = jnp.zeros((8, half_cols), f32)
    for i in range(ep):
        before[i] = running.astype(bf16)
        block = came[i].astype(f32)
        running = running * jnp.exp2(block[8:9] + block[9:10] + block[10:11]) + block[0:8]

    @pl.loop(1, ep)
    def _(k):
        returned(k).start()

    back[me] = before[me]

    @pl.loop(1, ep)
    def _(k):
        returned(k).wait()

    for e in range(ep):
        out_ref[8 * (e // 2) : 8 * (e // 2) + 8, e % 2 * half_cols : (e % 2 + 1) * half_cols] = back[e].astype(f32)


def shifted(value, distance):
    return lax.ppermute(value, EP, [(i, i + distance) for i in range(lax.axis_size(EP) - distance)])


def entering_state(message):
    ep, _, half_cols = message.shape
    sems = pltpu.SemaphoreType.DMA((ep,))
    return pl.pallas_call(
        entering_kernel,
        in_specs=[pl.BlockSpec(memory_space=pltpu.VMEM)],
        out_specs=pl.BlockSpec(memory_space=pltpu.VMEM),
        out_shape=jax.ShapeDtypeStruct((STATE, 2 * half_cols), f32),
        scratch_shapes=[
            pltpu.VMEM((ep, 16, half_cols), bf16),
            pltpu.VMEM((ep, 8, half_cols), bf16),
            pltpu.VMEM((ep, 8, half_cols), bf16),
            sems, sems, sems, sems,
        ],
        compiler_params=pltpu.CompilerParams(collective_id=0, has_side_effects=True),
        cost_estimate=cost(1e10, 3e6),
        name="entering",
    )(message)


def mixer_kernel(
    xs_ref, bs_ref, cs_ref, z_ref, row_ref, enter_ref, skip_ref, gain_ref, w_ref,
    out_ref, state, gated, normed,
):
    step = pl.program_id(0)
    inner = xs_ref.shape[1]
    group = bs_ref.shape[1]
    heads = row_ref.shape[0] // 2
    groups = group // STATE
    pairs = heads // groups // 2
    wide = inner // groups

    @pl.when(step == 0)
    def _():
        state[...] = enter_ref[...]

    mask = lax.broadcasted_iota(jnp.int32, (SPAN, SPAN), 0) >= lax.broadcasted_iota(
        jnp.int32, (SPAN, SPAN), 1
    )
    low = lanes_below((STATE, PAIR), HEAD)
    rows = row_ref[0:heads, :]
    cum = jnp.concatenate(
        [row_ref[heads : 2 * heads, :], jnp.zeros((128 - heads, SPAN), f32)], axis=0
    ).T
    factor = jnp.exp2(row_ref[heads : 2 * heads, SPAN - 1 : SPAN] - rows)
    shrink = expand_heads(jnp.exp2(cum[SPAN - 1 : SPAN, 0:heads]), heads)
    for g in range(groups):
        gcols = slice(g * STATE, (g + 1) * STATE)
        bt = bs_ref[:, gcols].astype(f32).T
        cmat = cs_ref[:, gcols]
        c32 = cmat.astype(f32)
        scores = mm_last(cmat, bs_ref[:, gcols])
        squares = jnp.zeros((SPAN, PAIR), f32)
        for p in range(pairs):
            q = g * pairs + p
            cols = slice(q * PAIR, (q + 1) * PAIR)
            lefts, downs = [], []
            for h in (2 * q, 2 * q + 1):
                col = jnp.broadcast_to(cum[:, h : h + 1], (SPAN, SPAN))
                decay = jnp.exp2(jnp.where(mask, col - rows[h : h + 1, :], -1e30))
                lefts.append(
                    jnp.concatenate([(scores * decay).astype(bf16), (c32 * jnp.exp2(col)).astype(bf16)], axis=1)
                )
                downs.append((bt * factor[h : h + 1, :]).astype(bf16))
            xp = xs_ref[:, cols]
            sp = state[:, cols]
            res = mm(jnp.concatenate(lefts, axis=0), jnp.concatenate([xp, sp.astype(bf16)], axis=0))
            add = mm(jnp.concatenate(downs, axis=0), xp)
            state[:, cols] = sp * shrink[q] + jnp.where(low, add[:STATE], add[STATE:])
            y = jnp.where(low, res[:SPAN], res[SPAN:]) + xp.astype(f32) * skip_ref[:, cols]
            y = y * silu(z_ref[:, cols].astype(f32))
            gated[:, cols] = y
            squares = squares + y * y
        scale = lax.rsqrt(jnp.sum(squares, axis=1, keepdims=True) * (1.0 / wide) + norm_eps)
        wcols = slice(g * wide, (g + 1) * wide)
        normed[:, wcols] = (gated[:, wcols] * scale * gain_ref[:, wcols]).astype(bf16)
    out_ref[...] = mm(normed[...], w_ref[...]).astype(bf16)


def mixer_half(
    features, gating, insert, query, presoftplus, entry_taps, insert_taps, query_taps,
    offset, fading, skip, spike, gain, projection,
):
    rows, inner = features.shape
    group = insert.shape[1]
    heads = offset.shape[0]
    width = projection.shape[1]
    every = inner + 2 * group
    ep = lax.axis_size(EP)
    last = jnp.concatenate([a[rows - 8 :] for a in (features, insert, query)], axis=1)
    halo = shifted(last, 1)
    taps = jnp.concatenate([entry_taps, insert_taps, query_taps], axis=1)
    steps = rows // SPAN

    def block(n):
        return pl.BlockSpec((SPAN, n), lambda i: (i, 0))

    def whole(*shape):
        return pl.BlockSpec(shape, lambda i: (0,) * len(shape))

    def across(n):
        return pl.BlockSpec((n, SPAN), lambda i: (0, i))

    xs, bs, cs, row, message = pl.pallas_call(
        states_kernel,
        grid=(steps,),
        in_specs=[
            block(inner), block(group), block(group), whole(8, every), whole(4, every),
            across(heads), across(heads), whole(heads, 1), whole(heads, 1),
        ],
        out_specs=[
            block(inner), block(group), block(group), across(2 * heads),
            whole(ep, 16, inner // 2),
        ],
        out_shape=[
            jax.ShapeDtypeStruct((rows, inner), bf16),
            jax.ShapeDtypeStruct((rows, group), bf16),
            jax.ShapeDtypeStruct((rows, group), bf16),
            jax.ShapeDtypeStruct((2 * heads, rows), f32),
            jax.ShapeDtypeStruct((ep, 16, inner // 2), bf16),
        ],
        scratch_shapes=[
            pltpu.VMEM((SPAN + 8, every), f32),
            pltpu.VMEM((STATE, inner), f32),
            pltpu.VMEM((1, inner), f32),
        ],
        compiler_params=params("arbitrary"),
        cost_estimate=cost(8e9, 1e7),
        name="states",
    )(
        features, insert, query, halo, taps, presoftplus.T, spike.T,
        offset.reshape(heads, 1), fading.reshape(heads, 1),
    )
    entering = entering_state(message)
    partial = pl.pallas_call(
        mixer_kernel,
        grid=(steps,),
        in_specs=[
            block(inner), block(group), block(group), block(inner), across(2 * heads),
            whole(STATE, inner), whole(1, inner), whole(1, inner), whole(inner, width),
        ],
        out_specs=block(width),
        out_shape=jax.ShapeDtypeStruct((rows, width), bf16),
        scratch_shapes=[
            pltpu.VMEM((STATE, inner), f32),
            pltpu.VMEM((SPAN, inner), f32),
            pltpu.VMEM((SPAN, inner), bf16),
        ],
        compiler_params=params("arbitrary"),
        cost_estimate=cost(2e10, 2e7),
        name="mixer",
    )(
        xs, bs, cs, gating, row, entering,
        jnp.repeat(skip, HEAD).reshape(1, inner), gain.reshape(1, inner), projection,
    )
    return lax.psum_scatter(partial, "tp", scatter_dimension=0, tiled=True)


FIRST = 16
SECOND = 40
OTHERS = 36


def second_slot(inside):
    other = inside < OTHERS
    return (
        jnp.where(other, inside // EARLY + 1, 0),
        jnp.where(other, inside % EARLY + LATE, inside - OTHERS + FIRST),
    )


def expert_of(rows, first, per, experts):
    at = lax.broadcasted_iota(jnp.int32, (rows, experts), 0) + first
    return (at // per == lax.broadcasted_iota(jnp.int32, (rows, experts), 1)).astype(bf16)


def route_kernel(x_ref, gain_ref, pick_ref, score_ref, token_ref, first_ref):
    tokens, width = x_ref.shape
    experts = first_ref.shape[0] // FIRST
    x = x_ref[...].astype(f32)
    x = x - jnp.mean(x, axis=1, keepdims=True)
    x = x * lax.rsqrt(jnp.mean(x * x, axis=1, keepdims=True) + norm_eps) * gain_ref[...]
    normed = x.astype(bf16)
    token_ref[:, 0:width] = normed
    weight = jnp.exp(score_ref[...])
    weight = weight / jnp.sum(weight, axis=0, keepdims=True)
    lane = lax.broadcasted_iota(jnp.int32, (experts, tokens), 0)
    taken = jnp.zeros((experts, tokens), f32)
    dense = jnp.zeros((experts, tokens), f32)
    for k in range(pick_ref.shape[0]):
        hit = pick_ref[k : k + 1, :] == lane
        taken = jnp.where(hit, 1.0, taken)
        dense = jnp.where(hit, weight[k : k + 1, :], dense)
    earlier = (
        lax.broadcasted_iota(jnp.int32, (tokens, tokens), 0)
        < lax.broadcasted_iota(jnp.int32, (tokens, tokens), 1)
    ).astype(bf16)
    slot = jnp.where(taken > 0, mm(taken.astype(bf16), earlier), -1.0)
    token_ref[:, width : width + 128] = jnp.concatenate(
        [slot, dense, jnp.zeros((128 - 2 * experts, tokens), f32)], axis=0
    ).T.astype(bf16)
    rows = experts * FIRST
    spread = mm(expert_of(rows, 0, FIRST, experts), slot.astype(bf16))
    wanted = lax.broadcasted_iota(jnp.int32, (rows, 1), 0) % FIRST
    first_ref[...] = mm((spread == wanted.astype(f32)).astype(bf16), normed).astype(bf16)


def second_kernel(table_ref, apart_ref, out_ref, *, experts):
    width = table_ref.shape[1] - 128
    rows = out_ref.shape[0]
    first = pl.program_id(0) * rows
    spread = mm_last(expert_of(rows, first, SECOND, experts), table_ref[:, width : width + experts])
    at = lax.broadcasted_iota(jnp.int32, (rows, 1), 0) + first
    block, wanted = second_slot(at % SECOND)
    hit = (spread == wanted.astype(f32)) & (apart_ref[...] == block)
    out_ref[...] = mm(hit.astype(bf16), table_ref[:, 0:width]).astype(bf16)


def expert_kernel(x_ref, gate_ref, up_ref, down_ref, out_ref):
    x = x_ref[...]
    g = jnp.minimum(mm(x, gate_ref[...]), clamp_top)
    u = jnp.clip(mm(x, up_ref[...]), -clamp_top, clamp_top) + 1.0
    act = g * (0.5 + 0.5 * jnp.tanh((0.5 * sigmoid_sharp) * g)) * u
    out_ref[...] = mm(act.astype(bf16), down_ref[...]).astype(bf16)


def expert(rows_in, gate, up, down):
    rows, width = rows_in.shape
    hidden = gate.shape[2]
    return pl.pallas_call(
        expert_kernel,
        grid=(rows // ROW_TILE,),
        in_specs=[
            pl.BlockSpec((ROW_TILE, width), lambda i: (i, 0)),
            pl.BlockSpec((None, width, hidden), lambda i: (0, 0, 0)),
            pl.BlockSpec((None, width, hidden), lambda i: (0, 0, 0)),
            pl.BlockSpec((None, hidden, width), lambda i: (0, 0, 0)),
        ],
        out_specs=pl.BlockSpec((ROW_TILE, width), lambda i: (i, 0)),
        out_shape=jax.ShapeDtypeStruct((rows, width), bf16),
        compiler_params=params("arbitrary"),
        cost_estimate=cost(6 * rows * width * hidden, 3 * 2 * width * hidden + 4 * rows * width),
        name="expert",
    )(rows_in, gate, up, down)


def joint_kernel(
    rows_hbm, first_ref, tags_ref, gate_hbm, up_hbm, down_hbm, out_ref,
    rows, gate, up, down, res, back, first_back, pick, pick_first, part, shares,
    load_sem, weight_sem, send_sem, recv_sem, first_send, first_recv, part_send, part_recv,
):
    ep, per, width = res.shape
    experts = ep
    tokens = out_ref.shape[0]
    blocks = tags_ref.shape[0] // tokens
    col_tile = part.shape[3]
    z, y, core = lax.axis_index("ep_0"), lax.axis_index("ep_1"), lax.axis_index("ep_2")
    tp = lax.axis_index("tp")
    me = (z * 4 + y) * 2 + core
    mesh_ids = pl.DeviceIdType.MESH

    def place(k):
        return (z + k // 2) % 4, (y + k // 8 + k // 2) % 4, (core + k) % 2

    def index(k):
        a, b, c = place(k)
        return (a * 4 + b) * 2 + c

    def device(k):
        a, b, c = place(k)
        return {"ep_0": a, "ep_1": b, "ep_2": c}

    def load(k):
        return pltpu.make_async_copy(rows_hbm.at[index(k)], rows.at[k], load_sem.at[k])

    def weights():
        return [
            pltpu.make_async_copy(src, dst, weight_sem.at[n])
            for n, (src, dst) in enumerate(((gate_hbm, gate), (up_hbm, up), (down_hbm, down)))
        ]

    def give_back(k):
        return pltpu.make_async_remote_copy(
            src_ref=res.at[k], dst_ref=back.at[me], send_sem=send_sem.at[k], recv_sem=recv_sem.at[k],
            device_id=device(k), device_id_type=mesh_ids,
        )

    def give_first(k):
        return pltpu.make_async_remote_copy(
            src_ref=first_ref.at[index(k)], dst_ref=first_back.at[me],
            send_sem=first_send.at[k], recv_sem=first_recv.at[k],
            device_id=device(k), device_id_type=mesh_ids,
        )

    def give_part(t, r):
        return pltpu.make_async_remote_copy(
            src_ref=part.at[t, r], dst_ref=shares.at[t, r],
            send_sem=part_send.at[t, r], recv_sem=part_recv.at[t, r],
            device_id={"tp": (tp + r) % blocks}, device_id_type=mesh_ids,
        )

    for w in weights():
        w.start()

    @pl.loop(0, ep)
    def _(k):
        load(k).start()

    barrier = pltpu.get_barrier_semaphore()

    @pl.loop(1, ep)
    def _(k):
        pl.semaphore_signal(barrier, inc=1, device_id=device(k), device_id_type=mesh_ids)

    for r in range(1, blocks):
        pl.semaphore_signal(
            barrier, inc=1, device_id={"tp": (tp + r) % blocks}, device_id_type=mesh_ids
        )
    pl.semaphore_wait(barrier, ep - 1 + blocks - 1)

    for w in weights():
        w.wait()

    group = 8

    @pl.loop(0, ep // group)
    def _(c):
        @pl.loop(0, group)
        def _(j):
            load(c * group + j).wait()

        x = rows[pl.ds(c * group, group)].reshape(group * per, width)
        g = jnp.minimum(mm(x, gate[...]), clamp_top)
        u = jnp.clip(mm(x, up[...]), -clamp_top, clamp_top) + 1.0
        act = (g * (0.5 + 0.5 * jnp.tanh((0.5 * sigmoid_sharp) * g)) * u).astype(bf16)
        res[pl.ds(c * group, group)] = mm(act, down[...]).astype(bf16).reshape(group, per, width)

        @pl.loop(0, group)
        def _(j):
            @pl.when(c * group + j > 0)
            def _():
                give_back(c * group + j).start()

    @pl.loop(1, ep)
    def _(k):
        give_first(k).start()

    back[me] = res[0]
    first_back[me] = first_ref[me]

    count = experts * per
    chosen = expert_of(count, 0, per, experts)
    block, wanted = second_slot(lax.broadcasted_iota(jnp.int32, (1, count), 1) % per)
    for r in range(blocks):
        q = (tp + r) % blocks
        table = tags_ref[pl.ds(pl.multiple_of(q * tokens, tokens), tokens), :]
        slot = mm_last(table[:, 0:experts], chosen)
        weight = mm_last(table[:, experts : 2 * experts], chosen)
        hit = (slot == wanted.astype(f32)) & (block == r)
        pick[r * tokens : (r + 1) * tokens, :] = jnp.where(hit, weight, 0.0).astype(bf16)
    own = tags_ref[pl.ds(pl.multiple_of(tp * tokens, tokens), tokens), :]
    chosen = expert_of(experts * FIRST, 0, FIRST, experts)
    slot = mm_last(own[:, 0:experts], chosen)
    weight = mm_last(own[:, experts : 2 * experts], chosen)
    at = lax.broadcasted_iota(jnp.int32, (1, experts * FIRST), 1) % FIRST
    pick_first[...] = jnp.where(slot == at.astype(f32), weight, 0.0).astype(bf16)

    @pl.loop(1, ep)
    def _(k):
        give_back(k).wait_recv()

    for t in range(width // col_tile):
        cols = slice(t * col_tile, (t + 1) * col_tile)
        got = mm(pick[...], back[:, :, cols].reshape(count, col_tile)).astype(bf16)
        part[t] = got.reshape(blocks, tokens, col_tile)
        for r in range(1, blocks):
            give_part(t, r).start()

    @pl.loop(1, ep)
    def _(k):
        give_first(k).wait_recv()

    for t in range(width // col_tile):
        cols = slice(t * col_tile, (t + 1) * col_tile)
        total = mm(pick_first[...], first_back[:, :, cols].reshape(experts * FIRST, col_tile))
        total = total + part[t, 0].astype(f32)
        for r in range(1, blocks):
            give_part(t, r).wait_recv()
            total = total + shares[t, r].astype(f32)
        out_ref[:, cols] = total.astype(bf16)

    @pl.loop(1, ep)
    def _(k):
        give_back(k).wait_send()
        give_first(k).wait_send()

    for t in range(width // col_tile):
        for r in range(1, blocks):
            give_part(t, r).wait_send()


def joint(second_in, first_res, tags, gate, up, down, tokens):
    ep, per, width = second_in.shape
    hidden = gate.shape[1]
    blocks = tags.shape[0] // tokens
    tiles = width // 512
    any_ref = pl.BlockSpec(memory_space=pl.ANY)
    vmem = pl.BlockSpec(memory_space=pltpu.VMEM)
    dma = pltpu.SemaphoreType.DMA
    return pl.pallas_call(
        joint_kernel,
        in_specs=[any_ref, vmem, vmem, any_ref, any_ref, any_ref],
        out_specs=vmem,
        out_shape=jax.ShapeDtypeStruct((tokens, width), bf16),
        scratch_shapes=[
            pltpu.VMEM((ep, per, width), bf16),
            pltpu.VMEM((width, hidden), bf16),
            pltpu.VMEM((width, hidden), bf16),
            pltpu.VMEM((hidden, width), bf16),
            pltpu.VMEM((ep, per, width), bf16),
            pltpu.VMEM((ep, per, width), bf16),
            pltpu.VMEM((ep, FIRST, width), bf16),
            pltpu.VMEM((blocks * tokens, ep * per), bf16),
            pltpu.VMEM((tokens, ep * FIRST), bf16),
            pltpu.VMEM((tiles, blocks, tokens, 512), bf16),
            pltpu.VMEM((tiles, blocks, tokens, 512), bf16),
            dma((ep,)), dma((3,)), dma((ep,)), dma((ep,)), dma((ep,)), dma((ep,)),
            dma((tiles, blocks)), dma((tiles, blocks)),
        ],
        compiler_params=pltpu.CompilerParams(
            collective_id=1, has_side_effects=True, vmem_limit_bytes=60 * 1024 * 1024
        ),
        cost_estimate=cost(4e10, 3e7),
        name="joint",
    )(second_in, first_res, tags, gate, up, down)


def exchanged(value):
    return lax.all_to_all(value, EP, split_axis=0, concat_axis=0, tiled=True)


def experts_half(sample, gain, pick, score, gate, up, down):
    tokens, width = sample.shape
    experts = lax.axis_size(EP)
    blocks = lax.axis_size("tp")
    every = width + 128
    own, first_out = pl.pallas_call(
        route_kernel,
        out_shape=[
            jax.ShapeDtypeStruct((tokens, every), bf16),
            jax.ShapeDtypeStruct((experts * FIRST, width), bf16),
        ],
        compiler_params=params(),
        cost_estimate=cost(1e9, 3e6),
        name="route",
    )(sample, gain.reshape(1, width), pick.T, score.T)
    apart = (jnp.arange(blocks * tokens, dtype=jnp.int32) // tokens - lax.axis_index("tp")) % blocks
    table = lax.all_gather(own, "tp", axis=0, tiled=True)
    first_in = exchanged(first_out.reshape(experts, FIRST, width))
    late_rows = lax.all_gather(first_in[:, :LATE], "tp", axis=0, tiled=True).reshape(-1, width)

    count = experts * SECOND
    tile = count // 4
    second_out = pl.pallas_call(
        functools.partial(second_kernel, experts=experts),
        grid=(count // tile,),
        in_specs=[
            pl.BlockSpec((blocks * tokens, every), lambda i: (0, 0)),
            pl.BlockSpec((1, blocks * tokens), lambda i: (0, 0)),
        ],
        out_specs=pl.BlockSpec((tile, width), lambda i: (i, 0)),
        out_shape=jax.ShapeDtypeStruct((count, width), bf16),
        compiler_params=params("arbitrary"),
        cost_estimate=cost(3.2e9, 1e7),
        name="second",
    )(table, apart.reshape(1, -1))
    second_in = exchanged(second_out.reshape(experts, SECOND, width))

    late_part = expert(late_rows, gate, up, down)
    own_part = expert(first_in[:, LATE:].reshape(-1, width), gate, up, down)
    late_sum = lax.psum_scatter(
        late_part.reshape(blocks * experts, LATE, width), "tp", scatter_dimension=0, tiled=True
    )
    first_res = jnp.concatenate([late_sum, own_part.reshape(experts, FIRST - LATE, width)], axis=1)
    return joint(second_in, first_res, table[:, width:], gate[0], up[0], down[0], tokens)


def body(*args):
    moe_out = experts_half(*args[14:])
    mixed = mixer_half(*args[:14])
    return (mixed, moe_out)


def solution(mesh):
    split = Mesh(mesh.devices.reshape(4, 4, 2, mesh.shape["tp"]), ("ep_0", "ep_1", "ep_2", "tp"))
    return jax.shard_map(
        body,
        mesh=split,
        in_specs=(
            P(EP, "tp"),
            P(EP, "tp"),
            P(EP, "tp"),
            P(EP, "tp"),
            P(EP, "tp"),
            P(None, "tp"),
            P(None, "tp"),
            P(None, "tp"),
            P("tp"),
            P("tp"),
            P("tp"),
            P(EP, "tp"),
            P("tp"),
            P("tp", None),
            P(EP_TP, None),
            P(),
            P(EP_TP, None),
            P(EP_TP, None),
            P(EP, None, "tp"),
            P(EP, None, "tp"),
            P(EP, "tp", None),
        ),
        out_specs=(P(EP_TP, None), P(EP_TP, None)),
        check_vma=False,
    )
```

```python
import functools

import jax
import jax.numpy as jnp
from jax import lax
from jax.experimental import pallas as pl
from jax.experimental.pallas import tpu as pltpu
from jax.sharding import Mesh
from jax.sharding import PartitionSpec as P


HEAD = 64
STATE = 128
SPAN = 128
PAIR = 2 * HEAD
CAP = 20
LATE = 8
EARLY = CAP - LATE
ROW_TILE = 256
EP = ("ep_0", "ep_1", "ep_2")
EP_TP = ("ep_0", "ep_1", "ep_2", "tp")

norm_eps = 1e-05
clamp_top = 7.0
sigmoid_sharp = 1.702
LOG2E = 1.4426950408889634
HIGHEST = lax.Precision.HIGHEST
f32 = jnp.float32
bf16 = jnp.bfloat16


def silu(v):
    half = 0.5 * v
    return half + half * jnp.tanh(half)


def mm(a, b):
    return jnp.dot(a, b, preferred_element_type=f32)


def mm_last(a, b):
    return lax.dot_general(a, b, (((1,), (1,)), ((), ())), preferred_element_type=f32)


def lanes_below(shape, limit):
    return lax.broadcasted_iota(jnp.int32, shape, 1) < limit


def params(*sem):
    return pltpu.CompilerParams(dimension_semantics=sem, vmem_limit_bytes=60 * 1024 * 1024)


def cost(flops, nbytes):
    return pl.CostEstimate(flops=int(flops), bytes_accessed=int(nbytes), transcendentals=0)


def expand_heads(row, heads):
    low = lanes_below((1, PAIR), HEAD)
    return [
        jnp.where(low, row[:, 2 * p : 2 * p + 1], row[:, 2 * p + 1 : 2 * p + 2])
        for p in range(heads // 2)
    ]


def states_kernel(
    x_ref, b_ref, c_ref, halo_ref, taps_ref, dtp_ref, spike_ref, off_ref, fade_ref,
    xs_ref, bs_ref, cs_ref, row_ref, send_ref, buf, state, total,
):
    step = pl.program_id(0)
    inner = x_ref.shape[1]
    group = b_ref.shape[1]
    heads = dtp_ref.shape[0]
    groups = group // STATE
    pairs = heads // groups // 2

    @pl.when(step == 0)
    def _():
        buf[0:8, :] = halo_ref[...].astype(f32)
        state[...] = jnp.zeros_like(state)
        total[...] = jnp.zeros_like(total)

    taps = taps_ref[...].astype(f32)
    for ref, out, base in ((x_ref, xs_ref, 0), (b_ref, bs_ref, inner), (c_ref, cs_ref, inner + group)):
        for j in range(0, ref.shape[1], 128):
            at = base + j
            cols = slice(at, at + 128)
            new = ref[:, j : j + 128].astype(f32)
            buf[8 : 8 + SPAN, cols] = new
            acc = new * taps[3:4, cols]
            for k in range(3):
                acc = acc + buf[5 + k : 5 + k + SPAN, cols] * taps[k : k + 1, cols]
            out[:, j : j + 128] = silu(acc).astype(bf16)
    buf[0:8, :] = buf[SPAN : SPAN + 8, :]

    pre = dtp_ref[...].astype(f32) + off_ref[...]
    dt = jnp.maximum(pre, 0.0) + jnp.log1p(jnp.exp(-jnp.abs(pre)))
    log_decay = (spike_ref[...] - jnp.exp(fade_ref[...]) * dt) * LOG2E
    upto = (
        lax.broadcasted_iota(jnp.int32, (SPAN, SPAN), 0)
        <= lax.broadcasted_iota(jnp.int32, (SPAN, SPAN), 1)
    ).astype(f32)
    cum = jnp.dot(log_decay, upto, precision=HIGHEST, preferred_element_type=f32)
    rows = cum - jnp.log2(dt)
    row_ref[0:heads, :] = rows
    row_ref[heads : 2 * heads, :] = cum
    factor = jnp.exp2(cum[:, SPAN - 1 : SPAN] - rows)
    end = jnp.concatenate([cum, jnp.zeros((128 - heads, SPAN), f32)], axis=0).T[SPAN - 1 : SPAN, 0:heads]
    total[...] = total[...] + jnp.concatenate(expand_heads(end, heads), axis=1)
    low = lanes_below((STATE, PAIR), HEAD)
    shrink = expand_heads(jnp.exp2(end), heads)
    for g in range(groups):
        bt = bs_ref[:, g * STATE : (g + 1) * STATE].astype(f32).T
        for p in range(pairs):
            q = g * pairs + p
            cols = slice(q * PAIR, (q + 1) * PAIR)
            left = jnp.concatenate(
                [bt * factor[2 * q : 2 * q + 1, :], bt * factor[2 * q + 1 : 2 * q + 2, :]], axis=0
            ).astype(bf16)
            res = mm(left, xs_ref[:, cols])
            state[:, cols] = state[:, cols] * shrink[q] + jnp.where(low, res[:STATE], res[STATE:])

    @pl.when(step == pl.num_programs(0) - 1)
    def _():
        half_cols = inner // 2
        t = total[0:1, :]
        hi = t.astype(bf16).astype(f32)
        mid = (t - hi).astype(bf16).astype(f32)
        tail = jnp.concatenate([hi, mid, t - hi - mid, jnp.zeros((5, inner), f32)], axis=0)
        for e in range(send_ref.shape[0]):
            rows_of, cols = slice(8 * (e // 2), 8 * (e // 2) + 8), slice(e % 2 * half_cols, (e % 2 + 1) * half_cols)
            send_ref[e] = jnp.concatenate([state[rows_of, cols], tail[:, cols]], axis=0).astype(bf16)


def place_of(device):
    return {"ep_0": device // 8, "ep_1": device // 2 % 4, "ep_2": device % 2}


def entering_kernel(msg_ref, out_ref, came, before, back, send_sem, recv_sem, send_sem2, recv_sem2):
    ep = msg_ref.shape[0]
    half_cols = msg_ref.shape[2]
    me = (lax.axis_index("ep_0") * 4 + lax.axis_index("ep_1")) * 2 + lax.axis_index("ep_2")
    barrier = pltpu.get_barrier_semaphore()

    @pl.loop(1, ep)
    def _(k):
        pl.semaphore_signal(
            barrier, inc=1, device_id=place_of((me + k) % ep), device_id_type=pl.DeviceIdType.MESH
        )

    pl.semaphore_wait(barrier, ep - 1)

    def there(k):
        to = (me + k) % ep
        return pltpu.make_async_remote_copy(
            src_ref=msg_ref.at[to], dst_ref=came.at[me], send_sem=send_sem.at[k], recv_sem=recv_sem.at[k],
            device_id=place_of(to), device_id_type=pl.DeviceIdType.MESH,
        )

    def returned(k):
        to = (me + k) % ep
        return pltpu.make_async_remote_copy(
            src_ref=before.at[to], dst_ref=back.at[me], send_sem=send_sem2.at[k], recv_sem=recv_sem2.at[k],
            device_id=place_of(to), device_id_type=pl.DeviceIdType.MESH,
        )

    @pl.loop(1, ep)
    def _(k):
        there(k).start()

    came[me] = msg_ref[me]

    @pl.loop(1, ep)
    def _(k):
        there(k).wait()

    running = jnp.zeros((8, half_cols), f32)
    for i in range(ep):
        before[i] = running.astype(bf16)
        block = came[i].astype(f32)
        running = running * jnp.exp2(block[8:9] + block[9:10] + block[10:11]) + block[0:8]

    @pl.loop(1, ep)
    def _(k):
        returned(k).start()

    back[me] = before[me]

    @pl.loop(1, ep)
    def _(k):
        returned(k).wait()

    for e in range(ep):
        out_ref[8 * (e // 2) : 8 * (e // 2) + 8, e % 2 * half_cols : (e % 2 + 1) * half_cols] = back[e].astype(f32)


def shifted(value, distance):
    return lax.ppermute(value, EP, [(i, i + distance) for i in range(lax.axis_size(EP) - distance)])


def entering_state(message):
    ep, _, half_cols = message.shape
    sems = pltpu.SemaphoreType.DMA((ep,))
    return pl.pallas_call(
        entering_kernel,
        in_specs=[pl.BlockSpec(memory_space=pltpu.VMEM)],
        out_specs=pl.BlockSpec(memory_space=pltpu.VMEM),
        out_shape=jax.ShapeDtypeStruct((STATE, 2 * half_cols), f32),
        scratch_shapes=[
            pltpu.VMEM((ep, 16, half_cols), bf16),
            pltpu.VMEM((ep, 8, half_cols), bf16),
            pltpu.VMEM((ep, 8, half_cols), bf16),
            sems, sems, sems, sems,
        ],
        compiler_params=pltpu.CompilerParams(collective_id=0, has_side_effects=True),
        cost_estimate=cost(1e10, 3e6),
        name="entering",
    )(message)


def mixer_kernel(
    xs_ref, bs_ref, cs_ref, z_ref, row_ref, enter_ref, skip_ref, gain_ref, w_ref,
    out_ref, state, gated, normed,
):
    step = pl.program_id(0)
    inner = xs_ref.shape[1]
    group = bs_ref.shape[1]
    heads = row_ref.shape[0] // 2
    groups = group // STATE
    pairs = heads // groups // 2
    wide = inner // groups

    @pl.when(step == 0)
    def _():
        state[...] = enter_ref[...]

    mask = lax.broadcasted_iota(jnp.int32, (SPAN, SPAN), 0) >= lax.broadcasted_iota(
        jnp.int32, (SPAN, SPAN), 1
    )
    low = lanes_below((STATE, PAIR), HEAD)
    rows = row_ref[0:heads, :]
    cum = jnp.concatenate(
        [row_ref[heads : 2 * heads, :], jnp.zeros((128 - heads, SPAN), f32)], axis=0
    ).T
    factor = jnp.exp2(row_ref[heads : 2 * heads, SPAN - 1 : SPAN] - rows)
    shrink = expand_heads(jnp.exp2(cum[SPAN - 1 : SPAN, 0:heads]), heads)
    for g in range(groups):
        gcols = slice(g * STATE, (g + 1) * STATE)
        bt = bs_ref[:, gcols].astype(f32).T
        cmat = cs_ref[:, gcols]
        c32 = cmat.astype(f32)
        scores = mm_last(cmat, bs_ref[:, gcols])
        squares = jnp.zeros((SPAN, PAIR), f32)
        for p in range(pairs):
            q = g * pairs + p
            cols = slice(q * PAIR, (q + 1) * PAIR)
            lefts, downs = [], []
            for h in (2 * q, 2 * q + 1):
                col = jnp.broadcast_to(cum[:, h : h + 1], (SPAN, SPAN))
                decay = jnp.exp2(jnp.where(mask, col - rows[h : h + 1, :], -1e30))
                lefts.append(
                    jnp.concatenate([(scores * decay).astype(bf16), (c32 * jnp.exp2(col)).astype(bf16)], axis=1)
                )
                downs.append((bt * factor[h : h + 1, :]).astype(bf16))
            xp = xs_ref[:, cols]
            sp = state[:, cols]
            res = mm(jnp.concatenate(lefts, axis=0), jnp.concatenate([xp, sp.astype(bf16)], axis=0))
            add = mm(jnp.concatenate(downs, axis=0), xp)
            state[:, cols] = sp * shrink[q] + jnp.where(low, add[:STATE], add[STATE:])
            y = jnp.where(low, res[:SPAN], res[SPAN:]) + xp.astype(f32) * skip_ref[:, cols]
            y = y * silu(z_ref[:, cols].astype(f32))
            gated[:, cols] = y
            squares = squares + y * y
        scale = lax.rsqrt(jnp.sum(squares, axis=1, keepdims=True) * (1.0 / wide) + norm_eps)
        wcols = slice(g * wide, (g + 1) * wide)
        normed[:, wcols] = (gated[:, wcols] * scale * gain_ref[:, wcols]).astype(bf16)
    out_ref[...] = mm(normed[...], w_ref[...]).astype(bf16)


def mixer_half(
    features, gating, insert, query, presoftplus, entry_taps, insert_taps, query_taps,
    offset, fading, skip, spike, gain, projection,
):
    rows, inner = features.shape
    group = insert.shape[1]
    heads = offset.shape[0]
    width = projection.shape[1]
    every = inner + 2 * group
    ep = lax.axis_size(EP)
    last = jnp.concatenate([a[rows - 8 :] for a in (features, insert, query)], axis=1)
    halo = shifted(last, 1)
    taps = jnp.concatenate([entry_taps, insert_taps, query_taps], axis=1)
    steps = rows // SPAN

    def block(n):
        return pl.BlockSpec((SPAN, n), lambda i: (i, 0))

    def whole(*shape):
        return pl.BlockSpec(shape, lambda i: (0,) * len(shape))

    def across(n):
        return pl.BlockSpec((n, SPAN), lambda i: (0, i))

    xs, bs, cs, row, message = pl.pallas_call(
        states_kernel,
        grid=(steps,),
        in_specs=[
            block(inner), block(group), block(group), whole(8, every), whole(4, every),
            across(heads), across(heads), whole(heads, 1), whole(heads, 1),
        ],
        out_specs=[
            block(inner), block(group), block(group), across(2 * heads),
            whole(ep, 16, inner // 2),
        ],
        out_shape=[
            jax.ShapeDtypeStruct((rows, inner), bf16),
            jax.ShapeDtypeStruct((rows, group), bf16),
            jax.ShapeDtypeStruct((rows, group), bf16),
            jax.ShapeDtypeStruct((2 * heads, rows), f32),
            jax.ShapeDtypeStruct((ep, 16, inner // 2), bf16),
        ],
        scratch_shapes=[
            pltpu.VMEM((SPAN + 8, every), f32),
            pltpu.VMEM((STATE, inner), f32),
            pltpu.VMEM((1, inner), f32),
        ],
        compiler_params=params("arbitrary"),
        cost_estimate=cost(8e9, 1e7),
        name="states",
    )(
        features, insert, query, halo, taps, presoftplus.T, spike.T,
        offset.reshape(heads, 1), fading.reshape(heads, 1),
    )
    entering = entering_state(message)
    partial = pl.pallas_call(
        mixer_kernel,
        grid=(steps,),
        in_specs=[
            block(inner), block(group), block(group), block(inner), across(2 * heads),
            whole(STATE, inner), whole(1, inner), whole(1, inner), whole(inner, width),
        ],
        out_specs=block(width),
        out_shape=jax.ShapeDtypeStruct((rows, width), bf16),
        scratch_shapes=[
            pltpu.VMEM((STATE, inner), f32),
            pltpu.VMEM((SPAN, inner), f32),
            pltpu.VMEM((SPAN, inner), bf16),
        ],
        compiler_params=params("arbitrary"),
        cost_estimate=cost(2e10, 2e7),
        name="mixer",
    )(
        xs, bs, cs, gating, row, entering,
        jnp.repeat(skip, HEAD).reshape(1, inner), gain.reshape(1, inner), projection,
    )
    return lax.psum_scatter(partial, "tp", scatter_dimension=0, tiled=True)


FIRST = 16
SECOND = 40
OTHERS = 36


def second_slot(inside):
    other = inside < OTHERS
    return (
        jnp.where(other, inside // EARLY + 1, 0),
        jnp.where(other, inside % EARLY + LATE, inside - OTHERS + FIRST),
    )


def expert_of(rows, first, per, experts):
    at = lax.broadcasted_iota(jnp.int32, (rows, experts), 0) + first
    return (at // per == lax.broadcasted_iota(jnp.int32, (rows, experts), 1)).astype(bf16)


def route_kernel(x_ref, gain_ref, pick_ref, score_ref, token_ref, first_ref):
    tokens, width = x_ref.shape
    experts = first_ref.shape[0] // FIRST
    x = x_ref[...].astype(f32)
    x = x - jnp.mean(x, axis=1, keepdims=True)
    x = x * lax.rsqrt(jnp.mean(x * x, axis=1, keepdims=True) + norm_eps) * gain_ref[...]
    normed = x.astype(bf16)
    token_ref[:, 0:width] = normed
    weight = jnp.exp(score_ref[...])
    weight = weight / jnp.sum(weight, axis=0, keepdims=True)
    lane = lax.broadcasted_iota(jnp.int32, (experts, tokens), 0)
    taken = jnp.zeros((experts, tokens), f32)
    dense = jnp.zeros((experts, tokens), f32)
    for k in range(pick_ref.shape[0]):
        hit = pick_ref[k : k + 1, :] == lane
        taken = jnp.where(hit, 1.0, taken)
        dense = jnp.where(hit, weight[k : k + 1, :], dense)
    earlier = (
        lax.broadcasted_iota(jnp.int32, (tokens, tokens), 0)
        < lax.broadcasted_iota(jnp.int32, (tokens, tokens), 1)
    ).astype(bf16)
    slot = jnp.where(taken > 0, mm(taken.astype(bf16), earlier), -1.0)
    token_ref[:, width : width + 128] = jnp.concatenate(
        [slot, dense, jnp.zeros((128 - 2 * experts, tokens), f32)], axis=0
    ).T.astype(bf16)
    rows = experts * FIRST
    spread = mm(expert_of(rows, 0, FIRST, experts), slot.astype(bf16))
    wanted = lax.broadcasted_iota(jnp.int32, (rows, 1), 0) % FIRST
    first_ref[...] = mm((spread == wanted.astype(f32)).astype(bf16), normed).astype(bf16)


def second_kernel(table_ref, apart_ref, out_ref, *, experts):
    width = table_ref.shape[1] - 128
    rows = out_ref.shape[0]
    first = pl.program_id(0) * rows
    spread = mm_last(expert_of(rows, first, SECOND, experts), table_ref[:, width : width + experts])
    at = lax.broadcasted_iota(jnp.int32, (rows, 1), 0) + first
    block, wanted = second_slot(at % SECOND)
    hit = (spread == wanted.astype(f32)) & (apart_ref[...] == block)
    out_ref[...] = mm(hit.astype(bf16), table_ref[:, 0:width]).astype(bf16)


def expert_kernel(x_ref, gate_ref, up_ref, down_ref, out_ref):
    x = x_ref[...]
    g = jnp.minimum(mm(x, gate_ref[...]), clamp_top)
    u = jnp.clip(mm(x, up_ref[...]), -clamp_top, clamp_top) + 1.0
    act = g * (0.5 + 0.5 * jnp.tanh((0.5 * sigmoid_sharp) * g)) * u
    out_ref[...] = mm(act.astype(bf16), down_ref[...]).astype(bf16)


def expert(rows_in, gate, up, down):
    rows, width = rows_in.shape
    hidden = gate.shape[2]
    return pl.pallas_call(
        expert_kernel,
        grid=(rows // ROW_TILE,),
        in_specs=[
            pl.BlockSpec((ROW_TILE, width), lambda i: (i, 0)),
            pl.BlockSpec((None, width, hidden), lambda i: (0, 0, 0)),
            pl.BlockSpec((None, width, hidden), lambda i: (0, 0, 0)),
            pl.BlockSpec((None, hidden, width), lambda i: (0, 0, 0)),
        ],
        out_specs=pl.BlockSpec((ROW_TILE, width), lambda i: (i, 0)),
        out_shape=jax.ShapeDtypeStruct((rows, width), bf16),
        compiler_params=params("arbitrary"),
        cost_estimate=cost(6 * rows * width * hidden, 3 * 2 * width * hidden + 4 * rows * width),
        name="expert",
    )(rows_in, gate, up, down)


def joint_kernel(
    rows_hbm, late_hbm, own_ref, tags_ref, gate_hbm, up_hbm, down_hbm, out_ref,
    rows, gate, up, down, res, back, late_all, late_sum, late_back, own_back,
    pick, pick_first, part, shares,
    load_sem, weight_sem, late_load, send_sem, recv_sem, share_send, share_recv,
    late_send, late_recv, own_send, own_recv, part_send, part_recv,
):
    ep, per, width = res.shape
    experts = ep
    tokens = out_ref.shape[0]
    blocks = tags_ref.shape[0] // tokens
    col_tile = part.shape[3]
    z, y, core = lax.axis_index("ep_0"), lax.axis_index("ep_1"), lax.axis_index("ep_2")
    tp = lax.axis_index("tp")
    me = (z * 4 + y) * 2 + core
    mesh_ids = pl.DeviceIdType.MESH

    def place(k):
        return (z + k // 2) % 4, (y + k // 8 + k // 2) % 4, (core + k) % 2

    def index(k):
        a, b, c = place(k)
        return (a * 4 + b) * 2 + c

    def device(k):
        a, b, c = place(k)
        return {"ep_0": a, "ep_1": b, "ep_2": c}

    def load(k):
        return pltpu.make_async_copy(rows_hbm.at[index(k)], rows.at[k], load_sem.at[k])

    def weights():
        return [
            pltpu.make_async_copy(src, dst, weight_sem.at[n])
            for n, (src, dst) in enumerate(((gate_hbm, gate), (up_hbm, up), (down_hbm, down)))
        ]

    def give_back(k):
        return pltpu.make_async_remote_copy(
            src_ref=res.at[k], dst_ref=back.at[me], send_sem=send_sem.at[k], recv_sem=recv_sem.at[k],
            device_id=device(k), device_id_type=mesh_ids,
        )

    def give_late(k):
        return pltpu.make_async_remote_copy(
            src_ref=late_sum.at[index(k)], dst_ref=late_back.at[me],
            send_sem=late_send.at[k], recv_sem=late_recv.at[k],
            device_id=device(k), device_id_type=mesh_ids,
        )

    def give_own(k):
        return pltpu.make_async_remote_copy(
            src_ref=own_ref.at[index(k)], dst_ref=own_back.at[me],
            send_sem=own_send.at[k], recv_sem=own_recv.at[k],
            device_id=device(k), device_id_type=mesh_ids,
        )

    def give_share(r):
        return pltpu.make_async_remote_copy(
            src_ref=late_hbm.at[(tp + r) % blocks], dst_ref=late_all.at[r],
            send_sem=share_send.at[r], recv_sem=share_recv.at[r],
            device_id={"tp": (tp + r) % blocks}, device_id_type=mesh_ids,
        )

    def give_part(t, r):
        return pltpu.make_async_remote_copy(
            src_ref=part.at[t, r], dst_ref=shares.at[t, r],
            send_sem=part_send.at[t, r], recv_sem=part_recv.at[t, r],
            device_id={"tp": (tp + r) % blocks}, device_id_type=mesh_ids,
        )

    for w in weights():
        w.start()

    @pl.loop(0, ep)
    def _(k):
        load(k).start()

    barrier = pltpu.get_barrier_semaphore()

    @pl.loop(1, ep)
    def _(k):
        pl.semaphore_signal(barrier, inc=1, device_id=device(k), device_id_type=mesh_ids)

    for r in range(1, blocks):
        pl.semaphore_signal(
            barrier, inc=1, device_id={"tp": (tp + r) % blocks}, device_id_type=mesh_ids
        )
    pl.semaphore_wait(barrier, ep - 1 + blocks - 1)

    for r in range(1, blocks):
        give_share(r).start()
    own_share = pltpu.make_async_copy(late_hbm.at[tp], late_all.at[0], late_load)
    own_share.start()

    for w in weights():
        w.wait()

    group = 8

    @pl.loop(0, ep // group)
    def _(c):
        @pl.loop(0, group)
        def _(j):
            load(c * group + j).wait()

        x = rows[pl.ds(c * group, group)].reshape(group * per, width)
        g = jnp.minimum(mm(x, gate[...]), clamp_top)
        u = jnp.clip(mm(x, up[...]), -clamp_top, clamp_top) + 1.0
        act = (g * (0.5 + 0.5 * jnp.tanh((0.5 * sigmoid_sharp) * g)) * u).astype(bf16)
        res[pl.ds(c * group, group)] = mm(act, down[...]).astype(bf16).reshape(group, per, width)

        @pl.loop(0, group)
        def _(j):
            @pl.when(c * group + j > 0)
            def _():
                give_back(c * group + j).start()

    @pl.loop(1, ep)
    def _(k):
        give_own(k).start()

    back[me] = res[0]
    own_back[me] = own_ref[me]

    count = experts * per
    chosen = expert_of(count, 0, per, experts)
    block, wanted = second_slot(lax.broadcasted_iota(jnp.int32, (1, count), 1) % per)
    for r in range(blocks):
        q = (tp + r) % blocks
        table = tags_ref[pl.ds(pl.multiple_of(q * tokens, tokens), tokens), :]
        slot = mm_last(table[:, 0:experts], chosen)
        weight = mm_last(table[:, experts : 2 * experts], chosen)
        hit = (slot == wanted.astype(f32)) & (block == r)
        pick[r * tokens : (r + 1) * tokens, :] = jnp.where(hit, weight, 0.0).astype(bf16)
    own = tags_ref[pl.ds(pl.multiple_of(tp * tokens, tokens), tokens), :]
    chosen = expert_of(experts * LATE, 0, LATE, experts)
    slot = mm_last(own[:, 0:experts], chosen)
    weight = mm_last(own[:, experts : 2 * experts], chosen)
    at = lax.broadcasted_iota(jnp.int32, (1, experts * LATE), 1) % LATE
    for n in range(FIRST // LATE):
        hit = slot == (at + n * LATE).astype(f32)
        pick_first[n] = jnp.where(hit, weight, 0.0).astype(bf16)

    own_share.wait()
    for r in range(1, blocks):
        give_share(r).wait_recv()

    @pl.loop(0, ep)
    def _(k):
        total = late_all[0, k].astype(f32)
        for r in range(1, blocks):
            total = total + late_all[r, k].astype(f32)
        late_sum[k] = total.astype(bf16)

    @pl.loop(1, ep)
    def _(k):
        give_late(k).start()

    late_back[me] = late_sum[me]

    @pl.loop(1, ep)
    def _(k):
        give_back(k).wait_recv()

    for t in range(width // col_tile):
        cols = slice(t * col_tile, (t + 1) * col_tile)
        got = mm(pick[...], back[:, :, cols].reshape(count, col_tile)).astype(bf16)
        part[t] = got.reshape(blocks, tokens, col_tile)
        for r in range(1, blocks):
            give_part(t, r).start()

    @pl.loop(1, ep)
    def _(k):
        give_own(k).wait_recv()
        give_late(k).wait_recv()

    for t in range(width // col_tile):
        cols = slice(t * col_tile, (t + 1) * col_tile)
        total = part[t, 0].astype(f32)
        for n, ref in enumerate((late_back, own_back)):
            total = total + mm(pick_first[n], ref[:, :, cols].reshape(experts * LATE, col_tile))
        for r in range(1, blocks):
            give_part(t, r).wait_recv()
            total = total + shares[t, r].astype(f32)
        out_ref[:, cols] = total.astype(bf16)

    @pl.loop(1, ep)
    def _(k):
        give_back(k).wait_send()
        give_own(k).wait_send()
        give_late(k).wait_send()

    for r in range(1, blocks):
        give_share(r).wait_send()
        for t in range(width // col_tile):
            give_part(t, r).wait_send()


def joint(second_in, late_part, own_part, tags, gate, up, down, tokens):
    ep, per, width = second_in.shape
    hidden = gate.shape[1]
    blocks = tags.shape[0] // tokens
    tiles = width // 512
    any_ref = pl.BlockSpec(memory_space=pl.ANY)
    vmem = pl.BlockSpec(memory_space=pltpu.VMEM)
    dma = pltpu.SemaphoreType.DMA
    return pl.pallas_call(
        joint_kernel,
        in_specs=[any_ref, any_ref, vmem, vmem, any_ref, any_ref, any_ref],
        out_specs=vmem,
        out_shape=jax.ShapeDtypeStruct((tokens, width), bf16),
        scratch_shapes=[
            pltpu.VMEM((ep, per, width), bf16),
            pltpu.VMEM((width, hidden), bf16),
            pltpu.VMEM((width, hidden), bf16),
            pltpu.VMEM((hidden, width), bf16),
            pltpu.VMEM((ep, per, width), bf16),
            pltpu.VMEM((ep, per, width), bf16),
            pltpu.VMEM((blocks, ep, LATE, width), bf16),
            pltpu.VMEM((ep, LATE, width), bf16),
            pltpu.VMEM((ep, LATE, width), bf16),
            pltpu.VMEM((ep, LATE, width), bf16),
            pltpu.VMEM((blocks * tokens, ep * per), bf16),
            pltpu.VMEM((FIRST // LATE, tokens, ep * LATE), bf16),
            pltpu.VMEM((tiles, blocks, tokens, 512), bf16),
            pltpu.VMEM((tiles, blocks, tokens, 512), bf16),
            dma((ep,)), dma((3,)), dma, dma((ep,)), dma((ep,)), dma((blocks,)), dma((blocks,)),
            dma((ep,)), dma((ep,)), dma((ep,)), dma((ep,)),
            dma((tiles, blocks)), dma((tiles, blocks)),
        ],
        compiler_params=pltpu.CompilerParams(
            collective_id=1, has_side_effects=True, vmem_limit_bytes=60 * 1024 * 1024
        ),
        cost_estimate=cost(4e10, 3e7),
        name="joint",
    )(second_in, late_part, own_part, tags, gate, up, down)


def exchanged(value):
    return lax.all_to_all(value, EP, split_axis=0, concat_axis=0, tiled=True)


def experts_half(sample, gain, pick, score, gate, up, down):
    tokens, width = sample.shape
    experts = lax.axis_size(EP)
    blocks = lax.axis_size("tp")
    every = width + 128
    own, first_out = pl.pallas_call(
        route_kernel,
        out_shape=[
            jax.ShapeDtypeStruct((tokens, every), bf16),
            jax.ShapeDtypeStruct((experts * FIRST, width), bf16),
        ],
        compiler_params=params(),
        cost_estimate=cost(1e9, 3e6),
        name="route",
    )(sample, gain.reshape(1, width), pick.T, score.T)
    apart = (jnp.arange(blocks * tokens, dtype=jnp.int32) // tokens - lax.axis_index("tp")) % blocks
    table = lax.all_gather(own, "tp", axis=0, tiled=True)
    first_in = exchanged(first_out.reshape(experts, FIRST, width))
    late_rows = lax.all_gather(first_in[:, :LATE], "tp", axis=0, tiled=True).reshape(-1, width)

    count = experts * SECOND
    tile = count // 4
    second_out = pl.pallas_call(
        functools.partial(second_kernel, experts=experts),
        grid=(count // tile,),
        in_specs=[
            pl.BlockSpec((blocks * tokens, every), lambda i: (0, 0)),
            pl.BlockSpec((1, blocks * tokens), lambda i: (0, 0)),
        ],
        out_specs=pl.BlockSpec((tile, width), lambda i: (i, 0)),
        out_shape=jax.ShapeDtypeStruct((count, width), bf16),
        compiler_params=params("arbitrary"),
        cost_estimate=cost(3.2e9, 1e7),
        name="second",
    )(table, apart.reshape(1, -1))
    second_in = exchanged(second_out.reshape(experts, SECOND, width))

    late_part = expert(late_rows, gate, up, down)
    own_part = expert(first_in[:, LATE:].reshape(-1, width), gate, up, down)
    return joint(
        second_in, late_part.reshape(blocks, experts, LATE, width),
        own_part.reshape(experts, FIRST - LATE, width), table[:, width:], gate[0], up[0], down[0], tokens,
    )


def body(*args):
    moe_out = experts_half(*args[14:])
    mixed = mixer_half(*args[:14])
    return (mixed, moe_out)


def solution(mesh):
    split = Mesh(mesh.devices.reshape(4, 4, 2, mesh.shape["tp"]), ("ep_0", "ep_1", "ep_2", "tp"))
    return jax.shard_map(
        body,
        mesh=split,
        in_specs=(
            P(EP, "tp"),
            P(EP, "tp"),
            P(EP, "tp"),
            P(EP, "tp"),
            P(EP, "tp"),
            P(None, "tp"),
            P(None, "tp"),
            P(None, "tp"),
            P("tp"),
            P("tp"),
            P("tp"),
            P(EP, "tp"),
            P("tp"),
            P("tp", None),
            P(EP_TP, None),
            P(),
            P(EP_TP, None),
            P(EP_TP, None),
            P(EP, None, "tp"),
            P(EP, None, "tp"),
            P(EP, "tp", None),
        ),
        out_specs=(P(EP_TP, None), P(EP_TP, None)),
        check_vma=False,
    )
```

```python
import functools

import jax
import jax.numpy as jnp
from jax import lax
from jax.experimental import pallas as pl
from jax.experimental.pallas import tpu as pltpu
from jax.sharding import Mesh
from jax.sharding import PartitionSpec as P


HEAD = 64
STATE = 128
SPAN = 128
PAIR = 2 * HEAD
CAP = 20
LATE = 8
EARLY = CAP - LATE
ROW_TILE = 256
EP = ("ep_0", "ep_1", "ep_2")
EP_TP = ("ep_0", "ep_1", "ep_2", "tp")

norm_eps = 1e-05
clamp_top = 7.0
sigmoid_sharp = 1.702
LOG2E = 1.4426950408889634
HIGHEST = lax.Precision.HIGHEST
f32 = jnp.float32
bf16 = jnp.bfloat16


def silu(v):
    half = 0.5 * v
    return half + half * jnp.tanh(half)


def mm(a, b):
    return jnp.dot(a, b, preferred_element_type=f32)


def mm_last(a, b):
    return lax.dot_general(a, b, (((1,), (1,)), ((), ())), preferred_element_type=f32)


def lanes_below(shape, limit):
    return lax.broadcasted_iota(jnp.int32, shape, 1) < limit


def params(*sem):
    return pltpu.CompilerParams(dimension_semantics=sem, vmem_limit_bytes=60 * 1024 * 1024)


def cost(flops, nbytes):
    return pl.CostEstimate(flops=int(flops), bytes_accessed=int(nbytes), transcendentals=0)


def expand_heads(row, heads):
    low = lanes_below((1, PAIR), HEAD)
    return [
        jnp.where(low, row[:, 2 * p : 2 * p + 1], row[:, 2 * p + 1 : 2 * p + 2])
        for p in range(heads // 2)
    ]


def states_kernel(
    x_ref, b_ref, c_ref, halo_ref, taps_ref, dtp_ref, spike_ref, off_ref, fade_ref,
    xs_ref, bs_ref, cs_ref, row_ref, send_ref, buf, state, total,
):
    step = pl.program_id(0)
    inner = x_ref.shape[1]
    group = b_ref.shape[1]
    heads = dtp_ref.shape[0]
    groups = group // STATE
    pairs = heads // groups // 2

    @pl.when(step == 0)
    def _():
        buf[0:8, :] = halo_ref[...].astype(f32)
        state[...] = jnp.zeros_like(state)
        total[...] = jnp.zeros_like(total)

    taps = taps_ref[...].astype(f32)
    for ref, out, base in ((x_ref, xs_ref, 0), (b_ref, bs_ref, inner), (c_ref, cs_ref, inner + group)):
        for j in range(0, ref.shape[1], 128):
            at = base + j
            cols = slice(at, at + 128)
            new = ref[:, j : j + 128].astype(f32)
            buf[8 : 8 + SPAN, cols] = new
            acc = new * taps[3:4, cols]
            for k in range(3):
                acc = acc + buf[5 + k : 5 + k + SPAN, cols] * taps[k : k + 1, cols]
            out[:, j : j + 128] = silu(acc).astype(bf16)
    buf[0:8, :] = buf[SPAN : SPAN + 8, :]

    diagonal = lax.broadcasted_iota(jnp.int32, (heads, heads), 0) == lax.broadcasted_iota(
        jnp.int32, (heads, heads), 1
    )

    def column(ref):
        return jnp.sum(jnp.where(diagonal, jnp.broadcast_to(ref[...], (heads, heads)), 0.0), axis=1, keepdims=True)

    pre = dtp_ref[...].astype(f32) + column(off_ref)
    dt = jnp.maximum(pre, 0.0) + jnp.log1p(jnp.exp(-jnp.abs(pre)))
    log_decay = (spike_ref[...] - jnp.exp(column(fade_ref)) * dt) * LOG2E
    upto = (
        lax.broadcasted_iota(jnp.int32, (SPAN, SPAN), 0)
        <= lax.broadcasted_iota(jnp.int32, (SPAN, SPAN), 1)
    ).astype(f32)
    cum = jnp.dot(log_decay, upto, precision=HIGHEST, preferred_element_type=f32)
    rows = cum - jnp.log2(dt)
    row_ref[0:heads, :] = rows
    row_ref[heads : 2 * heads, :] = cum
    factor = jnp.exp2(cum[:, SPAN - 1 : SPAN] - rows)
    end = jnp.concatenate([cum, jnp.zeros((128 - heads, SPAN), f32)], axis=0).T[SPAN - 1 : SPAN, 0:heads]
    total[...] = total[...] + jnp.concatenate(expand_heads(end, heads), axis=1)
    low = lanes_below((STATE, PAIR), HEAD)
    shrink = expand_heads(jnp.exp2(end), heads)
    for g in range(groups):
        bt = bs_ref[:, g * STATE : (g + 1) * STATE].astype(f32).T
        for p in range(pairs):
            q = g * pairs + p
            cols = slice(q * PAIR, (q + 1) * PAIR)
            left = jnp.concatenate(
                [bt * factor[2 * q : 2 * q + 1, :], bt * factor[2 * q + 1 : 2 * q + 2, :]], axis=0
            ).astype(bf16)
            res = mm(left, xs_ref[:, cols])
            state[:, cols] = state[:, cols] * shrink[q] + jnp.where(low, res[:STATE], res[STATE:])

    @pl.when(step == pl.num_programs(0) - 1)
    def _():
        half_cols = inner // 2
        t = total[0:1, :]
        hi = t.astype(bf16).astype(f32)
        mid = (t - hi).astype(bf16).astype(f32)
        tail = jnp.concatenate([hi, mid, t - hi - mid, jnp.zeros((5, inner), f32)], axis=0)
        for e in range(send_ref.shape[0]):
            rows_of, cols = slice(8 * (e // 2), 8 * (e // 2) + 8), slice(e % 2 * half_cols, (e % 2 + 1) * half_cols)
            send_ref[e] = jnp.concatenate([state[rows_of, cols], tail[:, cols]], axis=0).astype(bf16)


def place_of(device):
    return {"ep_0": device // 8, "ep_1": device // 2 % 4, "ep_2": device % 2}


def entering_kernel(msg_ref, out_ref, came, before, back, send_sem, recv_sem, send_sem2, recv_sem2):
    ep = msg_ref.shape[0]
    half_cols = msg_ref.shape[2]
    me = (lax.axis_index("ep_0") * 4 + lax.axis_index("ep_1")) * 2 + lax.axis_index("ep_2")
    barrier = pltpu.get_barrier_semaphore()

    @pl.loop(1, ep)
    def _(k):
        pl.semaphore_signal(
            barrier, inc=1, device_id=place_of((me + k) % ep), device_id_type=pl.DeviceIdType.MESH
        )

    pl.semaphore_wait(barrier, ep - 1)

    def there(k):
        to = (me + k) % ep
        return pltpu.make_async_remote_copy(
            src_ref=msg_ref.at[to], dst_ref=came.at[me], send_sem=send_sem.at[k], recv_sem=recv_sem.at[k],
            device_id=place_of(to), device_id_type=pl.DeviceIdType.MESH,
        )

    def returned(k):
        to = (me + k) % ep
        return pltpu.make_async_remote_copy(
            src_ref=before.at[to], dst_ref=back.at[me], send_sem=send_sem2.at[k], recv_sem=recv_sem2.at[k],
            device_id=place_of(to), device_id_type=pl.DeviceIdType.MESH,
        )

    @pl.loop(1, ep)
    def _(k):
        there(k).start()

    came[me] = msg_ref[me]

    @pl.loop(1, ep)
    def _(k):
        there(k).wait()

    running = jnp.zeros((8, half_cols), f32)
    for i in range(ep):
        before[i] = running.astype(bf16)
        block = came[i].astype(f32)
        running = running * jnp.exp2(block[8:9] + block[9:10] + block[10:11]) + block[0:8]

    @pl.loop(1, ep)
    def _(k):
        returned(k).start()

    back[me] = before[me]

    @pl.loop(1, ep)
    def _(k):
        returned(k).wait()

    for e in range(ep):
        out_ref[8 * (e // 2) : 8 * (e // 2) + 8, e % 2 * half_cols : (e % 2 + 1) * half_cols] = back[e].astype(f32)


def shifted(value, distance):
    return lax.ppermute(value, EP, [(i, i + distance) for i in range(lax.axis_size(EP) - distance)])


def entering_state(message):
    ep, _, half_cols = message.shape
    sems = pltpu.SemaphoreType.DMA((ep,))
    return pl.pallas_call(
        entering_kernel,
        in_specs=[pl.BlockSpec(memory_space=pltpu.VMEM)],
        out_specs=pl.BlockSpec(memory_space=pltpu.VMEM),
        out_shape=jax.ShapeDtypeStruct((STATE, 2 * half_cols), f32),
        scratch_shapes=[
            pltpu.VMEM((ep, 16, half_cols), bf16),
            pltpu.VMEM((ep, 8, half_cols), bf16),
            pltpu.VMEM((ep, 8, half_cols), bf16),
            sems, sems, sems, sems,
        ],
        compiler_params=pltpu.CompilerParams(collective_id=0, has_side_effects=True),
        cost_estimate=cost(1e10, 3e6),
        name="entering",
    )(message)


def mixer_kernel(
    xs_ref, bs_ref, cs_ref, z_ref, row_ref, enter_ref, skip_ref, gain_ref, w_ref,
    out_ref, state, gated, normed,
):
    step = pl.program_id(0)
    inner = xs_ref.shape[1]
    group = bs_ref.shape[1]
    heads = row_ref.shape[0] // 2
    groups = group // STATE
    pairs = heads // groups // 2
    wide = inner // groups

    @pl.when(step == 0)
    def _():
        state[...] = enter_ref[...]

    mask = lax.broadcasted_iota(jnp.int32, (SPAN, SPAN), 0) >= lax.broadcasted_iota(
        jnp.int32, (SPAN, SPAN), 1
    )
    low = lanes_below((STATE, PAIR), HEAD)
    skips = expand_heads(skip_ref[...], heads)
    rows = row_ref[0:heads, :]
    cum = jnp.concatenate(
        [row_ref[heads : 2 * heads, :], jnp.zeros((128 - heads, SPAN), f32)], axis=0
    ).T
    factor = jnp.exp2(row_ref[heads : 2 * heads, SPAN - 1 : SPAN] - rows)
    shrink = expand_heads(jnp.exp2(cum[SPAN - 1 : SPAN, 0:heads]), heads)
    for g in range(groups):
        gcols = slice(g * STATE, (g + 1) * STATE)
        bt = bs_ref[:, gcols].astype(f32).T
        cmat = cs_ref[:, gcols]
        c32 = cmat.astype(f32)
        scores = mm_last(cmat, bs_ref[:, gcols])
        squares = jnp.zeros((SPAN, PAIR), f32)
        for p in range(pairs):
            q = g * pairs + p
            cols = slice(q * PAIR, (q + 1) * PAIR)
            lefts, downs = [], []
            for h in (2 * q, 2 * q + 1):
                col = jnp.broadcast_to(cum[:, h : h + 1], (SPAN, SPAN))
                decay = jnp.exp2(jnp.where(mask, col - rows[h : h + 1, :], -1e30))
                lefts.append(
                    jnp.concatenate([(scores * decay).astype(bf16), (c32 * jnp.exp2(col)).astype(bf16)], axis=1)
                )
                downs.append((bt * factor[h : h + 1, :]).astype(bf16))
            xp = xs_ref[:, cols]
            sp = state[:, cols]
            res = mm(jnp.concatenate(lefts, axis=0), jnp.concatenate([xp, sp.astype(bf16)], axis=0))
            add = mm(jnp.concatenate(downs, axis=0), xp)
            state[:, cols] = sp * shrink[q] + jnp.where(low, add[:STATE], add[STATE:])
            y = jnp.where(low, res[:SPAN], res[SPAN:]) + xp.astype(f32) * skips[q]
            y = y * silu(z_ref[:, cols].astype(f32))
            gated[:, cols] = y
            squares = squares + y * y
        scale = lax.rsqrt(jnp.sum(squares, axis=1, keepdims=True) * (1.0 / wide) + norm_eps)
        wcols = slice(g * wide, (g + 1) * wide)
        normed[:, wcols] = (gated[:, wcols] * scale * gain_ref[:, wcols]).astype(bf16)
    out_ref[...] = mm(normed[...], w_ref[...]).astype(bf16)


def mixer_half(
    features, gating, insert, query, presoftplus, entry_taps, insert_taps, query_taps,
    offset, fading, skip, spike, gain, projection,
):
    rows, inner = features.shape
    group = insert.shape[1]
    heads = offset.shape[0]
    width = projection.shape[1]
    every = inner + 2 * group
    ep = lax.axis_size(EP)
    last = jnp.concatenate([a[rows - 8 :] for a in (features, insert, query)], axis=1)
    halo = shifted(last, 1)
    taps = jnp.concatenate([entry_taps, insert_taps, query_taps], axis=1)
    steps = rows // SPAN

    def block(n):
        return pl.BlockSpec((SPAN, n), lambda i: (i, 0))

    def whole(*shape):
        return pl.BlockSpec(shape, lambda i: (0,) * len(shape))

    def across(n):
        return pl.BlockSpec((n, SPAN), lambda i: (0, i))

    xs, bs, cs, row, message = pl.pallas_call(
        states_kernel,
        grid=(steps,),
        in_specs=[
            block(inner), block(group), block(group), whole(8, every), whole(4, every),
            across(heads), across(heads), whole(1, heads), whole(1, heads),
        ],
        out_specs=[
            block(inner), block(group), block(group), across(2 * heads),
            whole(ep, 16, inner // 2),
        ],
        out_shape=[
            jax.ShapeDtypeStruct((rows, inner), bf16),
            jax.ShapeDtypeStruct((rows, group), bf16),
            jax.ShapeDtypeStruct((rows, group), bf16),
            jax.ShapeDtypeStruct((2 * heads, rows), f32),
            jax.ShapeDtypeStruct((ep, 16, inner // 2), bf16),
        ],
        scratch_shapes=[
            pltpu.VMEM((SPAN + 8, every), f32),
            pltpu.VMEM((STATE, inner), f32),
            pltpu.VMEM((1, inner), f32),
        ],
        compiler_params=params("arbitrary"),
        cost_estimate=cost(8e9, 1e7),
        name="states",
    )(
        features, insert, query, halo, taps, presoftplus.T, spike.T,
        offset.reshape(1, heads), fading.reshape(1, heads),
    )
    entering = entering_state(message)
    partial = pl.pallas_call(
        mixer_kernel,
        grid=(steps,),
        in_specs=[
            block(inner), block(group), block(group), block(inner), across(2 * heads),
            whole(STATE, inner), whole(1, heads), whole(1, inner), whole(inner, width),
        ],
        out_specs=block(width),
        out_shape=jax.ShapeDtypeStruct((rows, width), bf16),
        scratch_shapes=[
            pltpu.VMEM((STATE, inner), f32),
            pltpu.VMEM((SPAN, inner), f32),
            pltpu.VMEM((SPAN, inner), bf16),
        ],
        compiler_params=params("arbitrary"),
        cost_estimate=cost(2e10, 2e7),
        name="mixer",
    )(
        xs, bs, cs, gating, row, entering,
        skip.reshape(1, heads), gain.reshape(1, inner), projection,
    )
    return lax.psum_scatter(partial, "tp", scatter_dimension=0, tiled=True)


FIRST = 16
SECOND = 40
OTHERS = 36


def second_slot(inside):
    other = inside < OTHERS
    return (
        jnp.where(other, inside // EARLY + 1, 0),
        jnp.where(other, inside % EARLY + LATE, inside - OTHERS + FIRST),
    )


def expert_of(rows, first, per, experts):
    at = lax.broadcasted_iota(jnp.int32, (rows, experts), 0) + first
    return (at // per == lax.broadcasted_iota(jnp.int32, (rows, experts), 1)).astype(bf16)


def route_kernel(x_ref, gain_ref, pick_ref, score_ref, token_ref, first_ref):
    tokens, width = x_ref.shape
    experts = first_ref.shape[0] // FIRST
    x = x_ref[...].astype(f32)
    x = x - jnp.mean(x, axis=1, keepdims=True)
    x = x * lax.rsqrt(jnp.mean(x * x, axis=1, keepdims=True) + norm_eps) * gain_ref[...]
    normed = x.astype(bf16)
    token_ref[:, 0:width] = normed
    weight = jnp.exp(score_ref[...])
    weight = weight / jnp.sum(weight, axis=0, keepdims=True)
    lane = lax.broadcasted_iota(jnp.int32, (experts, tokens), 0)
    taken = jnp.zeros((experts, tokens), f32)
    dense = jnp.zeros((experts, tokens), f32)
    for k in range(pick_ref.shape[0]):
        hit = pick_ref[k : k + 1, :] == lane
        taken = jnp.where(hit, 1.0, taken)
        dense = jnp.where(hit, weight[k : k + 1, :], dense)
    earlier = (
        lax.broadcasted_iota(jnp.int32, (tokens, tokens), 0)
        < lax.broadcasted_iota(jnp.int32, (tokens, tokens), 1)
    ).astype(bf16)
    slot = jnp.where(taken > 0, mm(taken.astype(bf16), earlier), -1.0)
    token_ref[:, width : width + 128] = jnp.concatenate(
        [slot, dense, jnp.zeros((128 - 2 * experts, tokens), f32)], axis=0
    ).T.astype(bf16)
    rows = experts * FIRST
    spread = mm(expert_of(rows, 0, FIRST, experts), slot.astype(bf16))
    wanted = lax.broadcasted_iota(jnp.int32, (rows, 1), 0) % FIRST
    first_ref[...] = mm((spread == wanted.astype(f32)).astype(bf16), normed).astype(bf16)


def second_kernel(table_ref, apart_ref, out_ref, *, experts):
    width = table_ref.shape[1] - 128
    rows = out_ref.shape[0]
    first = pl.program_id(0) * rows
    spread = mm_last(expert_of(rows, first, SECOND, experts), table_ref[:, width : width + experts])
    at = lax.broadcasted_iota(jnp.int32, (rows, 1), 0) + first
    block, wanted = second_slot(at % SECOND)
    hit = (spread == wanted.astype(f32)) & (apart_ref[...] == block)
    out_ref[...] = mm(hit.astype(bf16), table_ref[:, 0:width]).astype(bf16)


def expert_kernel(x_ref, gate_ref, up_ref, down_ref, out_ref):
    x = x_ref[...]
    g = jnp.minimum(mm(x, gate_ref[...]), clamp_top)
    u = jnp.clip(mm(x, up_ref[...]), -clamp_top, clamp_top) + 1.0
    act = g * (0.5 + 0.5 * jnp.tanh((0.5 * sigmoid_sharp) * g)) * u
    out_ref[...] = mm(act.astype(bf16), down_ref[...]).astype(bf16)


def expert(rows_in, gate, up, down):
    rows, width = rows_in.shape
    hidden = gate.shape[2]
    return pl.pallas_call(
        expert_kernel,
        grid=(rows // ROW_TILE,),
        in_specs=[
            pl.BlockSpec((ROW_TILE, width), lambda i: (i, 0)),
            pl.BlockSpec((None, width, hidden), lambda i: (0, 0, 0)),
            pl.BlockSpec((None, width, hidden), lambda i: (0, 0, 0)),
            pl.BlockSpec((None, hidden, width), lambda i: (0, 0, 0)),
        ],
        out_specs=pl.BlockSpec((ROW_TILE, width), lambda i: (i, 0)),
        out_shape=jax.ShapeDtypeStruct((rows, width), bf16),
        compiler_params=params("arbitrary"),
        cost_estimate=cost(6 * rows * width * hidden, 3 * 2 * width * hidden + 4 * rows * width),
        name="expert",
    )(rows_in, gate, up, down)


def joint_kernel(
    rows_hbm, late_hbm, own_ref, tags_ref, gate_hbm, up_hbm, down_hbm, out_ref,
    rows, gate, up, down, res, back, late_own, mid_own, mid, mid_sum, from_left, from_right,
    late_sum, late_back, own_back, pick, pick_first, part, part_mid, part_sum, part_left, part_right,
    load_sem, weight_sem, late_load, send_sem, recv_sem, share_send, share_recv,
    late_send, late_recv, own_send, own_recv, part_send, part_recv,
):
    ep, per, width = res.shape
    experts = ep
    tokens = out_ref.shape[0]
    blocks = tags_ref.shape[0] // tokens
    col_tile = part.shape[3]
    z, y, core = lax.axis_index("ep_0"), lax.axis_index("ep_1"), lax.axis_index("ep_2")
    tp = lax.axis_index("tp")
    me = (z * 4 + y) * 2 + core
    mesh_ids = pl.DeviceIdType.MESH

    def place(k):
        return (z + k // 2) % 4, (y + k // 8 + k // 2) % 4, (core + k) % 2

    def index(k):
        a, b, c = place(k)
        return (a * 4 + b) * 2 + c

    def device(k):
        a, b, c = place(k)
        return {"ep_0": a, "ep_1": b, "ep_2": c}

    def load(k):
        return pltpu.make_async_copy(rows_hbm.at[index(k)], rows.at[k], load_sem.at[k])

    def weights():
        return [
            pltpu.make_async_copy(src, dst, weight_sem.at[n])
            for n, (src, dst) in enumerate(((gate_hbm, gate), (up_hbm, up), (down_hbm, down)))
        ]

    def give_back(k):
        return pltpu.make_async_remote_copy(
            src_ref=res.at[k], dst_ref=back.at[me], send_sem=send_sem.at[k], recv_sem=recv_sem.at[k],
            device_id=device(k), device_id_type=mesh_ids,
        )

    def give_late(k):
        return pltpu.make_async_remote_copy(
            src_ref=late_sum.at[index(k)], dst_ref=late_back.at[me],
            send_sem=late_send.at[k], recv_sem=late_recv.at[k],
            device_id=device(k), device_id_type=mesh_ids,
        )

    def give_own(k):
        return pltpu.make_async_remote_copy(
            src_ref=own_ref.at[index(k)], dst_ref=own_back.at[me],
            send_sem=own_send.at[k], recv_sem=own_recv.at[k],
            device_id=device(k), device_id_type=mesh_ids,
        )

    half = ep // 2
    parts = (pl.ds(0, half), pl.ds(half, half))
    sides = (1, blocks - 1)
    opposite = (tp + 2) % blocks

    def along(side, src, dst, send, recv):
        return pltpu.make_async_remote_copy(
            src_ref=src, dst_ref=dst, send_sem=send, recv_sem=recv,
            device_id={"tp": (tp + sides[side]) % blocks}, device_id_type=mesh_ids,
        )

    def share(stage, side):
        owner = (tp + sides[side]) % blocks
        landing = (from_left, from_right)[side]
        if stage == 0:
            src, dst = late_hbm.at[opposite, parts[side]], mid.at[side]
        elif stage == 1:
            src, dst = late_hbm.at[owner, parts[1 - side]], landing.at[parts[1 - side]]
        else:
            src, dst = mid_sum.at[side], landing.at[parts[side]]
        return along(side, src, dst, share_send.at[stage, side], share_recv.at[stage, side])

    def own_loads():
        return [pltpu.make_async_copy(late_hbm.at[tp], late_own, late_load.at[2])] + [
            pltpu.make_async_copy(
                late_hbm.at[(tp + sides[n]) % blocks, parts[n]], mid_own.at[n], late_load.at[n]
            )
            for n in range(2)
        ]

    tiles = part.shape[0]

    def side_of(t):
        return 0 if t < tiles // 2 else 1

    def give_part(stage, t):
        side = side_of(t) if stage != 1 else 1 - side_of(t)
        landing = (part_left, part_right)[side]
        if stage == 0:
            src, dst = part.at[t, 2], part_mid.at[t]
        elif stage == 1:
            src, dst = part.at[t, sides[side]], landing.at[t]
        else:
            src, dst = part_sum.at[t], landing.at[t]
        return along(side, src, dst, part_send.at[stage, t], part_recv.at[stage, t])

    for w in weights():
        w.start()

    @pl.loop(0, ep)
    def _(k):
        load(k).start()

    barrier = pltpu.get_barrier_semaphore()

    @pl.loop(1, ep)
    def _(k):
        pl.semaphore_signal(barrier, inc=1, device_id=device(k), device_id_type=mesh_ids)

    for r in sides:
        pl.semaphore_signal(
            barrier, inc=1, device_id={"tp": (tp + r) % blocks}, device_id_type=mesh_ids
        )
    pl.semaphore_wait(barrier, ep - 1 + len(sides))

    for stage in range(2):
        for side in range(2):
            share(stage, side).start()
    for load_own in own_loads():
        load_own.start()

    for w in weights():
        w.wait()

    group = 8

    @pl.loop(0, ep // group)
    def _(c):
        @pl.loop(0, group)
        def _(j):
            load(c * group + j).wait()

        x = rows[pl.ds(c * group, group)].reshape(group * per, width)
        g = jnp.minimum(mm(x, gate[...]), clamp_top)
        u = jnp.clip(mm(x, up[...]), -clamp_top, clamp_top) + 1.0
        act = (g * (0.5 + 0.5 * jnp.tanh((0.5 * sigmoid_sharp) * g)) * u).astype(bf16)
        res[pl.ds(c * group, group)] = mm(act, down[...]).astype(bf16).reshape(group, per, width)

        @pl.loop(0, group)
        def _(j):
            @pl.when(c * group + j > 0)
            def _():
                give_back(c * group + j).start()

    @pl.loop(1, ep)
    def _(k):
        give_own(k).start()

    back[me] = res[0]
    own_back[me] = own_ref[me]

    for load_own in own_loads():
        load_own.wait()
    for side in range(2):
        share(0, side).wait_recv()

        @pl.loop(0, half)
        def _(k):
            mid_sum[side, k] = (mid_own[side, k].astype(f32) + mid[side, k].astype(f32)).astype(bf16)

        share(2, side).start()

    count = experts * per
    chosen = expert_of(count, 0, per, experts)
    block, wanted = second_slot(lax.broadcasted_iota(jnp.int32, (1, count), 1) % per)
    for r in range(blocks):
        q = (tp + r) % blocks
        table = tags_ref[pl.ds(pl.multiple_of(q * tokens, tokens), tokens), :]
        slot = mm_last(table[:, 0:experts], chosen)
        weight = mm_last(table[:, experts : 2 * experts], chosen)
        hit = (slot == wanted.astype(f32)) & (block == r)
        pick[r * tokens : (r + 1) * tokens, :] = jnp.where(hit, weight, 0.0).astype(bf16)
    own = tags_ref[pl.ds(pl.multiple_of(tp * tokens, tokens), tokens), :]
    chosen = expert_of(experts * LATE, 0, LATE, experts)
    slot = mm_last(own[:, 0:experts], chosen)
    weight = mm_last(own[:, experts : 2 * experts], chosen)
    at = lax.broadcasted_iota(jnp.int32, (1, experts * LATE), 1) % LATE
    for n in range(FIRST // LATE):
        hit = slot == (at + n * LATE).astype(f32)
        pick_first[n] = jnp.where(hit, weight, 0.0).astype(bf16)

    for stage in (1, 2):
        for side in range(2):
            share(stage, side).wait_recv()

    @pl.loop(0, ep)
    def _(k):
        total = from_left[k].astype(f32) + from_right[k].astype(f32)
        late_sum[k] = (total + late_own[k].astype(f32)).astype(bf16)

    @pl.loop(1, ep)
    def _(k):
        give_late(k).start()

    late_back[me] = late_sum[me]

    @pl.loop(1, ep)
    def _(k):
        give_back(k).wait_recv()

    for t in range(tiles):
        cols = slice(t * col_tile, (t + 1) * col_tile)
        got = mm(pick[...], back[:, :, cols].reshape(count, col_tile)).astype(bf16)
        part[t] = got.reshape(blocks, tokens, col_tile)
        give_part(0, t).start()
        give_part(1, t).start()

    for t in range(tiles):
        give_part(0, t).wait_recv()
        own_part = part[t, sides[side_of(t)]].astype(f32)
        part_sum[t] = (own_part + part_mid[t].astype(f32)).astype(bf16)
        give_part(2, t).start()

    @pl.loop(1, ep)
    def _(k):
        give_own(k).wait_recv()
        give_late(k).wait_recv()

    for t in range(tiles):
        cols = slice(t * col_tile, (t + 1) * col_tile)
        total = part[t, 0].astype(f32)
        for n, ref in enumerate((late_back, own_back)):
            total = total + mm(pick_first[n], ref[:, :, cols].reshape(experts * LATE, col_tile))
        for stage in (1, 2):
            give_part(stage, t).wait_recv()
        total = total + part_left[t].astype(f32) + part_right[t].astype(f32)
        out_ref[:, cols] = total.astype(bf16)

    @pl.loop(1, ep)
    def _(k):
        give_back(k).wait_send()
        give_own(k).wait_send()
        give_late(k).wait_send()

    for stage in range(3):
        for side in range(2):
            share(stage, side).wait_send()
        for t in range(tiles):
            give_part(stage, t).wait_send()


def joint(second_in, late_part, own_part, tags, gate, up, down, tokens):
    ep, per, width = second_in.shape
    hidden = gate.shape[1]
    blocks = tags.shape[0] // tokens
    tiles = width // 512
    any_ref = pl.BlockSpec(memory_space=pl.ANY)
    vmem = pl.BlockSpec(memory_space=pltpu.VMEM)
    dma = pltpu.SemaphoreType.DMA
    return pl.pallas_call(
        joint_kernel,
        in_specs=[any_ref, any_ref, vmem, vmem, any_ref, any_ref, any_ref],
        out_specs=vmem,
        out_shape=jax.ShapeDtypeStruct((tokens, width), bf16),
        scratch_shapes=[
            pltpu.VMEM((ep, per, width), bf16),
            pltpu.VMEM((width, hidden), bf16),
            pltpu.VMEM((width, hidden), bf16),
            pltpu.VMEM((hidden, width), bf16),
            pltpu.VMEM((ep, per, width), bf16),
            pltpu.VMEM((ep, per, width), bf16),
            pltpu.VMEM((ep, LATE, width), bf16),
            pltpu.VMEM((2, ep // 2, LATE, width), bf16),
            pltpu.VMEM((2, ep // 2, LATE, width), bf16),
            pltpu.VMEM((2, ep // 2, LATE, width), bf16),
            pltpu.VMEM((ep, LATE, width), bf16),
            pltpu.VMEM((ep, LATE, width), bf16),
            pltpu.VMEM((ep, LATE, width), bf16),
            pltpu.VMEM((ep, LATE, width), bf16),
            pltpu.VMEM((ep, LATE, width), bf16),
            pltpu.VMEM((blocks * tokens, ep * per), bf16),
            pltpu.VMEM((FIRST // LATE, tokens, ep * LATE), bf16),
            pltpu.VMEM((tiles, blocks, tokens, 512), bf16),
            pltpu.VMEM((tiles, tokens, 512), bf16),
            pltpu.VMEM((tiles, tokens, 512), bf16),
            pltpu.VMEM((tiles, tokens, 512), bf16),
            pltpu.VMEM((tiles, tokens, 512), bf16),
            dma((ep,)), dma((3,)), dma((3,)), dma((ep,)), dma((ep,)), dma((3, 2)), dma((3, 2)),
            dma((ep,)), dma((ep,)), dma((ep,)), dma((ep,)),
            dma((3, tiles)), dma((3, tiles)),
        ],
        compiler_params=pltpu.CompilerParams(
            collective_id=1, has_side_effects=True, vmem_limit_bytes=60 * 1024 * 1024
        ),
        cost_estimate=cost(4e10, 3e7),
        name="joint",
    )(second_in, late_part, own_part, tags, gate, up, down)


def exchanged(value):
    return lax.all_to_all(value, EP, split_axis=0, concat_axis=0, tiled=True)


def experts_half(sample, gain, pick, score, gate, up, down):
    tokens, width = sample.shape
    experts = lax.axis_size(EP)
    blocks = lax.axis_size("tp")
    every = width + 128
    own, first_out = pl.pallas_call(
        route_kernel,
        out_shape=[
            jax.ShapeDtypeStruct((tokens, every), bf16),
            jax.ShapeDtypeStruct((experts * FIRST, width), bf16),
        ],
        compiler_params=params(),
        cost_estimate=cost(1e9, 3e6),
        name="route",
    )(sample, gain.reshape(1, width), pick.T, score.T)
    apart = (jnp.arange(blocks * tokens, dtype=jnp.int32) // tokens - lax.axis_index("tp")) % blocks
    table = lax.all_gather(own, "tp", axis=0, tiled=True)
    first_in = exchanged(first_out.reshape(experts, FIRST, width))
    late_rows = lax.all_gather(first_in[:, :LATE], "tp", axis=0, tiled=True).reshape(-1, width)

    count = experts * SECOND
    tile = count // 4
    second_out = pl.pallas_call(
        functools.partial(second_kernel, experts=experts),
        grid=(count // tile,),
        in_specs=[
            pl.BlockSpec((blocks * tokens, every), lambda i: (0, 0)),
            pl.BlockSpec((1, blocks * tokens), lambda i: (0, 0)),
        ],
        out_specs=pl.BlockSpec((tile, width), lambda i: (i, 0)),
        out_shape=jax.ShapeDtypeStruct((count, width), bf16),
        compiler_params=params("arbitrary"),
        cost_estimate=cost(3.2e9, 1e7),
        name="second",
    )(table, apart.reshape(1, -1))
    second_in = exchanged(second_out.reshape(experts, SECOND, width))

    late_part = expert(late_rows, gate, up, down)
    own_part = expert(first_in[:, LATE:].reshape(-1, width), gate, up, down)
    return joint(
        second_in, late_part.reshape(blocks, experts, LATE, width),
        own_part.reshape(experts, FIRST - LATE, width), table[:, width:], gate[0], up[0], down[0], tokens,
    )


def body(*args):
    moe_out = experts_half(*args[14:])
    mixed = mixer_half(*args[:14])
    return (mixed, moe_out)


def solution(mesh):
    split = Mesh(mesh.devices.reshape(4, 4, 2, mesh.shape["tp"]), ("ep_0", "ep_1", "ep_2", "tp"))
    return jax.shard_map(
        body,
        mesh=split,
        in_specs=(
            P(EP, "tp"),
            P(EP, "tp"),
            P(EP, "tp"),
            P(EP, "tp"),
            P(EP, "tp"),
            P(None, "tp"),
            P(None, "tp"),
            P(None, "tp"),
            P("tp"),
            P("tp"),
            P("tp"),
            P(EP, "tp"),
            P("tp"),
            P("tp", None),
            P(EP_TP, None),
            P(),
            P(EP_TP, None),
            P(EP_TP, None),
            P(EP, None, "tp"),
            P(EP, None, "tp"),
            P(EP, "tp", None),
        ),
        out_specs=(P(EP_TP, None), P(EP_TP, None)),
        check_vma=False,
    )
```

```python
import functools

import jax
import jax.numpy as jnp
from jax import lax
from jax.experimental import pallas as pl
from jax.experimental.pallas import tpu as pltpu
from jax.sharding import Mesh
from jax.sharding import PartitionSpec as P


HEAD = 64
STATE = 128
SPAN = 128
PAIR = 2 * HEAD
CAP = 20
LATE = 8
EARLY = CAP - LATE
ROW_TILE = 256
EP = ("ep_0", "ep_1", "ep_2")
EP_TP = ("ep_0", "ep_1", "ep_2", "tp")

norm_eps = 1e-05
clamp_top = 7.0
sigmoid_sharp = 1.702
LOG2E = 1.4426950408889634
HIGHEST = lax.Precision.HIGHEST
f32 = jnp.float32
bf16 = jnp.bfloat16


def silu(v):
    half = 0.5 * v
    return half + half * jnp.tanh(half)


def mm(a, b):
    return jnp.dot(a, b, preferred_element_type=f32)


def mm_last(a, b):
    return lax.dot_general(a, b, (((1,), (1,)), ((), ())), preferred_element_type=f32)


def lanes_below(shape, limit):
    return lax.broadcasted_iota(jnp.int32, shape, 1) < limit


def params(*sem):
    return pltpu.CompilerParams(dimension_semantics=sem, vmem_limit_bytes=60 * 1024 * 1024)


def cost(flops, nbytes):
    return pl.CostEstimate(flops=int(flops), bytes_accessed=int(nbytes), transcendentals=0)


def expand_heads(row, heads):
    low = lanes_below((1, PAIR), HEAD)
    return [
        jnp.where(low, row[:, 2 * p : 2 * p + 1], row[:, 2 * p + 1 : 2 * p + 2])
        for p in range(heads // 2)
    ]


def states_kernel(
    x_ref, b_ref, c_ref, halo_ref, taps_ref, dtp_ref, spike_ref, off_ref, fade_ref,
    xs_ref, bs_ref, cs_ref, row_ref, send_ref, buf, state, total,
):
    step = pl.program_id(0)
    inner = x_ref.shape[1]
    group = b_ref.shape[1]
    heads = dtp_ref.shape[0]
    groups = group // STATE
    pairs = heads // groups // 2

    @pl.when(step == 0)
    def _():
        buf[0:8, :] = halo_ref[...].astype(f32)
        state[...] = jnp.zeros_like(state)
        total[...] = jnp.zeros_like(total)

    taps = taps_ref[...].astype(f32)
    for ref, out, base in ((x_ref, xs_ref, 0), (b_ref, bs_ref, inner), (c_ref, cs_ref, inner + group)):
        for j in range(0, ref.shape[1], 128):
            at = base + j
            cols = slice(at, at + 128)
            new = ref[:, j : j + 128].astype(f32)
            buf[8 : 8 + SPAN, cols] = new
            acc = new * taps[3:4, cols]
            for k in range(3):
                acc = acc + buf[5 + k : 5 + k + SPAN, cols] * taps[k : k + 1, cols]
            out[:, j : j + 128] = silu(acc).astype(bf16)
    buf[0:8, :] = buf[SPAN : SPAN + 8, :]

    diagonal = lax.broadcasted_iota(jnp.int32, (heads, heads), 0) == lax.broadcasted_iota(
        jnp.int32, (heads, heads), 1
    )

    def column(ref):
        return jnp.sum(jnp.where(diagonal, jnp.broadcast_to(ref[...], (heads, heads)), 0.0), axis=1, keepdims=True)

    pre = dtp_ref[...].astype(f32) + column(off_ref)
    dt = jnp.maximum(pre, 0.0) + jnp.log1p(jnp.exp(-jnp.abs(pre)))
    log_decay = (spike_ref[...] - jnp.exp(column(fade_ref)) * dt) * LOG2E
    upto = (
        lax.broadcasted_iota(jnp.int32, (SPAN, SPAN), 0)
        <= lax.broadcasted_iota(jnp.int32, (SPAN, SPAN), 1)
    ).astype(f32)
    cum = jnp.dot(log_decay, upto, precision=HIGHEST, preferred_element_type=f32)
    rows = cum - jnp.log2(dt)
    row_ref[0:heads, :] = rows
    row_ref[heads : 2 * heads, :] = cum
    factor = jnp.exp2(cum[:, SPAN - 1 : SPAN] - rows)
    end = jnp.concatenate([cum, jnp.zeros((128 - heads, SPAN), f32)], axis=0).T[SPAN - 1 : SPAN, 0:heads]
    total[...] = total[...] + jnp.concatenate(expand_heads(end, heads), axis=1)
    low = lanes_below((STATE, PAIR), HEAD)
    shrink = expand_heads(jnp.exp2(end), heads)
    for g in range(groups):
        bt = bs_ref[:, g * STATE : (g + 1) * STATE].astype(f32).T
        for p in range(pairs):
            q = g * pairs + p
            cols = slice(q * PAIR, (q + 1) * PAIR)
            left = jnp.concatenate(
                [bt * factor[2 * q : 2 * q + 1, :], bt * factor[2 * q + 1 : 2 * q + 2, :]], axis=0
            ).astype(bf16)
            res = mm(left, xs_ref[:, cols])
            state[:, cols] = state[:, cols] * shrink[q] + jnp.where(low, res[:STATE], res[STATE:])

    @pl.when(step == pl.num_programs(0) - 1)
    def _():
        half_cols = inner // 2
        t = total[0:1, :]
        hi = t.astype(bf16).astype(f32)
        mid = (t - hi).astype(bf16).astype(f32)
        tail = jnp.concatenate([hi, mid, t - hi - mid, jnp.zeros((5, inner), f32)], axis=0)
        for e in range(send_ref.shape[0]):
            rows_of, cols = slice(8 * (e // 2), 8 * (e // 2) + 8), slice(e % 2 * half_cols, (e % 2 + 1) * half_cols)
            send_ref[e] = jnp.concatenate([state[rows_of, cols], tail[:, cols]], axis=0).astype(bf16)


def place_of(device):
    return {"ep_0": device // 8, "ep_1": device // 2 % 4, "ep_2": device % 2}


def entering_kernel(msg_ref, out_ref, came, before, back, send_sem, recv_sem, send_sem2, recv_sem2):
    ep = msg_ref.shape[0]
    half_cols = msg_ref.shape[2]
    me = (lax.axis_index("ep_0") * 4 + lax.axis_index("ep_1")) * 2 + lax.axis_index("ep_2")
    barrier = pltpu.get_barrier_semaphore()

    @pl.loop(1, ep)
    def _(k):
        pl.semaphore_signal(
            barrier, inc=1, device_id=place_of((me + k) % ep), device_id_type=pl.DeviceIdType.MESH
        )

    pl.semaphore_wait(barrier, ep - 1)

    def there(k):
        to = (me + k) % ep
        return pltpu.make_async_remote_copy(
            src_ref=msg_ref.at[to], dst_ref=came.at[me], send_sem=send_sem.at[k], recv_sem=recv_sem.at[k],
            device_id=place_of(to), device_id_type=pl.DeviceIdType.MESH,
        )

    def returned(k):
        to = (me + k) % ep
        return pltpu.make_async_remote_copy(
            src_ref=before.at[to], dst_ref=back.at[me], send_sem=send_sem2.at[k], recv_sem=recv_sem2.at[k],
            device_id=place_of(to), device_id_type=pl.DeviceIdType.MESH,
        )

    @pl.loop(1, ep)
    def _(k):
        there(k).start()

    came[me] = msg_ref[me]

    @pl.loop(1, ep)
    def _(k):
        there(k).wait()

    running = jnp.zeros((8, half_cols), f32)
    for i in range(ep):
        before[i] = running.astype(bf16)
        block = came[i].astype(f32)
        running = running * jnp.exp2(block[8:9] + block[9:10] + block[10:11]) + block[0:8]

    @pl.loop(1, ep)
    def _(k):
        returned(k).start()

    back[me] = before[me]

    @pl.loop(1, ep)
    def _(k):
        returned(k).wait()

    for e in range(ep):
        out_ref[8 * (e // 2) : 8 * (e // 2) + 8, e % 2 * half_cols : (e % 2 + 1) * half_cols] = back[e].astype(f32)


def shifted(value, distance):
    return lax.ppermute(value, EP, [(i, i + distance) for i in range(lax.axis_size(EP) - distance)])


def entering_state(message):
    ep, _, half_cols = message.shape
    sems = pltpu.SemaphoreType.DMA((ep,))
    return pl.pallas_call(
        entering_kernel,
        in_specs=[pl.BlockSpec(memory_space=pltpu.VMEM)],
        out_specs=pl.BlockSpec(memory_space=pltpu.VMEM),
        out_shape=jax.ShapeDtypeStruct((STATE, 2 * half_cols), f32),
        scratch_shapes=[
            pltpu.VMEM((ep, 16, half_cols), bf16),
            pltpu.VMEM((ep, 8, half_cols), bf16),
            pltpu.VMEM((ep, 8, half_cols), bf16),
            sems, sems, sems, sems,
        ],
        compiler_params=pltpu.CompilerParams(collective_id=0, has_side_effects=True),
        cost_estimate=cost(1e10, 3e6),
        name="entering",
    )(message)


def mixer_kernel(
    xs_ref, bs_ref, cs_ref, z_ref, row_ref, enter_ref, skip_ref, gain_ref, w_ref,
    out_ref, state, gated, normed,
):
    step = pl.program_id(0)
    inner = xs_ref.shape[1]
    group = bs_ref.shape[1]
    heads = row_ref.shape[0] // 2
    groups = group // STATE
    pairs = heads // groups // 2
    wide = inner // groups

    @pl.when(step == 0)
    def _():
        state[...] = enter_ref[...]

    mask = lax.broadcasted_iota(jnp.int32, (SPAN, SPAN), 0) >= lax.broadcasted_iota(
        jnp.int32, (SPAN, SPAN), 1
    )
    low = lanes_below((STATE, PAIR), HEAD)
    skips = expand_heads(skip_ref[...], heads)
    rows = row_ref[0:heads, :]
    cum = jnp.concatenate(
        [row_ref[heads : 2 * heads, :], jnp.zeros((128 - heads, SPAN), f32)], axis=0
    ).T
    factor = jnp.exp2(row_ref[heads : 2 * heads, SPAN - 1 : SPAN] - rows)
    shrink = expand_heads(jnp.exp2(cum[SPAN - 1 : SPAN, 0:heads]), heads)
    for g in range(groups):
        gcols = slice(g * STATE, (g + 1) * STATE)
        bt = bs_ref[:, gcols].astype(f32).T
        cmat = cs_ref[:, gcols]
        c32 = cmat.astype(f32)
        scores = mm_last(cmat, bs_ref[:, gcols])
        squares = jnp.zeros((SPAN, PAIR), f32)
        for p in range(pairs):
            q = g * pairs + p
            cols = slice(q * PAIR, (q + 1) * PAIR)
            lefts, downs = [], []
            for h in (2 * q, 2 * q + 1):
                col = jnp.broadcast_to(cum[:, h : h + 1], (SPAN, SPAN))
                decay = jnp.exp2(jnp.where(mask, col - rows[h : h + 1, :], -1e30))
                lefts.append(
                    jnp.concatenate([(scores * decay).astype(bf16), (c32 * jnp.exp2(col)).astype(bf16)], axis=1)
                )
                downs.append((bt * factor[h : h + 1, :]).astype(bf16))
            xp = xs_ref[:, cols]
            sp = state[:, cols]
            res = mm(jnp.concatenate(lefts, axis=0), jnp.concatenate([xp, sp.astype(bf16)], axis=0))
            add = mm(jnp.concatenate(downs, axis=0), xp)
            state[:, cols] = sp * shrink[q] + jnp.where(low, add[:STATE], add[STATE:])
            y = jnp.where(low, res[:SPAN], res[SPAN:]) + xp.astype(f32) * skips[q]
            y = y * silu(z_ref[:, cols].astype(f32))
            gated[:, cols] = y
            squares = squares + y * y
        scale = lax.rsqrt(jnp.sum(squares, axis=1, keepdims=True) * (1.0 / wide) + norm_eps)
        wcols = slice(g * wide, (g + 1) * wide)
        normed[:, wcols] = (gated[:, wcols] * scale * gain_ref[:, wcols]).astype(bf16)
    out_ref[...] = mm(normed[...], w_ref[...]).astype(bf16)


def mixer_half(
    features, gating, insert, query, presoftplus, entry_taps, insert_taps, query_taps,
    offset, fading, skip, spike, gain, projection,
):
    rows, inner = features.shape
    group = insert.shape[1]
    heads = offset.shape[0]
    width = projection.shape[1]
    every = inner + 2 * group
    ep = lax.axis_size(EP)
    last = jnp.concatenate([a[rows - 8 :] for a in (features, insert, query)], axis=1)
    halo = shifted(last, 1)
    taps = jnp.concatenate([entry_taps, insert_taps, query_taps], axis=1)
    steps = rows // SPAN

    def block(n):
        return pl.BlockSpec((SPAN, n), lambda i: (i, 0))

    def whole(*shape):
        return pl.BlockSpec(shape, lambda i: (0,) * len(shape))

    def across(n):
        return pl.BlockSpec((n, SPAN), lambda i: (0, i))

    xs, bs, cs, row, message = pl.pallas_call(
        states_kernel,
        grid=(steps,),
        in_specs=[
            block(inner), block(group), block(group), whole(8, every), whole(4, every),
            across(heads), across(heads), whole(1, heads), whole(1, heads),
        ],
        out_specs=[
            block(inner), block(group), block(group), across(2 * heads),
            whole(ep, 16, inner // 2),
        ],
        out_shape=[
            jax.ShapeDtypeStruct((rows, inner), bf16),
            jax.ShapeDtypeStruct((rows, group), bf16),
            jax.ShapeDtypeStruct((rows, group), bf16),
            jax.ShapeDtypeStruct((2 * heads, rows), f32),
            jax.ShapeDtypeStruct((ep, 16, inner // 2), bf16),
        ],
        scratch_shapes=[
            pltpu.VMEM((SPAN + 8, every), f32),
            pltpu.VMEM((STATE, inner), f32),
            pltpu.VMEM((1, inner), f32),
        ],
        compiler_params=params("arbitrary"),
        cost_estimate=cost(8e9, 1e7),
        name="states",
    )(
        features, insert, query, halo, taps, presoftplus.T, spike.T,
        offset.reshape(1, heads), fading.reshape(1, heads),
    )
    entering = entering_state(message)
    partial = pl.pallas_call(
        mixer_kernel,
        grid=(steps,),
        in_specs=[
            block(inner), block(group), block(group), block(inner), across(2 * heads),
            whole(STATE, inner), whole(1, heads), whole(1, inner), whole(inner, width),
        ],
        out_specs=block(width),
        out_shape=jax.ShapeDtypeStruct((rows, width), bf16),
        scratch_shapes=[
            pltpu.VMEM((STATE, inner), f32),
            pltpu.VMEM((SPAN, inner), f32),
            pltpu.VMEM((SPAN, inner), bf16),
        ],
        compiler_params=params("arbitrary"),
        cost_estimate=cost(2e10, 2e7),
        name="mixer",
    )(
        xs, bs, cs, gating, row, entering,
        skip.reshape(1, heads), gain.reshape(1, inner), projection,
    )
    return lax.psum_scatter(partial, "tp", scatter_dimension=0, tiled=True)


FIRST = 16
SECOND = 40
OTHERS = 36


def second_slot(inside):
    other = inside < OTHERS
    return (
        jnp.where(other, inside // EARLY + 1, 0),
        jnp.where(other, inside % EARLY + LATE, inside - OTHERS + FIRST),
    )


def expert_of(rows, first, per, experts):
    at = lax.broadcasted_iota(jnp.int32, (rows, experts), 0) + first
    return (at // per == lax.broadcasted_iota(jnp.int32, (rows, experts), 1)).astype(bf16)


def route_kernel(x_ref, gain_ref, pick_ref, score_ref, token_ref, first_ref):
    tokens, width = x_ref.shape
    experts = first_ref.shape[0] // FIRST
    x = x_ref[...].astype(f32)
    x = x - jnp.mean(x, axis=1, keepdims=True)
    x = x * lax.rsqrt(jnp.mean(x * x, axis=1, keepdims=True) + norm_eps) * gain_ref[...]
    normed = x.astype(bf16)
    token_ref[:, 0:width] = normed
    weight = jnp.exp(score_ref[...])
    weight = weight / jnp.sum(weight, axis=0, keepdims=True)
    lane = lax.broadcasted_iota(jnp.int32, (experts, tokens), 0)
    taken = jnp.zeros((experts, tokens), f32)
    dense = jnp.zeros((experts, tokens), f32)
    for k in range(pick_ref.shape[0]):
        hit = pick_ref[k : k + 1, :] == lane
        taken = jnp.where(hit, 1.0, taken)
        dense = jnp.where(hit, weight[k : k + 1, :], dense)
    earlier = (
        lax.broadcasted_iota(jnp.int32, (tokens, tokens), 0)
        < lax.broadcasted_iota(jnp.int32, (tokens, tokens), 1)
    ).astype(bf16)
    slot = jnp.where(taken > 0, mm(taken.astype(bf16), earlier), -1.0)
    token_ref[:, width : width + 128] = jnp.concatenate(
        [slot, dense, jnp.zeros((128 - 2 * experts, tokens), f32)], axis=0
    ).T.astype(bf16)
    rows = experts * FIRST
    spread = mm(expert_of(rows, 0, FIRST, experts), slot.astype(bf16))
    wanted = lax.broadcasted_iota(jnp.int32, (rows, 1), 0) % FIRST
    first_ref[...] = mm((spread == wanted.astype(f32)).astype(bf16), normed).astype(bf16)


def second_kernel(table_ref, apart_ref, out_ref, *, experts):
    width = table_ref.shape[1] - 128
    rows = out_ref.shape[0]
    first = pl.program_id(0) * rows
    spread = mm_last(expert_of(rows, first, SECOND, experts), table_ref[:, width : width + experts])
    at = lax.broadcasted_iota(jnp.int32, (rows, 1), 0) + first
    block, wanted = second_slot(at % SECOND)
    hit = (spread == wanted.astype(f32)) & (apart_ref[...] == block)
    out_ref[...] = mm(hit.astype(bf16), table_ref[:, 0:width]).astype(bf16)


def expert_kernel(x_ref, gate_ref, up_ref, down_ref, out_ref):
    x = x_ref[...]
    g = jnp.minimum(mm(x, gate_ref[...]), clamp_top)
    u = jnp.clip(mm(x, up_ref[...]), -clamp_top, clamp_top) + 1.0
    act = g * (0.5 + 0.5 * jnp.tanh((0.5 * sigmoid_sharp) * g)) * u
    out_ref[...] = mm(act.astype(bf16), down_ref[...]).astype(bf16)


def expert(rows_in, gate, up, down):
    rows, width = rows_in.shape
    hidden = gate.shape[2]
    return pl.pallas_call(
        expert_kernel,
        grid=(rows // ROW_TILE,),
        in_specs=[
            pl.BlockSpec((ROW_TILE, width), lambda i: (i, 0)),
            pl.BlockSpec((None, width, hidden), lambda i: (0, 0, 0)),
            pl.BlockSpec((None, width, hidden), lambda i: (0, 0, 0)),
            pl.BlockSpec((None, hidden, width), lambda i: (0, 0, 0)),
        ],
        out_specs=pl.BlockSpec((ROW_TILE, width), lambda i: (i, 0)),
        out_shape=jax.ShapeDtypeStruct((rows, width), bf16),
        compiler_params=params("arbitrary"),
        cost_estimate=cost(6 * rows * width * hidden, 3 * 2 * width * hidden + 4 * rows * width),
        name="expert",
    )(rows_in, gate, up, down)


def joint_kernel(
    rows_hbm, late_hbm, own_ref, tags_ref, gate_hbm, up_hbm, down_hbm, out_ref,
    rows, gate, up, down, res, back, late_own, mid_own, mid, mid_sum, from_left, from_right,
    late_sum, late_back, own_back, pick, pick_first, mix, part, part_mid, part_sum, part_left, part_right,
    load_sem, weight_sem, late_load, send_sem, recv_sem, share_send, share_recv,
    late_send, late_recv, own_send, own_recv, part_send, part_recv,
):
    ep, per, width = res.shape
    experts = ep
    tokens = out_ref.shape[0]
    blocks = tags_ref.shape[0] // tokens
    col_tile = part.shape[3]
    z, y, core = lax.axis_index("ep_0"), lax.axis_index("ep_1"), lax.axis_index("ep_2")
    tp = lax.axis_index("tp")
    me = (z * 4 + y) * 2 + core
    mesh_ids = pl.DeviceIdType.MESH

    def place(k):
        return (z + k // 2) % 4, (y + k // 8 + k // 2) % 4, (core + k) % 2

    def index(k):
        a, b, c = place(k)
        return (a * 4 + b) * 2 + c

    def device(k):
        a, b, c = place(k)
        return {"ep_0": a, "ep_1": b, "ep_2": c}

    def load(k):
        return pltpu.make_async_copy(rows_hbm.at[index(k)], rows.at[k], load_sem.at[k])

    def weights():
        return [
            pltpu.make_async_copy(src, dst, weight_sem.at[n])
            for n, (src, dst) in enumerate(((gate_hbm, gate), (up_hbm, up), (down_hbm, down)))
        ]

    def give_back(k):
        return pltpu.make_async_remote_copy(
            src_ref=res.at[k], dst_ref=back.at[k], send_sem=send_sem.at[k], recv_sem=recv_sem.at[k],
            device_id=device(k), device_id_type=mesh_ids,
        )

    def give_late(k):
        return pltpu.make_async_remote_copy(
            src_ref=late_sum.at[index(k)], dst_ref=late_back.at[me],
            send_sem=late_send.at[k], recv_sem=late_recv.at[k],
            device_id=device(k), device_id_type=mesh_ids,
        )

    def give_own(k):
        return pltpu.make_async_remote_copy(
            src_ref=own_ref.at[index(k)], dst_ref=own_back.at[me],
            send_sem=own_send.at[k], recv_sem=own_recv.at[k],
            device_id=device(k), device_id_type=mesh_ids,
        )

    half = ep // 2
    parts = (pl.ds(0, half), pl.ds(half, half))
    sides = (1, blocks - 1)
    opposite = (tp + 2) % blocks

    def along(side, src, dst, send, recv):
        return pltpu.make_async_remote_copy(
            src_ref=src, dst_ref=dst, send_sem=send, recv_sem=recv,
            device_id={"tp": (tp + sides[side]) % blocks}, device_id_type=mesh_ids,
        )

    def share(stage, side):
        owner = (tp + sides[side]) % blocks
        landing = (from_left, from_right)[side]
        if stage == 0:
            src, dst = late_hbm.at[opposite, parts[side]], mid.at[side]
        elif stage == 1:
            src, dst = late_hbm.at[owner, parts[1 - side]], landing.at[parts[1 - side]]
        else:
            src, dst = mid_sum.at[side], landing.at[parts[side]]
        return along(side, src, dst, share_send.at[stage, side], share_recv.at[stage, side])

    def own_loads():
        return [pltpu.make_async_copy(late_hbm.at[tp], late_own, late_load.at[2])] + [
            pltpu.make_async_copy(
                late_hbm.at[(tp + sides[n]) % blocks, parts[n]], mid_own.at[n], late_load.at[n]
            )
            for n in range(2)
        ]

    tiles = part.shape[0]

    def side_of(t):
        return 0 if t < tiles // 2 else 1

    def give_part(stage, t):
        side = side_of(t) if stage != 1 else 1 - side_of(t)
        landing = (part_left, part_right)[side]
        if stage == 0:
            src, dst = part.at[t, 2], part_mid.at[t]
        elif stage == 1:
            src, dst = part.at[t, sides[side]], landing.at[t]
        else:
            src, dst = part_sum.at[t], landing.at[t]
        return along(side, src, dst, part_send.at[stage, t], part_recv.at[stage, t])

    group = 8

    @pl.loop(0, group)
    def _(k):
        load(k).start()

    for w in weights():
        w.start()

    @pl.loop(group, ep)
    def _(k):
        load(k).start()

    barrier = pltpu.get_barrier_semaphore()

    @pl.loop(1, ep)
    def _(k):
        pl.semaphore_signal(barrier, inc=1, device_id=device(k), device_id_type=mesh_ids)

    for r in sides:
        pl.semaphore_signal(
            barrier, inc=1, device_id={"tp": (tp + r) % blocks}, device_id_type=mesh_ids
        )
    pl.semaphore_wait(barrier, ep - 1 + len(sides))

    for stage in range(2):
        for side in range(2):
            share(stage, side).start()
    for load_own in own_loads():
        load_own.start()

    for w in weights():
        w.wait()

    @pl.loop(0, ep // group)
    def _(c):
        @pl.loop(0, group)
        def _(j):
            load(c * group + j).wait()

        x = rows[pl.ds(c * group, group)].reshape(group * per, width)
        g = jnp.minimum(mm(x, gate[...]), clamp_top)
        u = jnp.clip(mm(x, up[...]), -clamp_top, clamp_top) + 1.0
        act = (g * (0.5 + 0.5 * jnp.tanh((0.5 * sigmoid_sharp) * g)) * u).astype(bf16)
        res[pl.ds(c * group, group)] = mm(act, down[...]).astype(bf16).reshape(group, per, width)

        @pl.loop(0, group)
        def _(j):
            @pl.when(c * group + j > 0)
            def _():
                give_back(c * group + j).start()

    @pl.loop(1, ep)
    def _(k):
        give_own(k).start()

    back[0] = res[0]
    own_back[me] = own_ref[me]

    for load_own in own_loads():
        load_own.wait()
    for side in range(2):
        share(0, side).wait_recv()

        @pl.loop(0, half)
        def _(k):
            mid_sum[side, k] = (mid_own[side, k].astype(f32) + mid[side, k].astype(f32)).astype(bf16)

        share(2, side).start()

    count = group * per
    block, wanted = second_slot(lax.broadcasted_iota(jnp.int32, (1, count), 1) % per)
    for c in range(ep // group):
        sent = lax.broadcasted_iota(jnp.int32, (count, experts), 0) // per + c * group
        holder = (z + 64 - sent // 2) % 4 * 4 + (y + 64 - sent // 8 - sent // 2) % 4
        holder = holder * 2 + (core + 64 - sent) % 2
        chosen = (holder == lax.broadcasted_iota(jnp.int32, (count, experts), 1)).astype(bf16)
        for r in range(blocks):
            q = (tp + r) % blocks
            table = tags_ref[pl.ds(pl.multiple_of(q * tokens, tokens), tokens), :]
            slot = mm_last(table[:, 0:experts], chosen)
            weight = mm_last(table[:, experts : 2 * experts], chosen)
            hit = (slot == wanted.astype(f32)) & (block == r)
            pick[c, r * tokens : (r + 1) * tokens, :] = jnp.where(hit, weight, 0.0).astype(bf16)
    own = tags_ref[pl.ds(pl.multiple_of(tp * tokens, tokens), tokens), :]
    chosen = expert_of(experts * LATE, 0, LATE, experts)
    slot = mm_last(own[:, 0:experts], chosen)
    weight = mm_last(own[:, experts : 2 * experts], chosen)
    at = lax.broadcasted_iota(jnp.int32, (1, experts * LATE), 1) % LATE
    for n in range(FIRST // LATE):
        hit = slot == (at + n * LATE).astype(f32)
        pick_first[n] = jnp.where(hit, weight, 0.0).astype(bf16)

    def mixed_in(c, t):
        cols = slice(t * col_tile, (t + 1) * col_tile)
        got = back[c * group : (c + 1) * group, :, cols].reshape(count, col_tile)
        return mm(pick[c], got) if c == 0 else mix[:, cols] + mm(pick[c], got)

    def arrived(c):
        @pl.loop(max(c * group, 1), (c + 1) * group)
        def _(k):
            give_back(k).wait_recv()

    def mix_in(c):
        arrived(c)
        for t in range(tiles):
            mix[:, t * col_tile : (t + 1) * col_tile] = mixed_in(c, t)

    mix_in(0)
    mix_in(1)

    for stage in (1, 2):
        for side in range(2):
            share(stage, side).wait_recv()

    @pl.loop(0, ep)
    def _(k):
        total = from_left[k].astype(f32) + from_right[k].astype(f32)
        late_sum[k] = (total + late_own[k].astype(f32)).astype(bf16)

    @pl.loop(1, ep)
    def _(k):
        give_late(k).start()

    late_back[me] = late_sum[me]

    mix_in(2)
    arrived(3)

    for t in range(tiles):
        got = mixed_in(3, t).astype(bf16)
        part[t] = got.reshape(blocks, tokens, col_tile)
        give_part(0, t).start()
        give_part(1, t).start()

    for t in range(tiles):
        give_part(0, t).wait_recv()
        own_part = part[t, sides[side_of(t)]].astype(f32)
        part_sum[t] = (own_part + part_mid[t].astype(f32)).astype(bf16)
        give_part(2, t).start()

    @pl.loop(1, ep)
    def _(k):
        give_own(k).wait_recv()
        give_late(k).wait_recv()

    for t in range(tiles):
        cols = slice(t * col_tile, (t + 1) * col_tile)
        total = part[t, 0].astype(f32)
        for n, ref in enumerate((late_back, own_back)):
            total = total + mm(pick_first[n], ref[:, :, cols].reshape(experts * LATE, col_tile))
        for stage in (1, 2):
            give_part(stage, t).wait_recv()
        total = total + part_left[t].astype(f32) + part_right[t].astype(f32)
        out_ref[:, cols] = total.astype(bf16)

    @pl.loop(1, ep)
    def _(k):
        give_back(k).wait_send()
        give_own(k).wait_send()
        give_late(k).wait_send()

    for stage in range(3):
        for side in range(2):
            share(stage, side).wait_send()
        for t in range(tiles):
            give_part(stage, t).wait_send()


def joint(second_in, late_part, own_part, tags, gate, up, down, tokens):
    ep, per, width = second_in.shape
    hidden = gate.shape[1]
    blocks = tags.shape[0] // tokens
    tiles = width // 512
    any_ref = pl.BlockSpec(memory_space=pl.ANY)
    vmem = pl.BlockSpec(memory_space=pltpu.VMEM)
    dma = pltpu.SemaphoreType.DMA
    return pl.pallas_call(
        joint_kernel,
        in_specs=[any_ref, any_ref, vmem, vmem, any_ref, any_ref, any_ref],
        out_specs=vmem,
        out_shape=jax.ShapeDtypeStruct((tokens, width), bf16),
        scratch_shapes=[
            pltpu.VMEM((ep, per, width), bf16),
            pltpu.VMEM((width, hidden), bf16),
            pltpu.VMEM((width, hidden), bf16),
            pltpu.VMEM((hidden, width), bf16),
            pltpu.VMEM((ep, per, width), bf16),
            pltpu.VMEM((ep, per, width), bf16),
            pltpu.VMEM((ep, LATE, width), bf16),
            pltpu.VMEM((2, ep // 2, LATE, width), bf16),
            pltpu.VMEM((2, ep // 2, LATE, width), bf16),
            pltpu.VMEM((2, ep // 2, LATE, width), bf16),
            pltpu.VMEM((ep, LATE, width), bf16),
            pltpu.VMEM((ep, LATE, width), bf16),
            pltpu.VMEM((ep, LATE, width), bf16),
            pltpu.VMEM((ep, LATE, width), bf16),
            pltpu.VMEM((ep, LATE, width), bf16),
            pltpu.VMEM((ep // 8, blocks * tokens, 8 * per), bf16),
            pltpu.VMEM((FIRST // LATE, tokens, ep * LATE), bf16),
            pltpu.VMEM((blocks * tokens, width), f32),
            pltpu.VMEM((tiles, blocks, tokens, 512), bf16),
            pltpu.VMEM((tiles, tokens, 512), bf16),
            pltpu.VMEM((tiles, tokens, 512), bf16),
            pltpu.VMEM((tiles, tokens, 512), bf16),
            pltpu.VMEM((tiles, tokens, 512), bf16),
            dma((ep,)), dma((3,)), dma((3,)), dma((ep,)), dma((ep,)), dma((3, 2)), dma((3, 2)),
            dma((ep,)), dma((ep,)), dma((ep,)), dma((ep,)),
            dma((3, tiles)), dma((3, tiles)),
        ],
        compiler_params=pltpu.CompilerParams(
            collective_id=1, has_side_effects=True, vmem_limit_bytes=60 * 1024 * 1024
        ),
        cost_estimate=cost(4e10, 3e7),
        name="joint",
    )(second_in, late_part, own_part, tags, gate, up, down)


def exchanged(value):
    return lax.all_to_all(value, EP, split_axis=0, concat_axis=0, tiled=True)


def experts_half(sample, gain, pick, score, gate, up, down):
    tokens, width = sample.shape
    experts = lax.axis_size(EP)
    blocks = lax.axis_size("tp")
    every = width + 128
    own, first_out = pl.pallas_call(
        route_kernel,
        out_shape=[
            jax.ShapeDtypeStruct((tokens, every), bf16),
            jax.ShapeDtypeStruct((experts * FIRST, width), bf16),
        ],
        compiler_params=params(),
        cost_estimate=cost(1e9, 3e6),
        name="route",
    )(sample, gain.reshape(1, width), pick.T, score.T)
    apart = (jnp.arange(blocks * tokens, dtype=jnp.int32) // tokens - lax.axis_index("tp")) % blocks
    table = lax.all_gather(own, "tp", axis=0, tiled=True)
    first_in = exchanged(first_out.reshape(experts, FIRST, width))
    late_rows = lax.all_gather(first_in[:, :LATE], "tp", axis=0, tiled=True).reshape(-1, width)

    count = experts * SECOND
    tile = count // 4
    second_out = pl.pallas_call(
        functools.partial(second_kernel, experts=experts),
        grid=(count // tile,),
        in_specs=[
            pl.BlockSpec((blocks * tokens, every), lambda i: (0, 0)),
            pl.BlockSpec((1, blocks * tokens), lambda i: (0, 0)),
        ],
        out_specs=pl.BlockSpec((tile, width), lambda i: (i, 0)),
        out_shape=jax.ShapeDtypeStruct((count, width), bf16),
        compiler_params=params("arbitrary"),
        cost_estimate=cost(3.2e9, 1e7),
        name="second",
    )(table, apart.reshape(1, -1))
    second_in = exchanged(second_out.reshape(experts, SECOND, width))

    late_part = expert(late_rows, gate, up, down)
    own_part = expert(first_in[:, LATE:].reshape(-1, width), gate, up, down)
    return joint(
        second_in, late_part.reshape(blocks, experts, LATE, width),
        own_part.reshape(experts, FIRST - LATE, width), table[:, width:], gate[0], up[0], down[0], tokens,
    )


def body(*args):
    moe_out = experts_half(*args[14:])
    mixed = mixer_half(*args[:14])
    return (mixed, moe_out)


def solution(mesh):
    split = Mesh(mesh.devices.reshape(4, 4, 2, mesh.shape["tp"]), ("ep_0", "ep_1", "ep_2", "tp"))
    return jax.shard_map(
        body,
        mesh=split,
        in_specs=(
            P(EP, "tp"),
            P(EP, "tp"),
            P(EP, "tp"),
            P(EP, "tp"),
            P(EP, "tp"),
            P(None, "tp"),
            P(None, "tp"),
            P(None, "tp"),
            P("tp"),
            P("tp"),
            P("tp"),
            P(EP, "tp"),
            P("tp"),
            P("tp", None),
            P(EP_TP, None),
            P(),
            P(EP_TP, None),
            P(EP_TP, None),
            P(EP, None, "tp"),
            P(EP, None, "tp"),
            P(EP, "tp", None),
        ),
        out_specs=(P(EP_TP, None), P(EP_TP, None)),
        check_vma=False,
    )
```
